512 devices in a mesh: sp: 32 (over z, x), tp: 16 (over y, core).
Axes of the slice: x: 4, y: 8, z: 8, core: 2. Of those that a mesh axis runs over, the one named last changes fastest.
Arguments:
- query_one: bfloat16 [8192, 1024], P('sp', 'tp'), may hold values from -6 to 6
- key_one: bfloat16 [8192, 1024], P('sp', 'tp'), may hold values from -6 to 6
- value_one: bfloat16 [8192, 2048], P('sp', 'tp'), may hold values from -6 to 6
- gate_one: bfloat16 [8192, 2048], P('sp', 'tp'), may hold values from -6 to 6
- decay_one: float32 [2, 8192, 1024], P(None, 'sp', 'tp')
- query_two: bfloat16 [8192, 2048], P('sp', 'tp'), may hold values from -6 to 6
- key_two: bfloat16 [8192, 2048], P('sp', 'tp'), may hold values from -6 to 6
- value_two: bfloat16 [8192, 2048], P('sp', 'tp'), may hold values from -6 to 6
- gate_two: bfloat16 [8192, 2048], P('sp', 'tp'), may hold values from -6 to 6
- decay_two: float32 [2, 8192, 2048], P(None, 'sp', 'tp')
- head_gain: float32 [128], replicated, may hold values from 0.1 to 1.9
- proj_one: bfloat16 [2048, 2048], P('tp'), may hold values from -0.09375 to 0.09375
- proj_two: bfloat16 [2048, 2048], P('tp'), may hold values from -0.09375 to 0.09375
- stream: bfloat16 [8192, 2048], P('sp'), may hold values from -6 to 6
- gain_mix: float32 [2048], replicated, may hold values from 0.1 to 1.9
- gain_moe: float32 [2048], replicated, may hold values from 0.1 to 1.9
- routes: int32 [8192, 2], P('sp'), may hold values from 0 to 31, all different within a row; in each aligned block of 256 rows (0 to 255, 256 to 511, ...) at most 24 rows name the same one
- affinity: float32 [8192, 2], P('sp'), may hold values from 0.1 to 1
- expert_gate: bfloat16 [32, 2048, 2048], P('sp', None, 'tp'), may hold values from -0.125 to 0.125
- expert_up: bfloat16 [32, 2048, 2048], P('sp', None, 'tp'), may hold values from -0.125 to 0.125
- expert_down: bfloat16 [32, 2048, 2048], P('sp', 'tp'), may hold values from -0.125 to 0.125
Outputs:
- output: bfloat16 [8192, 2048], P(('sp', 'tp'))
The draws below stay inside these ranges and needn't reach their ends.
Inputs may be any that keep to these rules, and one draw needn't show every extreme that they name: `routes`: in the 256 rows of one index of sp no expert is named more than 24 times, a bound that some block reaches there in every draw; a row names 2 different experts.
All inputs are finite; a program needn't handle non-finite values.
Results may differ from the reference program's by a relative error of at most 0.017.
Values may be sent and summed in bfloat16 or wider, within the bound.
A program may use at most 64 MiB of HBM per device.

```python
import math
import jax
import jax.numpy as jnp
import numpy as np
from jax import lax

D = 2048
HEADS_A = 16
HEADS_B = 16
DK_A = 64
DK_B = 128
DV = 128
BLK = 64
FF_E = 2048
TOPK = 2
TOK_DEV = 256
STRING_LENGTH = 8192
EXPERTS = 32
CAP = 24
N_SP = 32
N_TP = 16


def decay_field(key, channels):
    keys = jax.random.split(key, 7)
    share = 0.5
    rapid_toggle = jax.random.bernoulli(keys[0], share, (2, 1, channels))
    quick = jax.random.uniform(keys[1], (2, 1, channels), jnp.float32, -0.5, 1.5)
    steady = math.log(STRING_LENGTH / 16.0) + jax.random.uniform(keys[2], (2, 1, channels), jnp.float32, 0.5, 1.5)
    floor_amount = jnp.where(rapid_toggle, quick, steady)
    spans = STRING_LENGTH // TOK_DEV
    additive_displacement = jnp.repeat(jax.random.uniform(keys[3], (2, spans, 1), jnp.float32, -0.7, 0.7), TOK_DEV, axis=1)
    jitter_magnitude = 0.7 * jax.random.truncated_normal(keys[4], -3.0, 3.0, (2, STRING_LENGTH, channels), jnp.float32)
    slot_numbers = jax.random.randint(keys[5], (2, 6), 0, STRING_LENGTH)
    sudden_jump = jnp.any(jnp.arange(STRING_LENGTH)[None, :, None] == slot_numbers[:, None, :], axis=2)[:, :, None]
    intensity_multiplier = jax.random.uniform(keys[6], (2, STRING_LENGTH, 1), jnp.float32, -11.0, -4.0)
    return jnp.where(sudden_jump & jnp.logical_not(rapid_toggle), intensity_multiplier, floor_amount + additive_displacement + jitter_magnitude).astype(jnp.float32)


def draw_decay_one(key, part):
    return decay_field(jax.random.fold_in(key, 11), HEADS_A * DK_A)


def draw_decay_two(key, part):
    return decay_field(jax.random.fold_in(key, 23), HEADS_B * DK_B)


def shard_levels(rng, shape, shards, smallest, high):
    level = 1.0
    for axis_at, shards_of in shards:
        heights = jax.random.uniform(jax.random.fold_in(jax.random.fold_in(rng, 6), axis_at), (shards_of,), jnp.float32, smallest / len(shards), high / len(shards))
        level = level * jnp.repeat(jnp.exp(heights), shape[axis_at] // shards_of).reshape((-1,) + (1,) * (len(shape) - 1 - axis_at))
    return level


def routed_block(stream_key, own, number, rows, count, top, bound, slope):
    ranking = jax.random.permutation(stream_key, count)
    packed, common = shares(count, rows * top, bound, slope, True), shares(count, rows * top, bound, slope, False)
    places = jnp.arange(count)

    def named(tallies, turn):
        used = int((tallies > 0).sum())
        fixed = max(1, used // 4)
        moved = fixed + (places - fixed + turn * (used - fixed)) % max(1, count - fixed)
        return jnp.zeros((count,), jnp.int32).at[ranking[jnp.where(places < fixed, places, moved)]].set(jnp.asarray(tallies, jnp.int32))

    tallies = jnp.where(number % 4 == 0, named(packed, number // 4), named(common, number - number // 4 - 1))
    mixed = jax.random.permutation(jax.random.fold_in(own, 3), count)
    donor, receiver = mixed[0:count // 2 * 2:2], mixed[1:count // 2 * 2:2]
    margin = jnp.minimum(tallies[donor] - 1, bound - tallies[receiver]) // 2
    margin = jnp.where((donor == ranking[0]) | (receiver == ranking[0]) | (tallies[receiver] == 0), 0, jnp.maximum(margin, 0))
    moved = jax.random.randint(jax.random.fold_in(own, 4), (count // 2,), 0, 1 << 20) % (margin + 1)
    tallies = tallies.at[donor].add(-moved).at[receiver].add(moved)
    labels = jnp.searchsorted(jnp.cumsum(tallies), jnp.arange(rows * top), side="right").astype(jnp.int32)
    listing = labels.reshape(top, rows).T
    listing = listing[jax.random.permutation(jax.random.fold_in(own, 1), rows)]
    turn = jax.random.randint(jax.random.fold_in(own, 2), (rows, 1), 0, top)
    return jnp.take_along_axis(listing, (jnp.arange(top)[None, :] + turn) % top, axis=1)


def shares(amount, total, bound, slope, full):
    loads = [(1 << 20) // math.isqrt(rank ** slope) + 1 for rank in range(1, amount + 1)]
    largest = bound if full else min(bound, max(-(-total // amount), total * loads[0] // sum(loads)))
    least = 1 if total - largest >= amount - 1 else 0
    given, rest = [largest] + [least] * (amount - 1), total - largest - least * (amount - 1)
    while rest > 0:
        movable = [i for i in range(1, amount) if given[i] < largest] or [i for i in range(1, amount) if given[i] < bound]
        pool, left = sum([loads[i] for i in movable]), rest
        for i in movable:
            addition = min(bound - given[i], max(1, left * loads[i] // pool), rest)
            given[i] = given[i] + addition
            rest = rest - addition
    return np.array(given)


def centred(own_key, extent, scale, limit, pieces=(), kind=jnp.bfloat16):
    values = jax.random.normal(own_key, extent, jnp.float32) * scale
    if len(pieces) > 0:
        values = shard_levels(own_key, extent, pieces, -0.22, 0.18) * values
    return jnp.clip(values, min=-limit, max=limit).astype(kind)


def setup_inputs(seed: int = 0) -> dict:
    seeds = jax.random.split(jax.random.key(seed), 22)
    query_one = centred(seeds[0], (STRING_LENGTH, HEADS_A * DK_A), 1.0, 6.0, ((0, 32), (1, 16)))
    key_one = centred(seeds[1], (STRING_LENGTH, HEADS_A * DK_A), 1.0, 6.0, ((0, 32), (1, 16)))
    value_one = centred(seeds[2], (STRING_LENGTH, HEADS_A * DV), 1.0, 6.0, ((0, 32), (1, 16)))
    gate_one = centred(seeds[3], (STRING_LENGTH, HEADS_A * DV), 1.0, 6.0, ((0, 32), (1, 16)))
    decay_one = draw_decay_one(jax.random.fold_in(seeds[21], 71), 0)
    query_two = centred(seeds[5], (STRING_LENGTH, HEADS_B * DK_B), 1.0, 6.0, ((0, 32), (1, 16)))
    key_two = centred(seeds[6], (STRING_LENGTH, HEADS_B * DK_B), 1.0, 6.0, ((0, 32), (1, 16)))
    value_two = centred(seeds[7], (STRING_LENGTH, HEADS_B * DV), 1.0, 6.0, ((0, 32), (1, 16)))
    gate_two = centred(seeds[8], (STRING_LENGTH, HEADS_B * DV), 1.0, 6.0, ((0, 32), (1, 16)))
    decay_two = draw_decay_two(jax.random.fold_in(seeds[21], 71), 0)
    head_gain = jnp.clip(1.0 + 0.18 * jax.random.normal(seeds[10], (DV,), jnp.float32), 0.1, 1.9)
    proj_one = centred(seeds[11], (HEADS_A * DV, D), ((HEADS_A + HEADS_B) * DV) ** -0.5, 0.09375, ((0, 16),))
    proj_two = centred(seeds[12], (HEADS_B * DV, D), ((HEADS_A + HEADS_B) * DV) ** -0.5, 0.09375, ((0, 16),))
    stream = centred(seeds[13], (STRING_LENGTH, D), 1.0, 6.0, ((0, 32),))
    gain_mix = jnp.clip(1.0 + 0.18 * jax.random.normal(seeds[14], (D,), jnp.float32), 0.1, 1.9)
    gain_moe = jnp.clip(1.0 + 0.18 * jax.random.normal(seeds[15], (D,), jnp.float32), 0.1, 1.9)
    routes_keys = jax.random.split(jax.random.fold_in(seeds[16], 1), STRING_LENGTH // TOK_DEV)
    routes_turns = jax.random.permutation(jax.random.fold_in(seeds[16], 3), STRING_LENGTH // TOK_DEV)
    routes = jax.vmap(lambda own, number: routed_block(jax.random.fold_in(seeds[16], 2), own, number, TOK_DEV, EXPERTS, TOPK, CAP, 2))(routes_keys, routes_turns).reshape((STRING_LENGTH, TOPK))
    affinity = jnp.clip(0.1 + 0.9 * jax.random.uniform(seeds[17], (STRING_LENGTH, TOPK), jnp.float32) ** shard_levels(seeds[17], (STRING_LENGTH, TOPK), ((0, 32),), -0.2, 0.2), 0.1, 1.0)
    expert_gate = centred(seeds[18], (EXPERTS, D, FF_E), D ** -0.5, 0.125, ((0, 32), (2, 16)))
    expert_up = centred(seeds[19], (EXPERTS, D, FF_E), D ** -0.5, 0.125, ((0, 32), (2, 16)))
    expert_down = centred(seeds[20], (EXPERTS, FF_E, D), FF_E ** -0.5, 0.125, ((0, 32), (1, 16)))
    return {"query_one": query_one, "key_one": key_one, "value_one": value_one, "gate_one": gate_one, "decay_one": decay_one, "query_two": query_two, "key_two": key_two, "value_two": value_two, "gate_two": gate_two, "decay_two": decay_two, "head_gain": head_gain, "proj_one": proj_one, "proj_two": proj_two, "stream": stream, "gain_mix": gain_mix, "gain_moe": gain_moe, "routes": routes, "affinity": affinity, "expert_gate": expert_gate, "expert_up": expert_up, "expert_down": expert_down}


normalizer_sharpness = 16.0
highest = lax.Precision.HIGHEST

def heads_first(values, heads):
    return values.reshape(values.shape[0], heads, -1).transpose(1, 0, 2)

def block_scan(query, key, value, logarithm_fading):
    heads, length, key_size = query.shape
    value_size = value.shape[-1]
    count = length // BLK

    def blocks(tensor):
        return tensor.reshape(heads, count, BLK, tensor.shape[-1])
    qb, kb, vb, gb = (blocks(query), blocks(key), blocks(value), blocks(logarithm_fading))
    cum = jnp.cumsum(gb, axis=2)
    last = cum[:, :, -1:, :]
    q_in = qb * jnp.exp(cum)
    k_in = kb * jnp.exp(-cum)
    k_st = kb * jnp.exp(last - cum)
    lower = jnp.tril(jnp.ones((BLK, BLK), dtype=bool))
    scores = jnp.where(lower, jnp.einsum('hnid,hnjd->hnij', q_in, k_in, precision=highest), 0.0)
    inner = jnp.einsum('hnij,hnjv->hniv', scores, vb, precision=highest)
    growth = jnp.einsum('hnjd,hnjv->hndv', k_st, vb, precision=highest)
    fading_speed = jnp.exp(last[:, :, 0, :])

    def step(state, inputs):
        factor, added = inputs
        return (factor[..., None] * state + added, state)
    final, starts = lax.scan(step, jnp.zeros((heads, key_size, value_size), jnp.float32), (fading_speed.transpose(1, 0, 2), growth.transpose(1, 0, 2, 3)))
    carried = jnp.einsum('hnid,hndv->hniv', q_in, starts.transpose(1, 0, 2, 3), precision=highest)
    return ((inner + carried).reshape(heads, length, value_size), final)

def group_mixed(query, key, value, fading_speed, key_size):
    heads = query.shape[1] // key_size
    qh = heads_first(query.astype(jnp.float32), heads) * key_size ** (-0.5)
    kh = heads_first(key.astype(jnp.float32), heads)
    vh = heads_first(value.astype(jnp.float32), heads)
    logarithm_fading = jax.nn.log_sigmoid(fading_speed) / normalizer_sharpness
    ahead = heads_first(logarithm_fading[0], heads)
    behind = heads_first(logarithm_fading[1], heads)
    forward, _ = block_scan(qh, kh, vh, ahead)
    backward, _ = block_scan(qh[:, ::-1], kh[:, ::-1], vh[:, ::-1], behind[:, ::-1])
    return forward + backward[:, ::-1]

def finish(mixed, gate, head_gain):
    normed = mixed * lax.rsqrt(lax.optimization_barrier(jnp.mean(mixed * mixed, axis=-1, keepdims=True)) + 1e-06) * head_gain
    flat = normed.transpose(1, 0, 2).reshape(mixed.shape[1], -1)
    return (flat * jax.nn.silu(gate.astype(jnp.float32))).astype(jnp.bfloat16)

def layer_norm(values, gain):
    mean = lax.optimization_barrier(jnp.mean(values, axis=-1, keepdims=True))
    spread = lax.optimization_barrier(jnp.mean(jnp.square(values - mean), axis=-1, keepdims=True))
    return (values - mean) * lax.rsqrt(spread + 1e-05) * gain

def reference(query_one, key_one, value_one, gate_one, decay_one, query_two, key_two, value_two, gate_two, decay_two, head_gain, proj_one, proj_two, stream, gain_mix, gain_moe, routes, affinity, expert_gate, expert_up, expert_down):
    heads_one = finish(group_mixed(query_one, key_one, value_one, decay_one, DK_A), gate_one, head_gain)
    heads_two = finish(group_mixed(query_two, key_two, value_two, decay_two, DK_B), gate_two, head_gain)
    width_one = HEADS_A // N_TP * DV
    width_two = HEADS_B // N_TP * DV
    total = jnp.zeros((STRING_LENGTH, D), jnp.float32)
    for block in range(N_TP):
        part = jnp.dot(heads_one[:, block * width_one:(block + 1) * width_one], proj_one[block * width_one:(block + 1) * width_one], preferred_element_type=jnp.float32)
        part = part + jnp.dot(heads_two[:, block * width_two:(block + 1) * width_two], proj_two[block * width_two:(block + 1) * width_two], preferred_element_type=jnp.float32)
        total = total + lax.optimization_barrier(part.astype(jnp.bfloat16)).astype(jnp.float32)
    attn = total.astype(jnp.bfloat16)
    settled = layer_norm(stream.astype(jnp.float32) + attn.astype(jnp.float32), gain_mix)
    moe_in = settled.astype(jnp.bfloat16)
    weights = (affinity / lax.optimization_barrier(jnp.sum(affinity, axis=-1, keepdims=True))).reshape(-1)
    assigned = STRING_LENGTH * TOPK
    flat_expert = routes.reshape(-1).astype(jnp.int32)
    order = jnp.argsort(flat_expert, stable=True).astype(jnp.int32)
    sorted_expert = flat_expert[order]
    counts = lax.optimization_barrier(jnp.sum((flat_expert[:, None] == jnp.arange(EXPERTS, dtype=jnp.int32)[None, :]).astype(jnp.int32), axis=0)).astype(jnp.int32)
    starts = (jnp.cumsum(counts).astype(jnp.int32) - counts).astype(jnp.int32)
    most_rows = N_SP * CAP
    slot = (jnp.arange(assigned, dtype=jnp.int32) - starts[sorted_expert]).astype(jnp.int32)
    table = jnp.full((EXPERTS * most_rows,), -1, jnp.int32).at[sorted_expert * most_rows + slot].set(order)
    table = table.reshape(EXPERTS, most_rows)
    unit_block = FF_E // N_TP

    def per_expert(acc, expert):
        entries = table[expert]
        valid = entries >= 0
        safe = jnp.where(valid, entries, 0).astype(jnp.int32)
        token = (safe // TOPK).astype(jnp.int32)
        rows = moe_in[token]
        gate = jnp.dot(rows, expert_gate[expert], preferred_element_type=jnp.float32)
        upward = jnp.dot(rows, expert_up[expert], preferred_element_type=jnp.float32)
        act = (jax.nn.silu(gate) * upward).astype(jnp.bfloat16)
        act_blocks = act.astype(jnp.float32).reshape(most_rows, N_TP, unit_block)
        down_blocks = expert_down[expert].astype(jnp.float32).reshape(N_TP, unit_block, D)
        partial_value = jnp.einsum('rbf,bfd->rbd', act_blocks, down_blocks, precision=highest)
        rounded = lax.optimization_barrier(partial_value.astype(jnp.bfloat16)).astype(jnp.float32)
        piece = lax.optimization_barrier(lax.optimization_barrier(jnp.sum(rounded, axis=1)).astype(jnp.bfloat16)).astype(jnp.float32)
        scale = jnp.where(valid, weights[safe], 0.0)
        return (acc.at[token].add(scale[:, None] * piece), None)
    mixture, _ = lax.scan(per_expert, jnp.zeros((STRING_LENGTH, D), jnp.float32), jnp.arange(EXPERTS, dtype=jnp.int32))
    return layer_norm(settled + mixture, gain_moe).astype(jnp.bfloat16)
```

```python
import functools

import jax
import jax.numpy as jnp
from jax import lax
from jax.experimental import pallas as pl
from jax.experimental.pallas import tpu as pltpu
from jax.sharding import PartitionSpec as P

MESH = pl.DeviceIdType.MESH
F32 = jnp.float32
BF16 = jnp.bfloat16
BLK = 64
LANES = 128
ANY = pl.ANY


def mm(a, b):
    return jnp.dot(a, b, preferred_element_type=F32)


def mm_t(a, b):
    return lax.dot_general(a, b, (((1,), (1,)), ((), ())), preferred_element_type=F32)


def tmm(a, b):
    return lax.dot_general(a, b, (((0,), (0,)), ((), ())), preferred_element_type=F32)


def iota(shape, dim):
    return lax.broadcasted_iota(jnp.int32, shape, dim)


def layer_norm(values, gain):
    mean = jnp.mean(values, axis=-1, keepdims=True)
    spread = jnp.mean(jnp.square(values - mean), axis=-1, keepdims=True)
    return (values - mean) * lax.rsqrt(spread + 1e-05) * gain


def kernel(
    cfg,
    q1h, k1h, v1h, g1h, d1h, q2h, k2h, v2h, g2h, d2h, hgh, p1h, p2h, sth, gmh, goh, rth, afh, egh, euh, edh,
    out,
    q1, k1, v1, g1, d1, q2, k2, v2, g2, d2, hg, own_proj, other_proj, stream, gm, go, rt, af, wgu, own_down, other_down,
    sbuf, sarr, fsum, sret, sback,
    qin, kin, grow, mixed, heads, heads_in, part,
    pbuf, parr, settled, msend, cols, dsend, darr, rows, acc, act, act_in, rbuf, rarr, rsend, rback,
    pick_hi, pick_lo, term, mix,
    load_sem, s_send, s_recv, sib_send, sib_recv, p_send, p_recv, t_send, t_recv,
    g_send, g_recv, f_send, f_recv, r_send, r_recv,
):
    nsp, ntp, toks, cap = cfg
    ny = ntp // 2
    half_way = ny // 2
    sp = lax.axis_index("sp")
    tp = lax.axis_index("tp")
    y = lax.div(tp, 2)
    c = lax.rem(tp, 2)
    sib = (sp, tp + 1 - 2 * c)
    blocks = toks // BLK
    own_rows = toks // ntp
    width = ntp * LANES
    per = LANES // nsp
    mrow = sbuf.shape[1]
    nrow = nsp * cap
    hrow = nrow // 2

    barrier = pltpu.get_barrier_semaphore()

    def greet_sp(k, carry):
        pl.semaphore_signal(barrier, inc=1, device_id=(lax.rem(sp + k, nsp), tp), device_id_type=MESH)
        return carry

    def greet_tp(k, carry):
        pl.semaphore_signal(barrier, inc=1, device_id=(sp, lax.rem(tp + k, ntp)), device_id_type=MESH)
        return carry

    lax.fori_loop(1, nsp, greet_sp, 0)
    lax.fori_loop(1, ntp, greet_tp, 0)

    loads = []

    def load(src, dst):
        copy = pltpu.make_async_copy(src, dst, load_sem.at[len(loads)])
        copy.start()
        loads.append(copy)
        return copy

    first = [load(a, b) for a, b in ((d1h, d1), (d2h, d2), (k1h, k1), (v1h, v1), (k2h, k2), (v2h, v2), (q1h, q1), (q2h, q2))]
    second = [
        load(a, b)
        for a, b in (
            (g1h, g1), (g2h, g2), (hgh, hg), (p1h, own_proj.at[0:LANES]), (p2h, own_proj.at[LANES:2 * LANES]),
            (sth.at[pl.ds(pl.multiple_of(tp * own_rows, own_rows), own_rows)], stream), (gmh, gm), (goh, go),
            (rth, rt), (afh, af),
            (egh.at[0], wgu.at[:, 0:LANES]), (euh.at[0], wgu.at[:, LANES:2 * LANES]), (edh.at[0], own_down),
        )
    ]

    r = iota((toks, toks), 0)
    s = iota((toks, toks), 1)
    tri = jnp.where((r // BLK == s // BLK) & (s <= r), 1.0, 0.0).astype(BF16)
    low = iota((1, LANES), 1) < LANES // 2
    m = iota((nsp * mrow, LANES), 0)
    o, i = m // mrow, m % mrow
    wanted = jnp.where(i < 3 * per, (i // per) * LANES + o * per + i % per, 3 * LANES + i - 3 * per)
    wanted = jnp.where(i < 3 * per + 3, wanted, -1)
    lane = iota((nsp * mrow, LANES), 1)
    pack = [jnp.where(wanted == lane + g * LANES, 1.0, 0.0).astype(BF16) for g in range(3)]
    lane16 = iota((nsp * mrow, 16), 1)
    pack.append(jnp.where(wanted[:, 0:16] == lane16 + 3 * LANES, 1.0, 0.0).astype(BF16))

    for copy in first:
        copy.wait()

    def two(a):
        return jnp.concatenate([a, a], axis=1)

    fading = (jnp.concatenate([d1[0], d1[1]], axis=1), d2[0], d2[1])
    keys = (two(k1[...].astype(F32)), k2[...].astype(F32), k2[...].astype(F32))
    queries = (two(q1[...].astype(F32)) * 64 ** (-0.5), q2[...].astype(F32) * 128 ** (-0.5), q2[...].astype(F32) * 128 ** (-0.5))
    values = (v1[...], v2[...], v2[...])
    totals = []
    for g in range(3):
        x = fading[g]
        logs = (jnp.minimum(x, 0.0) - jnp.log1p(jnp.exp(-jnp.abs(x)))) * (1.0 / 16.0)
        hi = logs.astype(BF16)
        rest = logs - hi.astype(F32)
        mid = rest.astype(BF16)
        lo = (rest - mid.astype(F32)).astype(BF16)
        cum = mm(tri, hi) + mm(tri, mid) + mm(tri, lo)
        rows_of = []
        for b in range(blocks):
            at = slice(b * BLK, (b + 1) * BLK)
            ahead = cum[at]
            tot = ahead[BLK - 1:BLK]
            behind = tot - ahead + logs[at]
            run = ahead if g == 1 else behind if g == 2 else jnp.where(low, ahead, behind)
            qin[g, at] = (queries[g][at] * jnp.exp(run)).astype(BF16)
            kin[g, at] = (keys[g][at] * jnp.exp(-run)).astype(BF16)
            kst = (keys[g][at] * jnp.exp(tot - run)).astype(BF16)
            grow[g, b] = tmm(values[g][at], kst)
            rows_of.append(tot)
        totals.append(rows_of)

    fades = [[jnp.exp(t) for t in row] for row in totals]

    def chained(g, order, start):
        state = start
        seen = {}
        for b in order:
            seen[b] = state
            state = fades[g][b] * state + grow[g, b]
        return seen, state

    up, down = list(range(blocks)), list(range(blocks - 1, -1, -1))
    zero = jnp.zeros((LANES, LANES), F32)
    ends = [
        jnp.where(low, chained(0, up, zero)[1], chained(0, down, zero)[1]),
        chained(1, up, zero)[1],
        chained(2, down, zero)[1],
    ]
    sums = [sum(row[1:], row[0]) for row in totals]
    r16 = iota((16, LANES), 0)
    tail = jnp.where(r16 == 0, sums[0], jnp.where(r16 == 1, sums[1], jnp.where(r16 == 2, sums[2], 0.0)))
    packed = mm(pack[3], tail.astype(BF16))
    for g in range(3):
        packed = packed + mm(pack[g], ends[g].astype(BF16))
    sbuf[...] = packed.astype(BF16).reshape(nsp, mrow, LANES)

    pl.semaphore_wait(barrier, nsp - 1 + ntp - 1)

    def over_sp(base, src, dst, size):
        def copy_to(k):
            to = lax.rem(sp + k, nsp)
            return pltpu.make_async_remote_copy(
                src.at[pl.ds(to * size, size)], dst.at[pl.ds(sp * size, size)],
                s_send.at[base * nsp + k], s_recv.at[base * nsp + k], device_id=(to, tp), device_id_type=MESH,
            )

        def go_out(k, carry):
            copy_to(k).start()
            return carry

        def come_in(k, carry):
            copy_to(k).wait_recv()
            return carry

        def left(k, carry):
            copy_to(k).wait_send()
            return carry

        return go_out, come_in, left

    pending = []

    def send_sp(base, src, dst, size):
        go_out, come_in, left = over_sp(base, src, dst, size)
        lax.fori_loop(1, nsp, go_out, 0)
        dst[pl.ds(sp * size, size)] = src[pl.ds(sp * size, size)]
        pending.append(lambda: lax.fori_loop(1, nsp, left, 0))
        return lambda: lax.fori_loop(1, nsp, come_in, 0)

    remote = []

    def push(src, dst, ssem, rsem, device):
        copy = pltpu.make_async_remote_copy(src, dst, ssem, rsem, device_id=device, device_id_type=MESH)
        copy.start()
        remote.append(copy)
        return copy

    arrive = send_sp(0, sbuf, sarr, 1)
    lend = [
        push(p1h, other_proj.at[0:LANES], sib_send.at[0], sib_recv.at[0], sib),
        push(p2h, other_proj.at[LANES:2 * LANES], sib_send.at[1], sib_recv.at[1], sib),
        push(edh.at[0], other_down, sib_send.at[2], sib_recv.at[2], sib),
    ]

    rr, cc = iota((BLK, BLK), 0), iota((BLK, BLK), 1)
    lower, upper = cc <= rr, cc >= rr
    for b in range(blocks):
        at = slice(b * BLK, (b + 1) * BLK)
        q, k = qin[0, at], kin[0, at]
        nil = jnp.zeros_like(q)
        score = jnp.where(lower, mm_t(jnp.where(low, q, nil), k), 0.0) + jnp.where(upper, mm_t(jnp.where(low, nil, q), k), 0.0)
        mixed[0, at] = mm(score.astype(BF16), values[0][at])
        score = jnp.where(lower, mm_t(qin[1, at], kin[1, at]), 0.0) + jnp.where(upper, mm_t(qin[2, at], kin[2, at]), 0.0)
        mixed[1, at] = mm(score.astype(BF16), values[1][at])

    arrive()
    row = iota((mrow, LANES), 0)
    in_a, in_b = row < per, row < 2 * per

    def tile_of(j):
        t = sarr[j].astype(F32)
        fade = jnp.where(in_a, t[3 * per:3 * per + 1], jnp.where(in_b, t[3 * per + 1:3 * per + 2], t[3 * per + 2:3 * per + 3]))
        return t, jnp.exp(fade)

    state = jnp.zeros((mrow, LANES), F32)
    for j in range(nsp):
        t, fade = tile_of(j)
        fsum[j] = state
        state = fade * state + t
    forward = (in_a & low) | (in_b & jnp.logical_not(in_a))
    state = jnp.zeros((mrow, LANES), F32)
    for j in range(nsp - 1, -1, -1):
        t, fade = tile_of(j)
        sret[j] = jnp.where(forward, fsum[j], state).astype(BF16)
        state = fade * state + t
    arrive = send_sp(1, sret, sback, 1)

    z = iota((LANES, nsp * mrow), 0)
    m = iota((LANES, nsp * mrow), 1)
    lift = (z // per) * mrow + z % per
    unpack = [jnp.where(m == lift + g * per, 1.0, 0.0).astype(BF16) for g in range(3)]

    for copy in second:
        copy.wait()
    experts = iota((nsp, toks), 0)
    hits = [jnp.where(rt[k:k + 1] == experts, 1.0, 0.0) for k in range(2)]
    before = jnp.where(r < s, 1.0, 0.0).astype(BF16)
    counts = mm((hits[0] + hits[1]).astype(BF16), before)
    places = [
        rt[k:k + 1] * cap + jnp.sum(hits[k] * counts, axis=0, keepdims=True).astype(jnp.int32) for k in range(2)
    ]

    arrive()
    back = sback[...].reshape(nsp * mrow, LANES)
    come = [mm(unpack[g], back) for g in range(3)]
    fwd_a, back_a = chained(0, up, come[0])[0], chained(0, down, come[0])[0]
    fwd_b, back_b = chained(1, up, come[1])[0], chained(2, down, come[2])[0]
    for b in range(blocks):
        at = slice(b * BLK, (b + 1) * BLK)
        one = mixed[0, at] + mm_t(qin[0, at], jnp.where(low, fwd_a[b], back_a[b]).astype(BF16))
        other = mixed[1, at] + mm_t(qin[1, at], fwd_b[b].astype(BF16)) + mm_t(qin[2, at], back_b[b].astype(BF16))
        done = []
        for value, gate in ((one, g1), (other, g2)):
            normed = value * lax.rsqrt(jnp.mean(value * value, axis=-1, keepdims=True) + 1e-06) * hg[...]
            done.append((normed * jax.nn.silu(gate[at].astype(F32))).astype(BF16))
        for n in range(BLK // own_rows):
            d = b * (BLK // own_rows) + n
            for k in range(2):
                heads[d % 2, d // 2, :, k * LANES:(k + 1) * LANES] = done[k][n * own_rows:(n + 1) * own_rows]

    shared = push(heads.at[1 - c], heads_in, sib_send.at[3], sib_recv.at[3], sib)
    piece = width // 4
    mine = heads[c].reshape(ny * own_rows, 2 * LANES)
    for n in range(4):
        at = slice(n * piece, (n + 1) * piece)
        part[:, :, at] = mm(mine, own_proj[:, at]).reshape(ny, own_rows, piece)
    for copy in lend[:2]:
        copy.wait_recv()
    shared.wait_recv()
    theirs = heads_in[...].reshape(ny * own_rows, 2 * LANES)
    for n in range(4):
        at = slice(n * piece, (n + 1) * piece)
        part[:, :, at] = part[:, :, at] + mm(theirs, other_proj[:, at]).reshape(ny, own_rows, piece)

    chains = ((1, 0, 0), (-1, 1, 0), (1, 1, 1), (-1, 0, 1))

    def chip(step):
        return lax.rem(y + step + ny, ny)

    def at_chip(place):
        return (sp, 2 * place + c)

    hw = width // 2
    sent = {}
    for t in range(half_way):
        for n, (way, chunk, skip) in enumerate(chains):
            h = t + skip
            if h >= half_way:
                continue
            at = slice(chunk * hw, (chunk + 1) * hw)
            total = part[chip(way * (half_way - h)), :, at]
            if t > 0:
                sent[n].wait_recv()
                total = total + parr[n, h - 1].astype(F32)
            pbuf[n, h] = total.astype(BF16)
            sent[n] = push(pbuf.at[n, h], parr.at[n, h], p_send.at[n, h], p_recv.at[n, h], at_chip(chip(way)))
    halves = []
    for chunk in range(2):
        total = part[y, :, chunk * hw:(chunk + 1) * hw]
        for n, (way, of, skip) in enumerate(chains):
            if of == chunk:
                sent[n].wait_recv()
                total = total + parr[n, half_way - 1].astype(F32)
        halves.append(total)
    attn = jnp.concatenate(halves, axis=1).astype(BF16).astype(F32)
    steady = layer_norm(stream[...].astype(F32) + attn, gm[...])
    settled[...] = steady
    msend[...] = steady.astype(BF16)

    def lanes_of(k):
        return pl.ds(pl.multiple_of(k * LANES, LANES), LANES)

    def rows_at(k):
        return pl.ds(pl.multiple_of(k * own_rows, own_rows), own_rows)

    def over_tp(base, src_of, dst):
        for k in range(1, ntp):
            to = lax.rem(tp + k, ntp)
            yield push(src_of(to), dst, t_send.at[base, k], t_recv.at[base, k], (sp, to))

    moved = list(over_tp(0, lambda to: msend.at[:, lanes_of(to)], cols.at[rows_at(tp)]))
    cols[rows_at(tp)] = msend[:, lanes_of(tp)]
    slots = iota((nrow, toks), 0)
    named = [slots == places[k] for k in range(2)]
    gather = jnp.where(named[0] | named[1], 1.0, 0.0).astype(BF16)
    for copy in moved:
        copy.wait_recv()
    dsend[...] = mm(gather, cols[...]).astype(BF16).reshape(nrow // 8, 8, LANES)
    arrive = send_sp(2, dsend, darr, cap // 8)

    share = af[0:1] + af[1:2]
    scaled = jnp.where(named[0], af[0:1] / share, 0.0) + jnp.where(named[1], af[1:2] / share, 0.0)
    scaled = scaled.T
    high = scaled.astype(BF16)
    pick_hi[...] = high
    pick_lo[...] = (scaled - high.astype(F32)).astype(BF16)

    arrive()
    rows[tp] = darr[...].reshape(nrow, LANES)

    def half(k):
        return slice(k * hrow, (k + 1) * hrow)

    def slot(place, core):
        return 2 * place + core

    def hand_on(n, h, chunk, place):
        at = rows.at[slot(place, c), half(chunk)]
        return push(at, at, f_send.at[n, h], f_recv.at[n, h], sib)

    def grow_acc(place, core, chunk, fresh=False):
        k = slot(place, core)
        w = wgu[pl.ds(pl.multiple_of(k * LANES, LANES), LANES)]
        more = mm(rows[k, half(chunk)], w)
        acc[half(chunk)] = more if fresh else acc[half(chunk)] + more

    def ring(n, h):
        way, chunk, skip = chains[n]
        at = rows.at[slot(chip(-way * h), c), half(chunk)]
        return push(at, at, g_send.at[n, h], g_recv.at[n, h], at_chip(chip(way)))

    link = {n: ring(n, 0) for n in range(4)}
    passed = [(hand_on(4, chunk, chunk, y), y, chunk) for chunk in range(2)]
    for chunk in range(2):
        grow_acc(y, c, chunk, fresh=True)
    for h in range(half_way):
        fresh = []
        for n, (way, chunk, skip) in enumerate(chains):
            if h >= half_way - skip:
                continue
            link[n].wait_recv()
            if h + 1 < half_way - skip:
                link[n] = ring(n, h + 1)
            place = chip(-way * (h + 1))
            fresh.append((hand_on(n, h, chunk, place), place, chunk))
        for copy, place, chunk in passed:
            copy.wait_recv()
            grow_acc(place, 1 - c, chunk)
        for copy, place, chunk in fresh:
            grow_acc(place, c, chunk)
        passed = fresh
    for copy, place, chunk in passed:
        copy.wait_recv()
        grow_acc(place, 1 - c, chunk)

    swap = []
    for chunk in range(2):
        at = half(chunk)
        act[at] = (jax.nn.silu(acc[at, 0:LANES]) * acc[at, LANES:2 * LANES]).astype(BF16)
        swap.append(push(act.at[at], act_in.at[at], sib_send.at[4 + chunk], sib_recv.at[4 + chunk], sib))
    lend[2].wait_recv()
    for copy in swap:
        copy.wait_recv()

    def own_part(place, chunk):
        at = lanes_of(slot(place, c))
        return mm(act[half(chunk)], own_down[:, at]) + mm(act_in[half(chunk)], other_down[:, at])

    sent = {}
    for t in range(half_way):
        for n, (way, chunk, skip) in enumerate(chains):
            h = t + skip
            if h >= half_way:
                continue
            total = own_part(chip(way * (half_way - h)), chunk)
            if t > 0:
                sent[n].wait_recv()
                total = total + rarr[n, h - 1].astype(F32)
            rbuf[n, h] = total.astype(BF16)
            sent[n] = push(rbuf.at[n, h], rarr.at[n, h], r_send.at[n, h], r_recv.at[n, h], at_chip(chip(way)))
    for chunk in range(2):
        total = own_part(y, chunk)
        for n, (way, of, skip) in enumerate(chains):
            if of == chunk:
                sent[n].wait_recv()
                total = total + rarr[n, half_way - 1].astype(F32)
        rsend[chunk * hrow // 8:(chunk + 1) * hrow // 8] = total.astype(BF16).reshape(hrow // 8, 8, LANES)
    send_sp(3, rsend, rback, cap // 8)()

    back = rback[...].reshape(nrow, LANES)
    term[...] = (mm(pick_hi[...], back) + mm(pick_lo[...], back)).astype(BF16)
    moved = list(over_tp(1, lambda to: term.at[rows_at(to)], mix.at[:, lanes_of(tp)]))
    mix[:, lanes_of(tp)] = term[rows_at(tp)]
    for copy in moved:
        copy.wait_recv()
    out[...] = layer_norm(settled[...] + mix[...].astype(F32), go[...]).astype(BF16)

    for wait in pending:
        wait()
    for copy in remote:
        copy.wait_send()


def layer(nsp, ntp, *args):
    (q1, k1, v1, g1, d1, q2, k2, v2, g2, d2, hg, p1, p2, st, gm, go, rt, af, eg, eu, ed) = args
    toks = q1.shape[0]
    width = st.shape[1]
    own_rows = toks // ntp
    cap = 3 * toks * 2 // (2 * nsp)
    nrow = nsp * cap
    ny = ntp // 2
    steps = ny // 2
    per = LANES // nsp
    mrow = -(-(3 * per + 3) // 16) * 16
    V = pltpu.VMEM
    D = pltpu.SemaphoreType.DMA
    one = (hg.reshape(1, -1), gm.reshape(1, -1), go.reshape(1, -1), rt.T, af.T)
    operands = (q1, k1, v1, g1, d1, q2, k2, v2, g2, d2, one[0], p1, p2, st, one[1], one[2], one[3], one[4], eg, eu, ed)
    scratch = [
        V(q1.shape, BF16), V(k1.shape, BF16), V(v1.shape, BF16), V(g1.shape, BF16), V(d1.shape, F32),
        V(q2.shape, BF16), V(k2.shape, BF16), V(v2.shape, BF16), V(g2.shape, BF16), V(d2.shape, F32),
        V((1, LANES), F32), V((2 * LANES, width), BF16), V((2 * LANES, width), BF16), V((own_rows, width), BF16),
        V((1, width), F32), V((1, width), F32), V((2, toks), jnp.int32), V((2, toks), F32),
        V((width, 2 * LANES), BF16), V((LANES, width), BF16), V((LANES, width), BF16),
        V((nsp, mrow, LANES), BF16), V((nsp, mrow, LANES), BF16), V((nsp, mrow, LANES), F32),
        V((nsp, mrow, LANES), BF16), V((nsp, mrow, LANES), BF16),
        V((3, toks, LANES), BF16), V((3, toks, LANES), BF16), V((3, toks // BLK, LANES, LANES), F32),
        V((2, toks, LANES), F32), V((2, ny, own_rows, 2 * LANES), BF16), V((ny, own_rows, 2 * LANES), BF16),
        V((ny, own_rows, width), F32),
        V((4, steps, own_rows, width // 2), BF16), V((4, steps, own_rows, width // 2), BF16),
        V((own_rows, width), F32), V((own_rows, width), BF16), V((toks, LANES), BF16),
        V((nrow // 8, 8, LANES), BF16), V((nrow // 8, 8, LANES), BF16), V((ntp, nrow, LANES), BF16),
        V((nrow, 2 * LANES), F32), V((nrow, LANES), BF16), V((nrow, LANES), BF16),
        V((4, steps, nrow // 2, LANES), BF16), V((4, steps, nrow // 2, LANES), BF16),
        V((nrow // 8, 8, LANES), BF16), V((nrow // 8, 8, LANES), BF16),
        V((toks, nrow), BF16), V((toks, nrow), BF16), V((toks, LANES), BF16), V((own_rows, width), BF16),
        D((21,)), D((4 * nsp,)), D((4 * nsp,)), D((6,)), D((6,)), D((4, steps)), D((4, steps)), D((2, ntp)), D((2, ntp)),
        D((4, steps)), D((4, steps)), D((5, max(steps, 2))), D((5, max(steps, 2))), D((4, steps)), D((4, steps)),
    ]
    return pl.pallas_call(
        functools.partial(kernel, (nsp, ntp, toks, cap)),
        out_shape=jax.ShapeDtypeStruct((own_rows, width), BF16),
        in_specs=[pl.BlockSpec(memory_space=ANY)] * len(operands),
        out_specs=pl.BlockSpec(memory_space=pltpu.VMEM),
        scratch_shapes=scratch,
        compiler_params=pltpu.CompilerParams(collective_id=0, has_side_effects=True, vmem_limit_bytes=60 * 1024 * 1024),
        name="layer",
    )(*operands)


def solution(mesh):
    spec = P("sp", "tp")
    fade = P(None, "sp", "tp")
    return jax.shard_map(
        functools.partial(layer, mesh.shape["sp"], mesh.shape["tp"]),
        mesh=mesh,
        in_specs=(
            spec, spec, spec, spec, fade, spec, spec, spec, spec, fade,
            P(), P("tp", None), P("tp", None), P("sp", None), P(), P(), P("sp", None), P("sp", None),
            P("sp", None, "tp"), P("sp", None, "tp"), P("sp", "tp", None),
        ),
        out_specs=P(("sp", "tp"), None),
        check_vma=False,
    )
```

```python
import functools

import jax
import jax.numpy as jnp
from jax import lax
from jax.experimental import pallas as pl
from jax.experimental.pallas import tpu as pltpu
from jax.sharding import PartitionSpec as P

MESH = pl.DeviceIdType.MESH
F32 = jnp.float32
BF16 = jnp.bfloat16
BLK = 64
CHUNKS = 4
LANES = 128
ANY = pl.ANY


def mm(a, b):
    return jnp.dot(a, b, preferred_element_type=F32)


def mm_t(a, b):
    return lax.dot_general(a, b, (((1,), (1,)), ((), ())), preferred_element_type=F32)


def tmm(a, b):
    return lax.dot_general(a, b, (((0,), (0,)), ((), ())), preferred_element_type=F32)


def iota(shape, dim):
    return lax.broadcasted_iota(jnp.int32, shape, dim)


def far_first(sizes):
    steps = [()]
    for size in sizes:
        steps = [done + (k,) for done in steps for k in range(size)]
    return sorted(steps, key=lambda d: (-sum(min(k, n - k) for k, n in zip(d, sizes)), d))


def layer_norm(values, gain):
    mean = jnp.mean(values, axis=-1, keepdims=True)
    spread = jnp.mean(jnp.square(values - mean), axis=-1, keepdims=True)
    return (values - mean) * lax.rsqrt(spread + 1e-05) * gain


def kernel(
    cfg,
    q1h, k1h, v1h, g1h, d1h, q2h, k2h, v2h, g2h, d2h, hgh, p1h, p2h, sth, gmh, goh, rth, afh, egh, euh, edh,
    out,
    q1, k1, v1, g1, d1, q2, k2, v2, g2, d2, hg, own_proj, other_proj, stream, gm, go, rt, af, wgu, down,
    sbuf, sarr, fsum, sret, sback,
    qin, kin, grow, mixed, heads, heads_in, part,
    pbuf, parr, settled, msend, cols, dsend, darr, rows, acc, act, rbuf, rarr, rsend, rback,
    pick_hi, pick_lo, term, mix,
    load_sem, s_send, s_recv, sib_send, sib_recv, p_send, p_recv, t_send, t_recv,
    g_send, g_recv, f_send, f_recv, r_send, r_recv,
):
    nsp, nx, ntp, toks, cap = cfg
    nz = nsp // nx
    ny = ntp // 2
    half_way = ny // 2
    sp = lax.axis_index("sp")
    tp = lax.axis_index("tp")
    y = lax.div(tp, 2)
    c = lax.rem(tp, 2)
    sib = (sp, tp + 1 - 2 * c)
    blocks = toks // BLK
    own_rows = toks // ntp
    width = ntp * LANES
    per = LANES // nsp
    mrow = sbuf.shape[1]
    nrow = nsp * cap
    crow = nrow // CHUNKS
    z_at, x_at = lax.div(sp, nx), lax.rem(sp, nx)
    sp_moves = far_first((nz, nx))
    tp_moves = far_first((ny, 2))

    scope = []

    def phase(name):
        if scope:
            scope.pop().__exit__(None, None, None)
        if name:
            scope.append(jax.named_scope(name))
            scope[0].__enter__()

    phase("greet")
    barrier = pltpu.get_barrier_semaphore()

    def greet_sp(k, carry):
        pl.semaphore_signal(barrier, inc=1, device_id=(lax.rem(sp + k, nsp), tp), device_id_type=MESH)
        return carry

    def greet_tp(k, carry):
        pl.semaphore_signal(barrier, inc=1, device_id=(sp, lax.rem(tp + k, ntp)), device_id_type=MESH)
        return carry

    lax.fori_loop(1, nsp, greet_sp, 0)
    lax.fori_loop(1, ntp, greet_tp, 0)

    loads = []

    def load(src, dst):
        copy = pltpu.make_async_copy(src, dst, load_sem.at[len(loads)])
        copy.start()
        loads.append(copy)
        return copy

    first = [load(a, b) for a, b in ((d1h, d1), (d2h, d2), (k1h, k1), (v1h, v1), (k2h, k2), (v2h, v2), (q1h, q1), (q2h, q2))]
    second = [
        load(a, b)
        for a, b in (
            (g1h, g1), (g2h, g2), (hgh, hg), (p1h, own_proj.at[0:LANES]), (p2h, own_proj.at[LANES:2 * LANES]),
            (sth.at[pl.ds(pl.multiple_of(tp * own_rows, own_rows), own_rows)], stream), (gmh, gm), (goh, go),
            (rth, rt), (afh, af),
            (egh.at[0], wgu.at[:, 0:LANES]), (euh.at[0], wgu.at[:, LANES:2 * LANES]), (edh.at[0], down.at[0:LANES]),
        )
    ]

    phase("constants")
    r = iota((toks, toks), 0)
    s = iota((toks, toks), 1)
    tri = jnp.where((r // BLK == s // BLK) & (s <= r), 1.0, 0.0).astype(BF16)
    low = iota((1, LANES), 1) < LANES // 2
    m = iota((nsp * mrow, LANES), 0)
    o, i = m // mrow, m % mrow
    wanted = jnp.where(i < 3 * per, (i // per) * LANES + o * per + i % per, 3 * LANES + i - 3 * per)
    wanted = jnp.where(i < 3 * per + 3, wanted, -1)
    lane = iota((nsp * mrow, LANES), 1)
    pack = [jnp.where(wanted == lane + g * LANES, 1.0, 0.0).astype(BF16) for g in range(3)]
    lane16 = iota((nsp * mrow, 16), 1)
    pack.append(jnp.where(wanted[:, 0:16] == lane16 + 3 * LANES, 1.0, 0.0).astype(BF16))

    phase("load_wait")
    for copy in first:
        copy.wait()
    phase("fading")

    def two(a):
        a = a[...].astype(F32)
        return jnp.concatenate([a, a], axis=0).T

    fading = (d1[...].T, d2[0], d2[1])
    keys = (two(k1), k2[...].astype(F32), k2[...].astype(F32))
    queries = (two(q1) * 64 ** (-0.5), q2[...].astype(F32) * 128 ** (-0.5), q2[...].astype(F32) * 128 ** (-0.5))
    values = (v1[...], v2[...], v2[...])
    totals = []
    for g in range(3):
        x = fading[g]
        logs = (jnp.minimum(x, 0.0) - jnp.log1p(jnp.exp(-jnp.abs(x)))) * (1.0 / 16.0)
        hi = logs.astype(BF16)
        rest = logs - hi.astype(F32)
        mid = rest.astype(BF16)
        lo = (rest - mid.astype(F32)).astype(BF16)
        cum = mm(tri, hi) + mm(tri, mid) + mm(tri, lo)
        rows_of = []
        for b in range(blocks):
            at = slice(b * BLK, (b + 1) * BLK)
            ahead = cum[at]
            tot = ahead[BLK - 1:BLK]
            behind = tot - ahead + logs[at]
            run = ahead if g == 1 else behind if g == 2 else jnp.where(low, ahead, behind)
            qin[g, at] = (queries[g][at] * jnp.exp(run)).astype(BF16)
            kin[g, at] = (keys[g][at] * jnp.exp(-run)).astype(BF16)
            kst = (keys[g][at] * jnp.exp(tot - run)).astype(BF16)
            grow[g, b] = tmm(values[g][at], kst)
            rows_of.append(tot)
        totals.append(rows_of)

    fades = [[jnp.exp(t) for t in row] for row in totals]

    def chained(g, order, start):
        state = start
        seen = {}
        for b in order:
            seen[b] = state
            state = fades[g][b] * state + grow[g, b]
        return seen, state

    phase("chain")
    rise, fall = list(range(blocks)), list(range(blocks - 1, -1, -1))
    zero = jnp.zeros((LANES, LANES), F32)
    ends = [
        jnp.where(low, chained(0, rise, zero)[1], chained(0, fall, zero)[1]),
        chained(1, rise, zero)[1],
        chained(2, fall, zero)[1],
    ]
    sums = [sum(row[1:], row[0]) for row in totals]
    r16 = iota((16, LANES), 0)
    tail = jnp.where(r16 == 0, sums[0], jnp.where(r16 == 1, sums[1], jnp.where(r16 == 2, sums[2], 0.0)))
    packed = mm(pack[3], tail.astype(BF16))
    for g in range(3):
        packed = packed + mm(pack[g], ends[g].astype(BF16))
    sbuf[...] = packed.astype(BF16).reshape(nsp, mrow, LANES)

    phase("barrier")
    pl.semaphore_wait(barrier, nsp - 1 + ntp - 1)

    unsent = []

    def sp_peer(move, way):
        return lax.rem(z_at + way * move[0] + nz, nz) * nx + lax.rem(x_at + way * move[1] + nx, nx)

    def send_sp(base, p, src, dst, way=1):
        copy = pltpu.make_async_remote_copy(
            src, dst, s_send.at[base * nsp + p], s_recv.at[base * nsp + p],
            device_id=(sp_peer(sp_moves[p], way), tp), device_id_type=MESH,
        )
        copy.start()
        unsent.append(copy)
        return copy

    def drain():
        while unsent:
            unsent.pop(0).wait_send()

    def push(src, dst, ssem, rsem, device):
        copy = pltpu.make_async_remote_copy(src, dst, ssem, rsem, device_id=device, device_id_type=MESH)
        copy.start()
        unsent.append(copy)
        return copy

    phase("send_states")
    coming = [send_sp(0, p, sbuf.at[sp_peer(sp_moves[p], 1)], sarr.at[sp]) for p in range(nsp - 1)]
    sarr[sp] = sbuf[sp]
    lend = [
        push(p1h, other_proj.at[0:LANES], sib_send.at[0], sib_recv.at[0], sib),
        push(p2h, other_proj.at[LANES:2 * LANES], sib_send.at[1], sib_recv.at[1], sib),
        push(edh.at[0], down.at[LANES:2 * LANES], sib_send.at[2], sib_recv.at[2], sib),
        push(egh.at[0], wgu.at[:, 2 * LANES:3 * LANES], sib_send.at[4], sib_recv.at[4], sib),
        push(euh.at[0], wgu.at[:, 3 * LANES:4 * LANES], sib_send.at[5], sib_recv.at[5], sib),
    ]

    phase("inner")
    rr, cc = iota((BLK, BLK), 0), iota((BLK, BLK), 1)
    lower, upper = cc <= rr, cc >= rr
    for b in range(blocks):
        at = slice(b * BLK, (b + 1) * BLK)
        q, k = qin[0, at], kin[0, at]
        nil = jnp.zeros_like(q)
        score = jnp.where(lower, mm_t(jnp.where(low, q, nil), k), 0.0) + jnp.where(upper, mm_t(jnp.where(low, nil, q), k), 0.0)
        mixed[0, at] = mm(score.astype(BF16), values[0][at])
        score = jnp.where(lower, mm_t(qin[1, at], kin[1, at]), 0.0) + jnp.where(upper, mm_t(qin[2, at], kin[2, at]), 0.0)
        mixed[1, at] = mm(score.astype(BF16), values[1][at])

    phase("wait_states")
    for copy in coming:
        copy.wait_recv()
    phase("scan")
    row = iota((mrow, LANES), 0)
    in_a, in_b = row < per, row < 2 * per

    def tile_of(j):
        t = sarr[j].astype(F32)
        fade = jnp.where(in_a, t[3 * per:3 * per + 1], jnp.where(in_b, t[3 * per + 1:3 * per + 2], t[3 * per + 2:3 * per + 3]))
        return t, jnp.exp(fade)

    state = jnp.zeros((mrow, LANES), F32)
    for j in range(nsp):
        t, fade = tile_of(j)
        fsum[j] = state
        state = fade * state + t
    forward = (in_a & low) | (in_b & jnp.logical_not(in_a))
    state = jnp.zeros((mrow, LANES), F32)
    for j in range(nsp - 1, -1, -1):
        t, fade = tile_of(j)
        sret[j] = jnp.where(forward, fsum[j], state).astype(BF16)
        state = fade * state + t
    phase("send_back")
    coming = [send_sp(1, p, sret.at[sp_peer(sp_moves[p], 1)], sback.at[sp]) for p in range(nsp - 1)]
    sback[sp] = sret[sp]

    phase("places")
    z = iota((LANES, nsp * mrow), 0)
    m = iota((LANES, nsp * mrow), 1)
    lift = (z // per) * mrow + z % per
    unpack = [jnp.where(m == lift + g * per, 1.0, 0.0).astype(BF16) for g in range(3)]

    for copy in second:
        copy.wait()
    experts = iota((nsp, toks), 0)
    hits = [jnp.where(rt[k:k + 1] == experts, 1.0, 0.0) for k in range(2)]
    before = jnp.where(r < s, 1.0, 0.0).astype(BF16)
    counts = mm((hits[0] + hits[1]).astype(BF16), before)
    places = [
        rt[k:k + 1] * cap + jnp.sum(hits[k] * counts, axis=0, keepdims=True).astype(jnp.int32) for k in range(2)
    ]

    phase("wait_back")
    for copy in coming:
        copy.wait_recv()
    phase("readout")
    back = sback[...].reshape(nsp * mrow, LANES)
    come = [mm(unpack[g], back) for g in range(3)]
    fwd_a, back_a = chained(0, rise, come[0])[0], chained(0, fall, come[0])[0]
    fwd_b, back_b = chained(1, rise, come[1])[0], chained(2, fall, come[2])[0]
    for b in range(blocks):
        at = slice(b * BLK, (b + 1) * BLK)
        one = mixed[0, at] + mm_t(qin[0, at], jnp.where(low, fwd_a[b], back_a[b]).astype(BF16))
        other = mixed[1, at] + mm_t(qin[1, at], fwd_b[b].astype(BF16)) + mm_t(qin[2, at], back_b[b].astype(BF16))
        done = []
        for value, gate in ((one, g1), (other, g2)):
            normed = value * lax.rsqrt(jnp.mean(value * value, axis=-1, keepdims=True) + 1e-06) * hg[...]
            done.append((normed * jax.nn.silu(gate[at].astype(F32))).astype(BF16))
        for n in range(BLK // own_rows):
            d = b * (BLK // own_rows) + n
            for k in range(2):
                heads[d % 2, d // 2, :, k * LANES:(k + 1) * LANES] = done[k][n * own_rows:(n + 1) * own_rows]

    phase("proj")
    shared = push(heads.at[1 - c], heads_in, sib_send.at[3], sib_recv.at[3], sib)
    piece = width // 4
    mine = heads[c].reshape(ny * own_rows, 2 * LANES)
    for n in range(4):
        at = slice(n * piece, (n + 1) * piece)
        part[:, :, at] = mm(mine, own_proj[:, at]).reshape(ny, own_rows, piece)
    for copy in lend[:2]:
        copy.wait_recv()
    shared.wait_recv()
    theirs = heads_in[...].reshape(ny * own_rows, 2 * LANES)
    for n in range(4):
        at = slice(n * piece, (n + 1) * piece)
        part[:, :, at] = part[:, :, at] + mm(theirs, other_proj[:, at]).reshape(ny, own_rows, piece)

    phase("attn_ring")
    chains = [(way, q, (q % 2 == 0) != (way == 1)) for q in range(CHUNKS) for way in (1, -1)]
    chain_no = {(way, q): n for n, (way, q, skip) in enumerate(chains)}

    def chip(step):
        return lax.rem(y + step + ny, ny)

    def at_chip(place):
        return (sp, 2 * place + c)

    wide = width // CHUNKS
    sent = {}
    for t in range(half_way):
        for n, (way, q, skip) in enumerate(chains):
            h = t + skip
            if h >= half_way:
                continue
            total = part[chip(way * (half_way - h)), :, q * wide:(q + 1) * wide]
            if t > 0:
                sent[n].wait_recv()
                total = total + parr[n, h - 1].astype(F32)
            pbuf[n, h] = total.astype(BF16)
            sent[n] = push(pbuf.at[n, h], parr.at[n, h], p_send.at[n, h], p_recv.at[n, h], at_chip(chip(way)))
    quarters = []
    for q in range(CHUNKS):
        total = part[y, :, q * wide:(q + 1) * wide]
        for way in (1, -1):
            n = chain_no[way, q]
            if n in sent:
                sent[n].wait_recv()
                total = total + parr[n, half_way - 1].astype(F32)
        quarters.append(total)
    phase("norm")
    attn = jnp.concatenate(quarters, axis=1).astype(BF16).astype(F32)
    steady = layer_norm(stream[...].astype(F32) + attn, gm[...])
    settled[...] = steady
    msend[...] = steady.astype(BF16)

    phase("rows_over_tp")

    def lanes_of(k):
        return pl.ds(pl.multiple_of(k * LANES, LANES), LANES)

    def rows_at(k):
        return pl.ds(pl.multiple_of(k * own_rows, own_rows), own_rows)

    def over_tp(base, src_of, dst):
        copies = []
        for p, (dy, dc) in enumerate(tp_moves[:-1]):
            to = 2 * chip(dy) + (lax.rem(c + dc, 2))
            copies.append(push(src_of(to), dst, t_send.at[base, p], t_recv.at[base, p], (sp, to)))
        return copies

    moved = over_tp(0, lambda to: msend.at[:, lanes_of(to)], cols.at[rows_at(tp)])
    cols[rows_at(tp)] = msend[:, lanes_of(tp)]
    slots = iota((nrow, toks), 0)
    named = [slots == places[k] for k in range(2)]
    gather = jnp.where(named[0] | named[1], 1.0, 0.0).astype(BF16)
    phase("rows_wait")
    for copy in moved:
        copy.wait_recv()
    phase("dispatch")
    dsend[...] = mm(gather, cols[...]).astype(BF16).reshape(nrow // 8, 8, LANES)
    unit = cap // 8
    rows_of_peer = lambda k: pl.ds(k * unit, unit)
    coming = [
        send_sp(2, p, dsend.at[rows_of_peer(sp_peer(sp_moves[p], 1))], darr.at[p * unit:(p + 1) * unit])
        for p in range(nsp - 1)
    ]
    darr[(nsp - 1) * unit:nsp * unit] = dsend[rows_of_peer(sp)]

    phase("weights")
    drain()
    share = af[0:1] + af[1:2]
    scaled = jnp.where(named[0], af[0:1] / share, 0.0) + jnp.where(named[1], af[1:2] / share, 0.0)
    scaled = scaled.T
    high = scaled.astype(BF16)
    pick_hi[...] = high
    pick_lo[...] = (scaled - high.astype(F32)).astype(BF16)

    phase("dispatch_wait")

    def chunk(q):
        return slice(q * crow, (q + 1) * crow)

    def slot(place, core):
        return 2 * place + core

    def hand_on(n, h, q, place):
        at = rows.at[slot(place, c), chunk(q)]
        return push(at, at, f_send.at[n, h], f_recv.at[n, h], sib)

    def ring(n, h):
        way, q, skip = chains[n]
        at = rows.at[slot(chip(-way * h), c), chunk(q)]
        return push(at, at, g_send.at[n, h], g_recv.at[n, h], at_chip(chip(way)))

    def grow_acc(copy, q, place, fresh=False):
        copy.wait_recv()
        both = jnp.concatenate([rows[slot(place, 0), chunk(q)], rows[slot(place, 1), chunk(q)]], axis=1)
        more = mm(both, wgu[pl.ds(pl.multiple_of(place * 2 * LANES, 2 * LANES), 2 * LANES)])
        acc[chunk(q)] = more if fresh else acc[chunk(q)] + more

    link, passed = {}, []
    peers = nsp // CHUNKS
    for q in range(CHUNKS):
        for p in range(q * nsp // CHUNKS, (q + 1) * nsp // CHUNKS):
            if p < nsp - 1:
                coming[p].wait_recv()
        rows[tp, chunk(q)] = darr[q * crow // 8:(q + 1) * crow // 8].reshape(crow, LANES)
        for way in (1, -1):
            n = chain_no[way, q]
            if half_way - chains[n][2] > 0:
                link[n] = ring(n, 0)
        passed.append((hand_on(len(chains), q, q, y), q, y, True))
    phase("gather_ring")
    for copy in lend[2:]:
        copy.wait_recv()
    for h in range(half_way - 1):
        fresh = []
        for n, (way, q, skip) in enumerate(chains):
            if h >= half_way - skip:
                continue
            link[n].wait_recv()
            if h + 1 < half_way - skip:
                link[n] = ring(n, h + 1)
            place = chip(-way * (h + 1))
            fresh.append((hand_on(n, h, q, place), q, place))
        for item in passed:
            grow_acc(*item)
        passed = fresh
    for item in passed:
        grow_acc(*item)

    def last_piece(q):
        way = 1 if q % 2 == 0 else -1
        n = chain_no[way, q]
        link[n].wait_recv()
        place = chip(half_way)
        return hand_on(n, half_way - 1, q, place), q, place

    def own_part(place, q):
        return mm(act[chunk(q)], down[:, lanes_of(slot(place, c))])

    sent = {}

    def reduce_step(n, t):
        way, q, skip = chains[n]
        h = t + skip
        if h >= half_way:
            return
        total = own_part(chip(way * (half_way - h)), q)
        if t > 0:
            sent[n].wait_recv()
            total = total + rarr[n, h - 1].astype(F32)
        rbuf[n, h] = total.astype(BF16)
        sent[n] = push(rbuf.at[n, h], rarr.at[n, h], r_send.at[n, h], r_recv.at[n, h], at_chip(chip(way)))

    def finish_rows(item):
        grow_acc(*item)
        q = item[1]
        a = acc[chunk(q)]
        for k in range(2):
            gate, up = a[:, 2 * k * LANES:(2 * k + 1) * LANES], a[:, (2 * k + 1) * LANES:(2 * k + 2) * LANES]
            act[chunk(q), k * LANES:(k + 1) * LANES] = (jax.nn.silu(gate) * up).astype(BF16)
        for way in (1, -1):
            reduce_step(chain_no[way, q], 0)

    drain()
    phase("last_pieces")
    waiting = [last_piece(0)]
    for q in range(1, CHUNKS):
        waiting.append(last_piece(q))
        finish_rows(waiting[q - 1])
    finish_rows(waiting[CHUNKS - 1])
    phase("reduce_ring")
    for t in range(1, half_way):
        for n in range(len(chains)):
            reduce_step(n, t)
    coming = []
    for q in range(CHUNKS):
        total = own_part(y, q)
        for way in (1, -1):
            n = chain_no[way, q]
            if n in sent:
                sent[n].wait_recv()
                total = total + rarr[n, half_way - 1].astype(F32)
        rsend[q * crow // 8:(q + 1) * crow // 8] = total.astype(BF16).reshape(crow // 8, 8, LANES)
        for p in range(q * nsp // CHUNKS, (q + 1) * nsp // CHUNKS):
            if p < nsp - 1:
                coming.append(send_sp(3, p, rsend.at[p * unit:(p + 1) * unit], rback.at[rows_of_peer(sp)], -1))
    rback[rows_of_peer(sp)] = rsend[(nsp - 1) * unit:nsp * unit]
    phase("return_wait")
    drain()
    for copy in coming:
        copy.wait_recv()
    phase("combine")

    back = rback[...].reshape(nrow, LANES)
    term[...] = (mm(pick_hi[...], back) + mm(pick_lo[...], back)).astype(BF16)
    phase("mix_over_tp")
    moved = over_tp(1, lambda to: term.at[rows_at(to)], mix.at[:, lanes_of(tp)])
    mix[:, lanes_of(tp)] = term[rows_at(tp)]
    for copy in moved:
        copy.wait_recv()
    phase("last_norm")
    out[...] = layer_norm(settled[...] + mix[...].astype(F32), go[...]).astype(BF16)

    phase("drain")
    drain()
    phase(None)


def layer(nsp, ntp, *args):
    (q1, k1, v1, g1, d1, q2, k2, v2, g2, d2, hg, p1, p2, st, gm, go, rt, af, eg, eu, ed) = args
    toks = q1.shape[0]
    width = st.shape[1]
    own_rows = toks // ntp
    cap = 3 * toks * 2 // (2 * nsp)
    nrow = nsp * cap
    ny = ntp // 2
    steps = ny // 2
    per = LANES // nsp
    mrow = -(-(3 * per + 3) // 16) * 16
    V = pltpu.VMEM
    D = pltpu.SemaphoreType.DMA
    one = (hg.reshape(1, -1), gm.reshape(1, -1), go.reshape(1, -1), rt.T, af.T)
    q1, k1 = q1.T, k1.T
    d1 = d1.transpose(0, 2, 1).reshape(2 * q1.shape[0], toks)
    operands = (q1, k1, v1, g1, d1, q2, k2, v2, g2, d2, one[0], p1, p2, st, one[1], one[2], one[3], one[4], eg, eu, ed)
    scratch = [
        V(q1.shape, BF16), V(k1.shape, BF16), V(v1.shape, BF16), V(g1.shape, BF16), V(d1.shape, F32),
        V(q2.shape, BF16), V(k2.shape, BF16), V(v2.shape, BF16), V(g2.shape, BF16), V(d2.shape, F32),
        V((1, LANES), F32), V((2 * LANES, width), BF16), V((2 * LANES, width), BF16), V((own_rows, width), BF16),
        V((1, width), F32), V((1, width), F32), V((2, toks), jnp.int32), V((2, toks), F32),
        V((width, 4 * LANES), BF16), V((2 * LANES, width), BF16),
        V((nsp, mrow, LANES), BF16), V((nsp, mrow, LANES), BF16), V((nsp, mrow, LANES), F32),
        V((nsp, mrow, LANES), BF16), V((nsp, mrow, LANES), BF16),
        V((3, toks, LANES), BF16), V((3, toks, LANES), BF16), V((3, toks // BLK, LANES, LANES), F32),
        V((2, toks, LANES), F32), V((2, ny, own_rows, 2 * LANES), BF16), V((ny, own_rows, 2 * LANES), BF16),
        V((ny, own_rows, width), F32),
        V((2 * CHUNKS, steps, own_rows, width // CHUNKS), BF16), V((2 * CHUNKS, steps, own_rows, width // CHUNKS), BF16),
        V((own_rows, width), F32), V((own_rows, width), BF16), V((toks, LANES), BF16),
        V((nrow // 8, 8, LANES), BF16), V((nrow // 8, 8, LANES), BF16), V((ntp, nrow, LANES), BF16),
        V((nrow, 4 * LANES), F32), V((nrow, 2 * LANES), BF16),
        V((2 * CHUNKS, steps, nrow // CHUNKS, LANES), BF16), V((2 * CHUNKS, steps, nrow // CHUNKS, LANES), BF16),
        V((nrow // 8, 8, LANES), BF16), V((nrow // 8, 8, LANES), BF16),
        V((toks, nrow), BF16), V((toks, nrow), BF16), V((toks, LANES), BF16), V((own_rows, width), BF16),
        D((21,)), D((4 * nsp,)), D((4 * nsp,)), D((6,)), D((6,)), D((2 * CHUNKS, steps)), D((2 * CHUNKS, steps)),
        D((2, ntp)), D((2, ntp)), D((2 * CHUNKS, steps)), D((2 * CHUNKS, steps)),
        D((2 * CHUNKS + 1, max(steps, CHUNKS))), D((2 * CHUNKS + 1, max(steps, CHUNKS))),
        D((2 * CHUNKS, steps)), D((2 * CHUNKS, steps)),
    ]
    return pl.pallas_call(
        functools.partial(kernel, (nsp, 4 if nsp % 4 == 0 else 1, ntp, toks, cap)),
        out_shape=jax.ShapeDtypeStruct((own_rows, width), BF16),
        in_specs=[pl.BlockSpec(memory_space=ANY)] * len(operands),
        out_specs=pl.BlockSpec(memory_space=pltpu.VMEM),
        scratch_shapes=scratch,
        compiler_params=pltpu.CompilerParams(collective_id=0, has_side_effects=True, vmem_limit_bytes=60 * 1024 * 1024),
        name="layer",
    )(*operands)


def solution(mesh):
    spec = P("sp", "tp")
    fade = P(None, "sp", "tp")
    return jax.shard_map(
        functools.partial(layer, mesh.shape["sp"], mesh.shape["tp"]),
        mesh=mesh,
        in_specs=(
            spec, spec, spec, spec, fade, spec, spec, spec, spec, fade,
            P(), P("tp", None), P("tp", None), P("sp", None), P(), P(), P("sp", None), P("sp", None),
            P("sp", None, "tp"), P("sp", None, "tp"), P("sp", "tp", None),
        ),
        out_specs=P(("sp", "tp"), None),
        check_vma=False,
    )
```

```python
import functools

import jax
import jax.numpy as jnp
from jax import lax
from jax.experimental import pallas as pl
from jax.experimental.pallas import tpu as pltpu
from jax.sharding import PartitionSpec as P

MESH = pl.DeviceIdType.MESH
F32 = jnp.float32
BF16 = jnp.bfloat16
BLK = 64
CHUNKS = 4
LANES = 128
ANY = pl.ANY


def mm(a, b):
    return jnp.dot(a, b, preferred_element_type=F32)


def mm_t(a, b):
    return lax.dot_general(a, b, (((1,), (1,)), ((), ())), preferred_element_type=F32)


def tmm(a, b):
    return lax.dot_general(a, b, (((0,), (0,)), ((), ())), preferred_element_type=F32)


def iota(shape, dim):
    return lax.broadcasted_iota(jnp.int32, shape, dim)


def far_first(sizes):
    steps = [()]
    for size in sizes:
        steps = [done + (k,) for done in steps for k in range(size)]
    return sorted(steps, key=lambda d: (-sum(min(k, n - k) for k, n in zip(d, sizes)), d))


def layer_norm(values, gain):
    mean = jnp.mean(values, axis=-1, keepdims=True)
    spread = jnp.mean(jnp.square(values - mean), axis=-1, keepdims=True)
    return (values - mean) * lax.rsqrt(spread + 1e-05) * gain


def kernel(
    cfg,
    q1h, k1h, v1h, g1h, d1h, q2h, k2h, v2h, g2h, d2h, hgh, p1h, p2h, sth, gmh, goh, rth, afh, egh, euh, edh,
    out,
    qk1, wide_in, gates, d1, d2, hg, own_proj, other_proj, stream, gains, rt, af, wgu, down,
    sbuf, sarr, fsum, sret, sback,
    qin, kin, grow, mixed, heads, heads_in, part,
    pbuf, parr, settled, msend, cols, dsend, darr, rows, acc, act, rbuf, rarr, rsend, rback,
    pick_hi, pick_lo, term, mix,
    sems,
):
    nsp, nx, ntp, toks, cap = cfg
    nz = nsp // nx
    ny = ntp // 2
    half_way = ny // 2
    sp = lax.axis_index("sp")
    tp = lax.axis_index("tp")
    y = lax.div(tp, 2)
    c = lax.rem(tp, 2)
    sib = (sp, tp + 1 - 2 * c)
    blocks = toks // BLK
    own_rows = toks // ntp
    width = ntp * LANES
    per = LANES // nsp
    mrow = sbuf.shape[1]
    nrow = nsp * cap
    crow = nrow // CHUNKS
    z_at, x_at = lax.div(sp, nx), lax.rem(sp, nx)
    sp_moves = far_first((nz, nx))
    tp_moves = far_first((ny, 2))

    def sp_peer(move, way):
        return lax.rem(z_at + way * move[0] + nz, nz) * nx + lax.rem(x_at + way * move[1] + nx, nx)

    def chip(step):
        return lax.rem(y + step + ny, ny)

    def tp_peer(move):
        return 2 * chip(move[0]) + lax.rem(c + move[1], 2)

    scope = []

    def phase(name):
        if scope:
            scope.pop().__exit__(None, None, None)
        if name:
            scope.append(jax.named_scope(name))
            scope[0].__enter__()

    numbers = iter(range(sems.shape[0]))

    def new_sem():
        return sems.at[next(numbers)]

    def await_bytes(ref, sem):
        pltpu.make_async_copy(ref, ref, sem).wait()

    def load(*pairs):
        sem = new_sem()
        for src, dst in pairs:
            pltpu.make_async_copy(src, dst, sem).start()
        return sem

    phase("greet")
    first = [
        (d1, load((d1h, d1))), (d2, load((d2h, d2))),
        (wide_in, load((k2h, wide_in.at[0]), (v1h, wide_in.at[1]), (v2h, wide_in.at[2]), (q2h, wide_in.at[3]))),
        (qk1, load((q1h, qk1.at[0]), (k1h, qk1.at[1]))),
    ]
    barrier = pltpu.get_barrier_semaphore()
    for move in sp_moves[:-1]:
        pl.semaphore_signal(barrier, inc=1, device_id=(sp_peer(move, 1), tp), device_id_type=MESH)
    for move in tp_moves[:-1]:
        pl.semaphore_signal(barrier, inc=1, device_id=(sp, tp_peer(move)), device_id_type=MESH)
    own_stream = sth.at[pl.ds(pl.multiple_of(tp * own_rows, own_rows), own_rows)]
    second = [
        (gates, load((g1h, gates.at[0]), (g2h, gates.at[1]))), (hg, load((hgh, hg))),
        (own_proj, load((p1h, own_proj.at[0:LANES]), (p2h, own_proj.at[LANES:2 * LANES]))),
        (stream, load((own_stream, stream))), (gains, load((gmh, gains.at[0:1]), (goh, gains.at[1:2]))),
        (rt, load((rth, rt))), (af, load((afh, af))),
        (wgu.at[:, 0:2 * LANES], load((egh.at[0], wgu.at[:, 0:LANES]), (euh.at[0], wgu.at[:, LANES:2 * LANES]))),
        (down.at[0:LANES], load((edh.at[0], down.at[0:LANES]))),
    ]

    phase("constants")
    r = iota((toks, toks), 0)
    s = iota((toks, toks), 1)
    tri = jnp.where((r // BLK == s // BLK) & (s <= r), 1.0, 0.0).astype(BF16)
    low = iota((1, LANES), 1) < LANES // 2
    m = iota((nsp * mrow, LANES), 0)
    o, i = m // mrow, m % mrow
    wanted = jnp.where(i < 3 * per, (i // per) * LANES + o * per + i % per, 3 * LANES + i - 3 * per)
    wanted = jnp.where(i < 3 * per + 3, wanted, -1)
    lane = iota((nsp * mrow, LANES), 1)
    pack = [jnp.where(wanted == lane + g * LANES, 1.0, 0.0).astype(BF16) for g in range(3)]
    lane16 = iota((nsp * mrow, 16), 1)
    pack.append(jnp.where(wanted[:, 0:16] == lane16 + 3 * LANES, 1.0, 0.0).astype(BF16))

    phase("load_wait")
    for item in first:
        await_bytes(*item)
    phase("fading")

    def two(a):
        a = a.astype(F32)
        return jnp.concatenate([a, a], axis=0).T

    fading = (d1[...].T, d2[0], d2[1])
    keys = (two(qk1[1]), wide_in[0].astype(F32), wide_in[0].astype(F32))
    queries = (two(qk1[0]) * 64 ** (-0.5), wide_in[3].astype(F32) * 128 ** (-0.5), wide_in[3].astype(F32) * 128 ** (-0.5))
    values = (wide_in[1], wide_in[2], wide_in[2])
    totals = []
    for g in range(3):
        x = fading[g]
        logs = (jnp.minimum(x, 0.0) - jnp.log1p(jnp.exp(-jnp.abs(x)))) * (1.0 / 16.0)
        hi = logs.astype(BF16)
        rest = logs - hi.astype(F32)
        mid = rest.astype(BF16)
        lo = (rest - mid.astype(F32)).astype(BF16)
        cum = mm(tri, hi) + mm(tri, mid) + mm(tri, lo)
        rows_of = []
        for b in range(blocks):
            at = slice(b * BLK, (b + 1) * BLK)
            ahead = cum[at]
            tot = ahead[BLK - 1:BLK]
            behind = tot - ahead + logs[at]
            run = ahead if g == 1 else behind if g == 2 else jnp.where(low, ahead, behind)
            qin[g, at] = (queries[g][at] * jnp.exp(run)).astype(BF16)
            kin[g, at] = (keys[g][at] * jnp.exp(-run)).astype(BF16)
            kst = (keys[g][at] * jnp.exp(tot - run)).astype(BF16)
            grow[g, b] = tmm(values[g][at], kst)
            rows_of.append(tot)
        totals.append(rows_of)

    fades = [[jnp.exp(t) for t in row] for row in totals]

    def chained(g, order, start):
        state = start
        seen = {}
        for b in order:
            seen[b] = state
            state = fades[g][b] * state + grow[g, b]
        return seen, state

    phase("chain")
    rise, fall = list(range(blocks)), list(range(blocks - 1, -1, -1))
    zero = jnp.zeros((LANES, LANES), F32)
    ends = [
        jnp.where(low, chained(0, rise, zero)[1], chained(0, fall, zero)[1]),
        chained(1, rise, zero)[1],
        chained(2, fall, zero)[1],
    ]
    sums = [sum(row[1:], row[0]) for row in totals]
    r16 = iota((16, LANES), 0)
    tail = jnp.where(r16 == 0, sums[0], jnp.where(r16 == 1, sums[1], jnp.where(r16 == 2, sums[2], 0.0)))
    packed = mm(pack[3], tail.astype(BF16))
    for g in range(3):
        packed = packed + mm(pack[g], ends[g].astype(BF16))
    sbuf[...] = packed.astype(BF16).reshape(nsp, mrow, LANES)

    phase("barrier")
    pl.semaphore_wait(barrier, nsp - 1 + ntp - 1)

    left = []

    def push(src, dst, ssem, rsem, device):
        pltpu.make_async_remote_copy(src, dst, ssem, rsem, device_id=device, device_id_type=MESH).start()

    def lend(size, *pairs):
        ssem, rsem = new_sem(), new_sem()
        for src, dst in pairs:
            push(src, dst, ssem, rsem, sib)
        left.append((size, ssem))
        return size, rsem

    def drain():
        while left:
            await_bytes(*left.pop(0))

    def to_sp(p, way=1):
        return (sp_peer(sp_moves[p], way), tp)

    phase("send_states")
    def over_sp(src, dst):
        ssem, rsem = new_sem(), new_sem()
        for p in range(nsp - 1):
            to = to_sp(p)
            push(src.at[to[0]], dst.at[sp], ssem, rsem, to)
        left.append((src.at[0:nsp - 1], ssem))
        dst[sp] = src[sp]
        return dst.at[0:nsp - 1], rsem

    coming = over_sp(sbuf, sarr)
    lent_proj = lend(other_proj, (p1h, other_proj.at[0:LANES]), (p2h, other_proj.at[LANES:2 * LANES]))
    lent_wgu = lend(
        wgu.at[:, 2 * LANES:4 * LANES], (egh.at[0], wgu.at[:, 2 * LANES:3 * LANES]), (euh.at[0], wgu.at[:, 3 * LANES:4 * LANES])
    )
    lent_down = lend(down.at[LANES:2 * LANES], (edh.at[0], down.at[LANES:2 * LANES]))

    phase("inner")
    rr, cc = iota((BLK, BLK), 0), iota((BLK, BLK), 1)
    lower, upper = cc <= rr, cc >= rr
    for b in range(blocks):
        at = slice(b * BLK, (b + 1) * BLK)
        q, k = qin[0, at], kin[0, at]
        nil = jnp.zeros_like(q)
        score = jnp.where(lower, mm_t(jnp.where(low, q, nil), k), 0.0) + jnp.where(upper, mm_t(jnp.where(low, nil, q), k), 0.0)
        mixed[0, at] = mm(score.astype(BF16), values[0][at])
        score = jnp.where(lower, mm_t(qin[1, at], kin[1, at]), 0.0) + jnp.where(upper, mm_t(qin[2, at], kin[2, at]), 0.0)
        mixed[1, at] = mm(score.astype(BF16), values[1][at])

    phase("wait_states")
    await_bytes(*coming)
    phase("scan")
    row = iota((mrow, LANES), 0)
    in_a, in_b = row < per, row < 2 * per

    def tile_of(j):
        t = sarr[j].astype(F32)
        fade = jnp.where(in_a, t[3 * per:3 * per + 1], jnp.where(in_b, t[3 * per + 1:3 * per + 2], t[3 * per + 2:3 * per + 3]))
        return t, jnp.exp(fade)

    state = jnp.zeros((mrow, LANES), F32)
    for j in range(nsp):
        t, fade = tile_of(j)
        fsum[j] = state
        state = fade * state + t
    forward = (in_a & low) | (in_b & jnp.logical_not(in_a))
    state = jnp.zeros((mrow, LANES), F32)
    for j in range(nsp - 1, -1, -1):
        t, fade = tile_of(j)
        sret[j] = jnp.where(forward, fsum[j], state).astype(BF16)
        state = fade * state + t
    phase("send_back")
    coming = over_sp(sret, sback)

    phase("places")
    z = iota((LANES, nsp * mrow), 0)
    m = iota((LANES, nsp * mrow), 1)
    lift = (z // per) * mrow + z % per
    unpack = [jnp.where(m == lift + g * per, 1.0, 0.0).astype(BF16) for g in range(3)]

    for item in second:
        await_bytes(*item)
    experts = iota((nsp, toks), 0)
    hits = [jnp.where(rt[k:k + 1] == experts, 1.0, 0.0) for k in range(2)]
    before = jnp.where(r < s, 1.0, 0.0).astype(BF16)
    counts = mm((hits[0] + hits[1]).astype(BF16), before)
    places = [
        rt[k:k + 1] * cap + jnp.sum(hits[k] * counts, axis=0, keepdims=True).astype(jnp.int32) for k in range(2)
    ]

    phase("wait_back")
    await_bytes(*coming)
    phase("readout")
    back = sback[...].reshape(nsp * mrow, LANES)
    come = [mm(unpack[g], back) for g in range(3)]
    fwd_a, back_a = chained(0, rise, come[0])[0], chained(0, fall, come[0])[0]
    fwd_b, back_b = chained(1, rise, come[1])[0], chained(2, fall, come[2])[0]
    for b in range(blocks):
        at = slice(b * BLK, (b + 1) * BLK)
        one = mixed[0, at] + mm_t(qin[0, at], jnp.where(low, fwd_a[b], back_a[b]).astype(BF16))
        other = mixed[1, at] + mm_t(qin[1, at], fwd_b[b].astype(BF16)) + mm_t(qin[2, at], back_b[b].astype(BF16))
        done = []
        for value, gate in ((one, gates.at[0]), (other, gates.at[1])):
            normed = value * lax.rsqrt(jnp.mean(value * value, axis=-1, keepdims=True) + 1e-06) * hg[...]
            done.append((normed * jax.nn.silu(gate[at].astype(F32))).astype(BF16))
        for n in range(BLK // own_rows):
            d = b * (BLK // own_rows) + n
            for k in range(2):
                heads[d % 2, d // 2, :, k * LANES:(k + 1) * LANES] = done[k][n * own_rows:(n + 1) * own_rows]

    phase("proj")
    shared = lend(heads_in, (heads.at[1 - c], heads_in))
    piece = width // 4
    mine = heads[c].reshape(ny * own_rows, 2 * LANES)
    for n in range(4):
        at = slice(n * piece, (n + 1) * piece)
        part[:, :, at] = mm(mine, own_proj[:, at]).reshape(ny, own_rows, piece)
    await_bytes(*lent_proj)
    await_bytes(*shared)
    theirs = heads_in[...].reshape(ny * own_rows, 2 * LANES)
    for n in range(4):
        at = slice(n * piece, (n + 1) * piece)
        part[:, :, at] = part[:, :, at] + mm(theirs, other_proj[:, at]).reshape(ny, own_rows, piece)

    phase("attn_ring")
    chains = [(way, q, (q % 2 == 0) != (way == 1)) for q in range(CHUNKS) for way in (1, -1)]
    chain_no = {(way, q): n for n, (way, q, skip) in enumerate(chains)}

    def at_chip(place):
        return (sp, 2 * place + c)

    wide = width // CHUNKS
    sent, pieces, all_sent = {}, 0, new_sem()
    for t in range(half_way):
        for n, (way, q, skip) in enumerate(chains):
            h = t + skip
            if h >= half_way:
                continue
            total = part[chip(way * (half_way - h)), :, q * wide:(q + 1) * wide]
            if t > 0:
                await_bytes(parr.at[n, h - 1], sent[n])
                total = total + parr[n, h - 1].astype(F32)
            pbuf[n, h] = total.astype(BF16)
            sent[n] = new_sem()
            push(pbuf.at[n, h], parr.at[n, h], all_sent, sent[n], at_chip(chip(way)))
            pieces += 1
    quarters = []
    for q in range(CHUNKS):
        total = part[y, :, q * wide:(q + 1) * wide]
        for way in (1, -1):
            n = chain_no[way, q]
            if n in sent:
                await_bytes(parr.at[n, half_way - 1], sent[n])
                total = total + parr[n, half_way - 1].astype(F32)
        quarters.append(total)
    left.append((pbuf.at[0:pieces // half_way], all_sent))
    phase("norm")
    attn = jnp.concatenate(quarters, axis=1).astype(BF16).astype(F32)
    steady = layer_norm(stream[...].astype(F32) + attn, gains[0:1])
    settled[...] = steady
    msend[...] = steady.astype(BF16)

    phase("rows_over_tp")

    def lanes_of(k):
        return pl.ds(pl.multiple_of(k * LANES, LANES), LANES)

    def rows_at(k):
        return pl.ds(pl.multiple_of(k * own_rows, own_rows), own_rows)

    def over_tp(src_of, dst):
        ssem, rsem = new_sem(), new_sem()
        for move in tp_moves[:-1]:
            to = tp_peer(move)
            push(src_of(to), dst, ssem, rsem, (sp, to))
        size = cols.at[0:(ntp - 1) * own_rows]
        left.append((size, ssem))
        return size, rsem

    moved = over_tp(lambda to: msend.at[:, lanes_of(to)], cols.at[rows_at(tp)])
    cols[rows_at(tp)] = msend[:, lanes_of(tp)]
    slots = iota((nrow, toks), 0)
    named = [slots == places[k] for k in range(2)]
    gather = jnp.where(named[0] | named[1], 1.0, 0.0).astype(BF16)
    phase("rows_wait")
    await_bytes(*moved)
    phase("dispatch")
    dsend[...] = mm(gather, cols[...]).astype(BF16).reshape(nrow // 8, 8, LANES)
    unit = cap // 8
    rows_of_peer = lambda k: pl.ds(k * unit, unit)
    all_sent, coming = new_sem(), []
    for q in range(CHUNKS):
        span = range(q * nsp // CHUNKS, min((q + 1) * nsp // CHUNKS, nsp - 1))
        rsem = new_sem()
        for p in span:
            to = to_sp(p)
            push(dsend.at[rows_of_peer(to[0])], darr.at[p * unit:(p + 1) * unit], all_sent, rsem, to)
        coming.append((darr.at[span[0] * unit:(span[-1] + 1) * unit], rsem) if span else None)
    left.append((dsend.at[0:(nsp - 1) * unit], all_sent))
    darr[(nsp - 1) * unit:nsp * unit] = dsend[rows_of_peer(sp)]

    phase("weights")
    drain()
    share = af[0:1] + af[1:2]
    scaled = jnp.where(named[0], af[0:1] / share, 0.0) + jnp.where(named[1], af[1:2] / share, 0.0)
    scaled = scaled.T
    high = scaled.astype(BF16)
    pick_hi[...] = high
    pick_lo[...] = (scaled - high.astype(F32)).astype(BF16)

    phase("dispatch_wait")

    def chunk(q):
        return slice(q * crow, (q + 1) * crow)

    def slot(place, core):
        return 2 * place + core

    ring_sent, hand_sent = new_sem(), new_sem()
    counts_of = [0, 0]

    def hand_on(q, place):
        at = rows.at[slot(place, c), chunk(q)]
        rsem = new_sem()
        push(at, at, hand_sent, rsem, sib)
        counts_of[1] += 1
        return rows.at[slot(place, 1 - c), chunk(q)], rsem

    def ring(n, h):
        way, q, skip = chains[n]
        at = rows.at[slot(chip(-way * h), c), chunk(q)]
        rsem = new_sem()
        push(at, at, ring_sent, rsem, at_chip(chip(way)))
        counts_of[0] += 1
        return rows.at[slot(chip(-way * (h + 1)), c), chunk(q)], rsem

    def grow_acc(copy, q, place, fresh=False):
        await_bytes(*copy)
        both = jnp.concatenate([rows[slot(place, 0), chunk(q)], rows[slot(place, 1), chunk(q)]], axis=1)
        more = mm(both, wgu[pl.ds(pl.multiple_of(place * 2 * LANES, 2 * LANES), 2 * LANES)])
        acc[chunk(q)] = more if fresh else acc[chunk(q)] + more

    link, passed = {}, []
    for q in range(CHUNKS):
        if coming[q]:
            await_bytes(*coming[q])
        rows[tp, chunk(q)] = darr[q * crow // 8:(q + 1) * crow // 8].reshape(crow, LANES)
        for way in (1, -1):
            n = chain_no[way, q]
            if half_way - chains[n][2] > 0:
                link[n] = ring(n, 0)
        passed.append((hand_on(q, y), q, y, True))
    phase("gather_ring")
    await_bytes(*lent_wgu)
    await_bytes(*lent_down)
    for h in range(half_way - 1):
        fresh = []
        for n, (way, q, skip) in enumerate(chains):
            if h >= half_way - skip:
                continue
            await_bytes(*link[n])
            if h + 1 < half_way - skip:
                link[n] = ring(n, h + 1)
            place = chip(-way * (h + 1))
            fresh.append((hand_on(q, place), q, place))
        for item in passed:
            grow_acc(*item)
        passed = fresh
    for item in passed:
        grow_acc(*item)

    def last_piece(q):
        way = 1 if q % 2 == 0 else -1
        n = chain_no[way, q]
        await_bytes(*link[n])
        place = chip(half_way)
        return hand_on(q, place), q, place

    def own_part(place, q):
        return mm(act[chunk(q)], down[:, lanes_of(slot(place, c))])

    sent, reduced, all_sent = {}, [0], new_sem()

    def reduce_step(n, t):
        way, q, skip = chains[n]
        h = t + skip
        if h >= half_way:
            return
        total = own_part(chip(way * (half_way - h)), q)
        if t > 0:
            await_bytes(rarr.at[n, h - 1], sent[n])
            total = total + rarr[n, h - 1].astype(F32)
        rbuf[n, h] = total.astype(BF16)
        sent[n] = new_sem()
        push(rbuf.at[n, h], rarr.at[n, h], all_sent, sent[n], at_chip(chip(way)))
        reduced[0] += 1

    def finish_rows(item):
        grow_acc(*item)
        q = item[1]
        a = acc[chunk(q)]
        for k in range(2):
            gate, up = a[:, 2 * k * LANES:(2 * k + 1) * LANES], a[:, (2 * k + 1) * LANES:(2 * k + 2) * LANES]
            act[chunk(q), k * LANES:(k + 1) * LANES] = (jax.nn.silu(gate) * up).astype(BF16)
        for way in (1, -1):
            reduce_step(chain_no[way, q], 0)

    drain()
    phase("last_pieces")
    waiting = [last_piece(0)]
    for q in range(1, CHUNKS):
        waiting.append(last_piece(q))
        finish_rows(waiting[q - 1])
    finish_rows(waiting[CHUNKS - 1])
    phase("reduce_ring")
    for t in range(1, half_way):
        for n in range(len(chains)):
            reduce_step(n, t)
    left.append((rbuf.at[0:reduced[0] // half_way], all_sent))
    left.append((rows.at[0:counts_of[0] // CHUNKS], ring_sent))
    left.append((rows.at[0:counts_of[1] // CHUNKS], hand_sent))
    all_sent, arrived = new_sem(), new_sem()
    for q in range(CHUNKS):
        total = own_part(y, q)
        for way in (1, -1):
            n = chain_no[way, q]
            if n in sent:
                await_bytes(rarr.at[n, half_way - 1], sent[n])
                total = total + rarr[n, half_way - 1].astype(F32)
        rsend[q * crow // 8:(q + 1) * crow // 8] = total.astype(BF16).reshape(crow // 8, 8, LANES)
        for p in range(q * nsp // CHUNKS, min((q + 1) * nsp // CHUNKS, nsp - 1)):
            push(rsend.at[p * unit:(p + 1) * unit], rback.at[rows_of_peer(sp)], all_sent, arrived, to_sp(p, -1))
    left.append((rsend.at[0:(nsp - 1) * unit], all_sent))
    rback[rows_of_peer(sp)] = rsend[(nsp - 1) * unit:nsp * unit]
    phase("return_wait")
    drain()
    await_bytes(rback.at[0:(nsp - 1) * unit], arrived)
    phase("combine")

    back = rback[...].reshape(nrow, LANES)
    term[...] = (mm(pick_hi[...], back) + mm(pick_lo[...], back)).astype(BF16)
    phase("mix_over_tp")
    moved = over_tp(lambda to: term.at[rows_at(to)], mix.at[:, lanes_of(tp)])
    mix[:, lanes_of(tp)] = term[rows_at(tp)]
    await_bytes(*moved)
    phase("last_norm")
    out[...] = layer_norm(settled[...] + mix[...].astype(F32), gains[1:2]).astype(BF16)

    phase("drain")
    drain()
    phase(None)


def layer(nsp, ntp, *args):
    (q1, k1, v1, g1, d1, q2, k2, v2, g2, d2, hg, p1, p2, st, gm, go, rt, af, eg, eu, ed) = args
    toks = q1.shape[0]
    width = st.shape[1]
    own_rows = toks // ntp
    cap = 3 * toks * 2 // (2 * nsp)
    nrow = nsp * cap
    ny = ntp // 2
    steps = ny // 2
    per = LANES // nsp
    mrow = -(-(3 * per + 3) // 16) * 16
    V = pltpu.VMEM
    D = pltpu.SemaphoreType.DMA
    one = (hg.reshape(1, -1), gm.reshape(1, -1), go.reshape(1, -1), rt.T, af.T)
    q1, k1 = q1.T, k1.T
    d1 = d1.transpose(0, 2, 1).reshape(2 * q1.shape[0], toks)
    operands = (q1, k1, v1, g1, d1, q2, k2, v2, g2, d2, one[0], p1, p2, st, one[1], one[2], one[3], one[4], eg, eu, ed)
    scratch = [
        V((2, *q1.shape), BF16), V((4, *q2.shape), BF16), V((2, *q2.shape), BF16), V(d1.shape, F32), V(d2.shape, F32),
        V((1, LANES), F32), V((2 * LANES, width), BF16), V((2 * LANES, width), BF16), V((own_rows, width), BF16),
        V((2, width), F32), V((2, toks), jnp.int32), V((2, toks), F32),
        V((width, 4 * LANES), BF16), V((2 * LANES, width), BF16),
        V((nsp, mrow, LANES), BF16), V((nsp, mrow, LANES), BF16), V((nsp, mrow, LANES), F32),
        V((nsp, mrow, LANES), BF16), V((nsp, mrow, LANES), BF16),
        V((3, toks, LANES), BF16), V((3, toks, LANES), BF16), V((3, toks // BLK, LANES, LANES), F32),
        V((2, toks, LANES), F32), V((2, ny, own_rows, 2 * LANES), BF16), V((ny, own_rows, 2 * LANES), BF16),
        V((ny, own_rows, width), F32),
        V((2 * CHUNKS, steps, own_rows, width // CHUNKS), BF16), V((2 * CHUNKS, steps, own_rows, width // CHUNKS), BF16),
        V((own_rows, width), F32), V((own_rows, width), BF16), V((toks, LANES), BF16),
        V((nrow // 8, 8, LANES), BF16), V((nrow // 8, 8, LANES), BF16), V((ntp, nrow, LANES), BF16),
        V((nrow, 4 * LANES), F32), V((nrow, 2 * LANES), BF16),
        V((2 * CHUNKS, steps, nrow // CHUNKS, LANES), BF16), V((2 * CHUNKS, steps, nrow // CHUNKS, LANES), BF16),
        V((nrow // 8, 8, LANES), BF16), V((nrow // 8, 8, LANES), BF16),
        V((toks, nrow), BF16), V((toks, nrow), BF16), V((toks, LANES), BF16), V((own_rows, width), BF16),
        D((156,)),
    ]
    return pl.pallas_call(
        functools.partial(kernel, (nsp, 4 if nsp % 4 == 0 else 1, ntp, toks, cap)),
        out_shape=jax.ShapeDtypeStruct((own_rows, width), BF16),
        in_specs=[pl.BlockSpec(memory_space=ANY)] * len(operands),
        out_specs=pl.BlockSpec(memory_space=pltpu.VMEM),
        scratch_shapes=scratch,
        compiler_params=pltpu.CompilerParams(collective_id=0, has_side_effects=True, vmem_limit_bytes=60 * 1024 * 1024),
        name="layer",
    )(*operands)


def solution(mesh):
    spec = P("sp", "tp")
    fade = P(None, "sp", "tp")
    return jax.shard_map(
        functools.partial(layer, mesh.shape["sp"], mesh.shape["tp"]),
        mesh=mesh,
        in_specs=(
            spec, spec, spec, spec, fade, spec, spec, spec, spec, fade,
            P(), P("tp", None), P("tp", None), P("sp", None), P(), P(), P("sp", None), P("sp", None),
            P("sp", None, "tp"), P("sp", None, "tp"), P("sp", "tp", None),
        ),
        out_specs=P(("sp", "tp"), None),
        check_vma=False,
    )
```

```python
import functools

import jax
import jax.numpy as jnp
from jax import lax
from jax.experimental import pallas as pl
from jax.experimental.pallas import tpu as pltpu
from jax.sharding import PartitionSpec as P

MESH = pl.DeviceIdType.MESH
F32 = jnp.float32
BF16 = jnp.bfloat16
BLK = 64
CHUNKS = 4
LANES = 128
ANY = pl.ANY


def mm(a, b):
    return jnp.dot(a, b, preferred_element_type=F32)


def mm_t(a, b):
    return lax.dot_general(a, b, (((1,), (1,)), ((), ())), preferred_element_type=F32)


def tmm(a, b):
    return lax.dot_general(a, b, (((0,), (0,)), ((), ())), preferred_element_type=F32)


def iota(shape, dim):
    return lax.broadcasted_iota(jnp.int32, shape, dim)


def far_first(sizes):
    steps = [()]
    for size in sizes:
        steps = [done + (k,) for done in steps for k in range(size)]
    return sorted(steps, key=lambda d: (-sum(min(k, n - k) for k, n in zip(d, sizes)), d))


def layer_norm(values, gain):
    mean = jnp.mean(values, axis=-1, keepdims=True)
    spread = jnp.mean(jnp.square(values - mean), axis=-1, keepdims=True)
    return (values - mean) * lax.rsqrt(spread + 1e-05) * gain


def kernel(
    cfg,
    q1h, k1h, v1h, g1h, d1h, q2h, k2h, v2h, g2h, d2h, hgh, p1h, p2h, sth, gmh, goh, rth, afh, egh, euh, edh,
    out,
    qk1, wide_in, gates, d1, d2, hg, own_proj, other_proj, stream, gains, rt, af, wgu, down,
    sbuf, sarr, fsum, sret, sback,
    qin, kin, grow, mixed, heads, heads_in, part,
    pbuf, parr, settled, settled_cols, own_stats, stats, chosen, xsend, xarr, tilt, cols, dsend, darr, rows, acc, act, rbuf, rarr, rsend, rback,
    pick_hi, pick_lo, term, mix,
    sems,
):
    nsp, nx, ntp, toks, cap = cfg
    nz = nsp // nx
    ny = ntp // 2
    half_way = ny // 2
    sp = lax.axis_index("sp")
    tp = lax.axis_index("tp")
    y = lax.div(tp, 2)
    c = lax.rem(tp, 2)
    sib = (sp, tp + 1 - 2 * c)
    blocks = toks // BLK
    own_rows = toks // ntp
    width = ntp * LANES
    per = LANES // nsp
    mrow = sbuf.shape[1]
    nrow = nsp * cap
    crow = nrow // CHUNKS
    z_at, x_at = lax.div(sp, nx), lax.rem(sp, nx)
    sp_moves = far_first((nz, nx))
    tp_moves = far_first((ny, 2))

    def sp_peer(move, way):
        return lax.rem(z_at + way * move[0] + nz, nz) * nx + lax.rem(x_at + way * move[1] + nx, nx)

    def chip(step):
        return lax.rem(y + step + ny, ny)

    def tp_peer(move):
        return 2 * chip(move[0]) + lax.rem(c + move[1], 2)

    scope = []

    def phase(name):
        if scope:
            scope.pop().__exit__(None, None, None)
        if name:
            scope.append(jax.named_scope(name))
            scope[0].__enter__()

    numbers = iter(range(sems.shape[0]))

    def new_sem():
        return sems.at[next(numbers)]

    def await_bytes(ref, sem):
        pltpu.make_async_copy(ref, ref, sem).wait()

    def load(*pairs):
        sem = new_sem()
        for src, dst in pairs:
            pltpu.make_async_copy(src, dst, sem).start()
        return sem

    phase("greet")
    first = [
        (d1, load((d1h, d1))), (d2, load((d2h, d2))),
        (wide_in, load((k2h, wide_in.at[0]), (v1h, wide_in.at[1]), (v2h, wide_in.at[2]), (q2h, wide_in.at[3]))),
        (qk1, load((q1h, qk1.at[0]), (k1h, qk1.at[1]))),
    ]
    barrier = pltpu.get_barrier_semaphore()
    for move in sp_moves[:-1]:
        pl.semaphore_signal(barrier, inc=1, device_id=(sp_peer(move, 1), tp), device_id_type=MESH)
    for move in tp_moves[:-1]:
        pl.semaphore_signal(barrier, inc=1, device_id=(sp, tp_peer(move)), device_id_type=MESH)
    own_stream = sth.at[:, pl.ds(pl.multiple_of(tp * LANES, LANES), LANES)]
    second = [
        (gates, load((g1h, gates.at[0]), (g2h, gates.at[1]))), (hg, load((hgh, hg))),
        (own_proj, load((p1h, own_proj.at[0:LANES]), (p2h, own_proj.at[LANES:2 * LANES]))),
        (stream, load((own_stream, stream))), (gains, load((gmh, gains.at[0:1]), (goh, gains.at[1:2]))),
        (rt, load((rth, rt))), (af, load((afh, af))),
        (wgu.at[:, 0:2 * LANES], load((egh.at[0], wgu.at[:, 0:LANES]), (euh.at[0], wgu.at[:, LANES:2 * LANES]))),
        (down.at[0:LANES], load((edh.at[0], down.at[0:LANES]))),
    ]

    phase("constants")
    r = iota((toks, toks), 0)
    s = iota((toks, toks), 1)
    tri = jnp.where((r // BLK == s // BLK) & (s <= r), 1.0, 0.0).astype(BF16)
    low = iota((1, LANES), 1) < LANES // 2
    m = iota((nsp * mrow, LANES), 0)
    o, i = m // mrow, m % mrow
    wanted = jnp.where(i < 3 * per, (i // per) * LANES + o * per + i % per, 3 * LANES + i - 3 * per)
    wanted = jnp.where(i < 3 * per + 3, wanted, -1)
    lane = iota((nsp * mrow, LANES), 1)
    pack = [jnp.where(wanted == lane + g * LANES, 1.0, 0.0).astype(BF16) for g in range(3)]
    lane16 = iota((nsp * mrow, 16), 1)
    pack.append(jnp.where(wanted[:, 0:16] == lane16 + 3 * LANES, 1.0, 0.0).astype(BF16))

    phase("load_wait")
    for item in first:
        await_bytes(*item)
    phase("fading")

    def two(a):
        a = a.astype(F32)
        return jnp.concatenate([a, a], axis=0).T

    fading = (d1[...].T, d2[0], d2[1])
    keys = (two(qk1[1]), wide_in[0].astype(F32), wide_in[0].astype(F32))
    queries = (two(qk1[0]) * 64 ** (-0.5), wide_in[3].astype(F32) * 128 ** (-0.5), wide_in[3].astype(F32) * 128 ** (-0.5))
    values = (wide_in[1], wide_in[2], wide_in[2])
    totals = []
    for g in range(3):
        x = fading[g]
        logs = (jnp.minimum(x, 0.0) - jnp.log1p(jnp.exp(-jnp.abs(x)))) * (1.0 / 16.0)
        hi = logs.astype(BF16)
        rest = logs - hi.astype(F32)
        mid = rest.astype(BF16)
        lo = (rest - mid.astype(F32)).astype(BF16)
        cum = mm(tri, hi) + mm(tri, mid) + mm(tri, lo)
        rows_of = []
        for b in range(blocks):
            at = slice(b * BLK, (b + 1) * BLK)
            ahead = cum[at]
            tot = ahead[BLK - 1:BLK]
            behind = tot - ahead + logs[at]
            run = ahead if g == 1 else behind if g == 2 else jnp.where(low, ahead, behind)
            qin[g, at] = (queries[g][at] * jnp.exp(run)).astype(BF16)
            kin[g, at] = (keys[g][at] * jnp.exp(-run)).astype(BF16)
            kst = (keys[g][at] * jnp.exp(tot - run)).astype(BF16)
            grow[g, b] = tmm(values[g][at], kst)
            rows_of.append(tot)
        totals.append(rows_of)

    fades = [[jnp.exp(t) for t in row] for row in totals]

    def chained(g, order, start):
        state = start
        seen = {}
        for b in order:
            seen[b] = state
            state = fades[g][b] * state + grow[g, b]
        return seen, state

    phase("chain")
    rise, fall = list(range(blocks)), list(range(blocks - 1, -1, -1))
    zero = jnp.zeros((LANES, LANES), F32)
    ends = [
        jnp.where(low, chained(0, rise, zero)[1], chained(0, fall, zero)[1]),
        chained(1, rise, zero)[1],
        chained(2, fall, zero)[1],
    ]
    sums = [sum(row[1:], row[0]) for row in totals]
    r16 = iota((16, LANES), 0)
    tail = jnp.where(r16 == 0, sums[0], jnp.where(r16 == 1, sums[1], jnp.where(r16 == 2, sums[2], 0.0)))
    packed = mm(pack[3], tail.astype(BF16))
    for g in range(3):
        packed = packed + mm(pack[g], ends[g].astype(BF16))
    sbuf[...] = packed.astype(BF16).reshape(nsp, mrow, LANES)

    phase("barrier")
    pl.semaphore_wait(barrier, nsp - 1 + ntp - 1)

    left = []

    def push(src, dst, ssem, rsem, device):
        pltpu.make_async_remote_copy(src, dst, ssem, rsem, device_id=device, device_id_type=MESH).start()

    def lend(size, *pairs):
        ssem, rsem = new_sem(), new_sem()
        for src, dst in pairs:
            push(src, dst, ssem, rsem, sib)
        left.append((size, ssem))
        return size, rsem

    def drain():
        while left:
            await_bytes(*left.pop(0))

    def to_sp(p, way=1):
        return (sp_peer(sp_moves[p], way), tp)

    phase("send_states")
    def over_sp(src, dst):
        ssem, rsem = new_sem(), new_sem()
        for p in range(nsp - 1):
            to = to_sp(p)
            push(src.at[to[0]], dst.at[sp], ssem, rsem, to)
        left.append((src.at[0:nsp - 1], ssem))
        dst[sp] = src[sp]
        return dst.at[0:nsp - 1], rsem

    coming = over_sp(sbuf, sarr)
    lent_proj = lend(other_proj, (p1h, other_proj.at[0:LANES]), (p2h, other_proj.at[LANES:2 * LANES]))
    lent_wgu = lend(
        wgu.at[:, 2 * LANES:4 * LANES], (egh.at[0], wgu.at[:, 2 * LANES:3 * LANES]), (euh.at[0], wgu.at[:, 3 * LANES:4 * LANES])
    )
    lent_down = lend(down.at[LANES:2 * LANES], (edh.at[0], down.at[LANES:2 * LANES]))

    phase("inner")
    rr, cc = iota((BLK, BLK), 0), iota((BLK, BLK), 1)
    lower, upper = cc <= rr, cc >= rr
    for b in range(blocks):
        at = slice(b * BLK, (b + 1) * BLK)
        q, k = qin[0, at], kin[0, at]
        nil = jnp.zeros_like(q)
        score = jnp.where(lower, mm_t(jnp.where(low, q, nil), k), 0.0) + jnp.where(upper, mm_t(jnp.where(low, nil, q), k), 0.0)
        mixed[0, at] = mm(score.astype(BF16), values[0][at])
        score = jnp.where(lower, mm_t(qin[1, at], kin[1, at]), 0.0) + jnp.where(upper, mm_t(qin[2, at], kin[2, at]), 0.0)
        mixed[1, at] = mm(score.astype(BF16), values[1][at])

    phase("wait_states")
    await_bytes(*coming)
    phase("scan")
    row = iota((mrow, LANES), 0)
    in_a, in_b = row < per, row < 2 * per

    def tile_of(j):
        t = sarr[j].astype(F32)
        fade = jnp.where(in_a, t[3 * per:3 * per + 1], jnp.where(in_b, t[3 * per + 1:3 * per + 2], t[3 * per + 2:3 * per + 3]))
        return t, jnp.exp(fade)

    state = jnp.zeros((mrow, LANES), F32)
    for j in range(nsp):
        t, fade = tile_of(j)
        fsum[j] = state
        state = fade * state + t
    forward = (in_a & low) | (in_b & jnp.logical_not(in_a))
    state = jnp.zeros((mrow, LANES), F32)
    for j in range(nsp - 1, -1, -1):
        t, fade = tile_of(j)
        sret[j] = jnp.where(forward, fsum[j], state).astype(BF16)
        state = fade * state + t
    phase("send_back")
    coming = over_sp(sret, sback)

    phase("places")
    z = iota((LANES, nsp * mrow), 0)
    m = iota((LANES, nsp * mrow), 1)
    lift = (z // per) * mrow + z % per
    unpack = [jnp.where(m == lift + g * per, 1.0, 0.0).astype(BF16) for g in range(3)]

    for item in second:
        await_bytes(*item)
    experts = iota((nsp, toks), 0)
    hits = [jnp.where(rt[k:k + 1] == experts, 1.0, 0.0) for k in range(2)]
    before = jnp.where(r < s, 1.0, 0.0).astype(BF16)
    counts = mm((hits[0] + hits[1]).astype(BF16), before)
    places = [
        rt[k:k + 1] * cap + jnp.sum(hits[k] * counts, axis=0, keepdims=True).astype(jnp.int32) for k in range(2)
    ]

    phase("wait_back")
    await_bytes(*coming)
    phase("readout")
    back = sback[...].reshape(nsp * mrow, LANES)
    come = [mm(unpack[g], back) for g in range(3)]
    fwd_a, back_a = chained(0, rise, come[0])[0], chained(0, fall, come[0])[0]
    fwd_b, back_b = chained(1, rise, come[1])[0], chained(2, fall, come[2])[0]
    for b in range(blocks):
        at = slice(b * BLK, (b + 1) * BLK)
        one = mixed[0, at] + mm_t(qin[0, at], jnp.where(low, fwd_a[b], back_a[b]).astype(BF16))
        other = mixed[1, at] + mm_t(qin[1, at], fwd_b[b].astype(BF16)) + mm_t(qin[2, at], back_b[b].astype(BF16))
        done = []
        for value, gate in ((one, gates.at[0]), (other, gates.at[1])):
            normed = value * lax.rsqrt(jnp.mean(value * value, axis=-1, keepdims=True) + 1e-06) * hg[...]
            done.append((normed * jax.nn.silu(gate[at].astype(F32))).astype(BF16))
        for k in range(2):
            heads[at, k * LANES:(k + 1) * LANES] = done[k]

    phase("proj")
    shared = lend(heads_in, (heads, heads_in))

    def lanes_of(k):
        return pl.ds(pl.multiple_of(k * LANES, LANES), LANES)

    def rows_at(k):
        return pl.ds(pl.multiple_of(k * own_rows, own_rows), own_rows)

    def slot(place, core):
        return 2 * place + core

    for d in range(ny):
        part[d] = mm(heads[...], own_proj[:, lanes_of(slot(d, c))])
    await_bytes(*lent_proj)
    await_bytes(*shared)
    for d in range(ny):
        part[d] = part[d] + mm(heads_in[...], other_proj[:, lanes_of(slot(d, c))])

    phase("attn_ring")
    chains = [(way, q, (q % 2 == 0) != (way == 1)) for q in range(CHUNKS) for way in (1, -1)]
    chain_no = {(way, q): n for n, (way, q, skip) in enumerate(chains)}

    def at_chip(place):
        return (sp, 2 * place + c)

    tall = toks // CHUNKS
    pieces, all_sent = [0], new_sem()

    def span(q):
        return slice(q * tall, (q + 1) * tall)

    def toward(n, kind, total, hops):
        way = chains[n][0]
        sem = new_sem()
        pbuf[n, kind] = total.astype(BF16)
        push(pbuf.at[n, kind], parr.at[n, kind], all_sent, sem, at_chip(chip(way * hops)))
        pieces[0] += 1
        return parr.at[n, kind], sem

    def added(total, item):
        await_bytes(*item)
        return total + item[0][...].astype(F32)

    third, fourth, near, merged = {}, {}, {}, {}
    for n, (way, q, skip) in enumerate(chains):
        third[n] = toward(n, 0, part[chip(3 * way), span(q)], 1)
        if not skip:
            fourth[n] = toward(n, 1, part[chip(4 * way), span(q)], 2)
    for n, (way, q, skip) in enumerate(chains):
        near[n] = toward(n, 2, part[chip(way), span(q)], 1)
    for n, (way, q, skip) in enumerate(chains):
        total = added(part[chip(2 * way), span(q)], third[n])
        if not skip:
            total = added(total, fourth[n])
        merged[n] = toward(n, 3, total, 2)
    own_gain = gains[0:1, lanes_of(tp)]
    for q in range(CHUNKS):
        total = part[y, span(q)]
        for items in (near, merged):
            for way in (1, -1):
                total = added(total, items[chain_no[way, q]])
        summed = stream[span(q)].astype(F32) + total.astype(BF16).astype(F32)
        settled_cols[span(q)] = summed
        cols[span(q)] = ((summed - jnp.mean(summed, axis=-1, keepdims=True)) * own_gain).astype(BF16)
    left.append((pbuf.at[0:pieces[0] // 4], all_sent))
    phase("dispatch")

    def over_tp(src_of, dst, size):
        ssem, rsem = new_sem(), new_sem()
        for move in tp_moves[:-1]:
            to = tp_peer(move)
            push(src_of(to), dst, ssem, rsem, (sp, to))
        left.append((size, ssem))
        return size, rsem

    slots = iota((nrow, toks), 0)
    named = [slots == places[k] for k in range(2)]
    gather = jnp.where(named[0] | named[1], 1.0, 0.0).astype(BF16)
    chosen[...] = gather
    dsend[...] = mm(gather, cols[...]).astype(BF16).reshape(nrow // 8, 8, LANES)
    unit = cap // 8
    rows_of_peer = lambda k: pl.ds(k * unit, unit)

    def to_experts(src, dst):
        all_sent, coming = new_sem(), []
        for q in range(CHUNKS):
            some = range(q * nsp // CHUNKS, min((q + 1) * nsp // CHUNKS, nsp - 1))
            rsem = new_sem()
            for p in some:
                to = to_sp(p)
                push(src.at[rows_of_peer(to[0])], dst.at[p * unit:(p + 1) * unit], all_sent, rsem, to)
            coming.append((dst.at[some[0] * unit:(some[-1] + 1) * unit], rsem) if some else None)
        left.append((src.at[0:(nsp - 1) * unit], all_sent))
        dst[(nsp - 1) * unit:nsp * unit] = src[rows_of_peer(sp)]
        return coming

    coming = to_experts(dsend, darr)
    rowed = over_tp(lambda to: settled_cols.at[rows_at(to)], settled.at[:, lanes_of(tp)], settled_cols.at[0:(ntp - 1) * own_rows])
    settled[:, lanes_of(tp)] = settled_cols[rows_at(tp)]
    phase("weights")
    share = af[0:1] + af[1:2]
    scaled = jnp.where(named[0], af[0:1] / share, 0.0) + jnp.where(named[1], af[1:2] / share, 0.0)
    scaled = scaled.T
    high = scaled.astype(BF16)
    pick_hi[...] = high
    pick_lo[...] = (scaled - high.astype(F32)).astype(BF16)

    phase("stats")
    await_bytes(*rowed)
    whole = settled[...]
    mean = jnp.mean(whole, axis=-1, keepdims=True)
    spread = jnp.mean(jnp.square(whole - mean), axis=-1, keepdims=True)
    rate = lax.rsqrt(spread + 1e-05)
    settled[...] = (whole - mean) * rate * gains[0:1]
    lane = iota((own_rows, LANES), 1)
    offset = jnp.zeros((own_rows, LANES), F32)
    for k in range(ntp):
        shift = jnp.mean(whole[:, k * LANES:(k + 1) * LANES], axis=-1, keepdims=True) - mean
        offset = jnp.where((lane % ntp == k) & (lane < 3 * ntp), shift, offset)
    coarse = offset.astype(BF16).astype(F32)
    offset = jnp.where((lane >= ntp) & (lane < 2 * ntp), offset - coarse, coarse)
    for k in range(3):
        top = rate.astype(BF16).astype(F32)
        offset = jnp.where(lane == 3 * ntp + k, top, offset)
        rate = rate - top
    own_stats[...] = offset.astype(BF16)
    told = over_tp(lambda to: own_stats, stats.at[rows_at(tp)], stats.at[0:(ntp - 1) * own_rows])
    stats[rows_at(tp)] = own_stats[...]
    phase("dispatch_wait")

    def chunk(q):
        return slice(q * crow, (q + 1) * crow)

    ring_sent, hand_sent = new_sem(), new_sem()
    counts_of = [0, 0]

    def hand_on(q, place):
        at = rows.at[slot(place, c), chunk(q)]
        rsem = new_sem()
        push(at, at, hand_sent, rsem, sib)
        counts_of[1] += 1
        return rows.at[slot(place, 1 - c), chunk(q)], rsem

    def ring(n, h):
        way, q, skip = chains[n]
        at = rows.at[slot(chip(-way * h), c), chunk(q)]
        rsem = new_sem()
        push(at, at, ring_sent, rsem, at_chip(chip(way)))
        counts_of[0] += 1
        return rows.at[slot(chip(-way * (h + 1)), c), chunk(q)], rsem

    def grow_acc(copy, q, place, fresh=False):
        await_bytes(*copy)
        both = jnp.concatenate([rows[slot(place, 0), chunk(q)], rows[slot(place, 1), chunk(q)]], axis=1)
        more = mm(both, wgu[pl.ds(pl.multiple_of(place * 2 * LANES, 2 * LANES), 2 * LANES)])
        acc[chunk(q)] = more if fresh else acc[chunk(q)] + more

    link, passed = {}, []
    for q in range(CHUNKS):
        if coming[q]:
            await_bytes(*coming[q])
        rows[tp, chunk(q)] = darr[q * crow // 8:(q + 1) * crow // 8].reshape(crow, LANES)
        for way in (1, -1):
            n = chain_no[way, q]
            if half_way - chains[n][2] > 0:
                link[n] = ring(n, 0)
        passed.append((hand_on(q, y), q, y, True))
    phase("gather_ring")
    await_bytes(*lent_wgu)
    await_bytes(*lent_down)
    for h in range(half_way - 1):
        fresh = []
        for n, (way, q, skip) in enumerate(chains):
            if h >= half_way - skip:
                continue
            await_bytes(*link[n])
            if h + 1 < half_way - skip:
                link[n] = ring(n, h + 1)
            place = chip(-way * (h + 1))
            fresh.append((hand_on(q, place), q, place))
        for item in passed:
            grow_acc(*item)
        passed = fresh
        if h == 0:
            await_bytes(*told)
            xsend[...] = mm(chosen[...], stats[...]).astype(BF16).reshape(nrow // 8, 8, LANES)
            facts = to_experts(xsend, xarr)
            apart = jnp.where(iota((ntp, width), 1) // LANES == iota((ntp, width), 0), gains[0:1], 0.0)
            coarse = apart.astype(BF16)
            fine = (apart - coarse.astype(F32)).astype(BF16)
            slope = mm(coarse, wgu[...]) + mm(fine, wgu[...])
            coarse = slope.astype(BF16)
            fine = (slope - coarse.astype(F32)).astype(BF16)
            tilt[0:ntp], tilt[ntp:2 * ntp], tilt[2 * ntp:3 * ntp] = coarse, coarse, fine
            tilt[3 * ntp:LANES] = jnp.zeros((LANES - 3 * ntp, 4 * LANES), BF16)
    for item in passed:
        grow_acc(*item)
    for item in facts:
        if item:
            await_bytes(*item)

    def last_piece(q):
        way = 1 if q % 2 == 0 else -1
        n = chain_no[way, q]
        await_bytes(*link[n])
        place = chip(half_way)
        return hand_on(q, place), q, place

    def own_part(place, q):
        return mm(act[chunk(q)], down[:, lanes_of(slot(place, c))])

    sent, reduced, all_sent = {}, [0], new_sem()

    def reduce_step(n, t):
        way, q, skip = chains[n]
        h = t + skip
        if h >= half_way:
            return
        total = own_part(chip(way * (half_way - h)), q)
        if t > 0:
            await_bytes(rarr.at[n, h - 1], sent[n])
            total = total + rarr[n, h - 1].astype(F32)
        rbuf[n, h] = total.astype(BF16)
        sent[n] = new_sem()
        push(rbuf.at[n, h], rarr.at[n, h], all_sent, sent[n], at_chip(chip(way)))
        reduced[0] += 1

    def finish_rows(item):
        grow_acc(*item)
        q = item[1]
        told_rows = xarr[q * crow // 8:(q + 1) * crow // 8].reshape(crow, LANES)
        rate = told_rows[:, 3 * ntp:3 * ntp + 3].astype(F32)
        a = (acc[chunk(q)] + mm(told_rows, tilt[...])) * jnp.sum(rate, axis=-1, keepdims=True)
        for k in range(2):
            gate, up = a[:, 2 * k * LANES:(2 * k + 1) * LANES], a[:, (2 * k + 1) * LANES:(2 * k + 2) * LANES]
            act[chunk(q), k * LANES:(k + 1) * LANES] = (jax.nn.silu(gate) * up).astype(BF16)
        for way in (1, -1):
            reduce_step(chain_no[way, q], 0)

    drain()
    phase("last_pieces")
    waiting = [last_piece(0)]
    for q in range(1, CHUNKS):
        waiting.append(last_piece(q))
        finish_rows(waiting[q - 1])
    finish_rows(waiting[CHUNKS - 1])
    phase("reduce_ring")
    for t in range(1, half_way):
        for n in range(len(chains)):
            reduce_step(n, t)
    left.append((rbuf.at[0:reduced[0] // half_way], all_sent))
    left.append((rows.at[0:counts_of[0] // CHUNKS], ring_sent))
    left.append((rows.at[0:counts_of[1] // CHUNKS], hand_sent))
    all_sent, arrived = new_sem(), new_sem()
    for q in range(CHUNKS):
        total = own_part(y, q)
        for way in (1, -1):
            n = chain_no[way, q]
            if n in sent:
                await_bytes(rarr.at[n, half_way - 1], sent[n])
                total = total + rarr[n, half_way - 1].astype(F32)
        rsend[q * crow // 8:(q + 1) * crow // 8] = total.astype(BF16).reshape(crow // 8, 8, LANES)
        for p in range(q * nsp // CHUNKS, min((q + 1) * nsp // CHUNKS, nsp - 1)):
            push(rsend.at[p * unit:(p + 1) * unit], rback.at[rows_of_peer(sp)], all_sent, arrived, to_sp(p, -1))
    left.append((rsend.at[0:(nsp - 1) * unit], all_sent))
    rback[rows_of_peer(sp)] = rsend[(nsp - 1) * unit:nsp * unit]
    phase("return_wait")
    drain()
    await_bytes(rback.at[0:(nsp - 1) * unit], arrived)
    phase("combine")

    back = rback[...].reshape(nrow, LANES)
    term[...] = (mm(pick_hi[...], back) + mm(pick_lo[...], back)).astype(BF16)
    phase("mix_over_tp")
    moved = over_tp(lambda to: term.at[rows_at(to)], mix.at[:, lanes_of(tp)], cols.at[0:(ntp - 1) * own_rows])
    mix[:, lanes_of(tp)] = term[rows_at(tp)]
    await_bytes(*moved)
    phase("last_norm")
    out[...] = layer_norm(settled[...] + mix[...].astype(F32), gains[1:2]).astype(BF16)

    phase("drain")
    drain()
    phase(None)


def layer(nsp, ntp, *args):
    (q1, k1, v1, g1, d1, q2, k2, v2, g2, d2, hg, p1, p2, st, gm, go, rt, af, eg, eu, ed) = args
    toks = q1.shape[0]
    width = st.shape[1]
    own_rows = toks // ntp
    cap = 3 * toks * 2 // (2 * nsp)
    nrow = nsp * cap
    ny = ntp // 2
    steps = ny // 2
    per = LANES // nsp
    mrow = -(-(3 * per + 3) // 16) * 16
    V = pltpu.VMEM
    D = pltpu.SemaphoreType.DMA
    one = (hg.reshape(1, -1), gm.reshape(1, -1), go.reshape(1, -1), rt.T, af.T)
    q1, k1 = q1.T, k1.T
    d1 = d1.transpose(0, 2, 1).reshape(2 * q1.shape[0], toks)
    operands = (q1, k1, v1, g1, d1, q2, k2, v2, g2, d2, one[0], p1, p2, st, one[1], one[2], one[3], one[4], eg, eu, ed)
    scratch = [
        V((2, *q1.shape), BF16), V((4, *q2.shape), BF16), V((2, *q2.shape), BF16), V(d1.shape, F32), V(d2.shape, F32),
        V((1, LANES), F32), V((2 * LANES, width), BF16), V((2 * LANES, width), BF16), V((toks, LANES), BF16),
        V((2, width), F32), V((2, toks), jnp.int32), V((2, toks), F32),
        V((width, 4 * LANES), BF16), V((2 * LANES, width), BF16),
        V((nsp, mrow, LANES), BF16), V((nsp, mrow, LANES), BF16), V((nsp, mrow, LANES), F32),
        V((nsp, mrow, LANES), BF16), V((nsp, mrow, LANES), BF16),
        V((3, toks, LANES), BF16), V((3, toks, LANES), BF16), V((3, toks // BLK, LANES, LANES), F32),
        V((2, toks, LANES), F32), V((toks, 2 * LANES), BF16), V((toks, 2 * LANES), BF16),
        V((ny, toks, LANES), F32),
        V((2 * CHUNKS, 4, toks // CHUNKS, LANES), BF16), V((2 * CHUNKS, 4, toks // CHUNKS, LANES), BF16),
        V((own_rows, width), F32), V((toks, LANES), F32), V((own_rows, LANES), BF16), V((toks, LANES), BF16),
        V((nrow, toks), BF16), V((nrow // 8, 8, LANES), BF16), V((nrow // 8, 8, LANES), BF16), V((LANES, 4 * LANES), BF16),
        V((toks, LANES), BF16),
        V((nrow // 8, 8, LANES), BF16), V((nrow // 8, 8, LANES), BF16), V((ntp, nrow, LANES), BF16),
        V((nrow, 4 * LANES), F32), V((nrow, 2 * LANES), BF16),
        V((2 * CHUNKS, steps, nrow // CHUNKS, LANES), BF16), V((2 * CHUNKS, steps, nrow // CHUNKS, LANES), BF16),
        V((nrow // 8, 8, LANES), BF16), V((nrow // 8, 8, LANES), BF16),
        V((toks, nrow), BF16), V((toks, nrow), BF16), V((toks, LANES), BF16), V((own_rows, width), BF16),
        D((163,)),
    ]
    return pl.pallas_call(
        functools.partial(kernel, (nsp, 4 if nsp % 4 == 0 else 1, ntp, toks, cap)),
        out_shape=jax.ShapeDtypeStruct((own_rows, width), BF16),
        in_specs=[pl.BlockSpec(memory_space=ANY)] * len(operands),
        out_specs=pl.BlockSpec(memory_space=pltpu.VMEM),
        scratch_shapes=scratch,
        compiler_params=pltpu.CompilerParams(collective_id=0, has_side_effects=True, vmem_limit_bytes=60 * 1024 * 1024),
        name="layer",
    )(*operands)


def solution(mesh):
    spec = P("sp", "tp")
    fade = P(None, "sp", "tp")
    return jax.shard_map(
        functools.partial(layer, mesh.shape["sp"], mesh.shape["tp"]),
        mesh=mesh,
        in_specs=(
            spec, spec, spec, spec, fade, spec, spec, spec, spec, fade,
            P(), P("tp", None), P("tp", None), P("sp", None), P(), P(), P("sp", None), P("sp", None),
            P("sp", None, "tp"), P("sp", None, "tp"), P("sp", "tp", None),
        ),
        out_specs=P(("sp", "tp"), None),
        check_vma=False,
    )
```

```python
import functools

import jax
import jax.numpy as jnp
from jax import lax
from jax.experimental import pallas as pl
from jax.experimental.pallas import tpu as pltpu
from jax.sharding import PartitionSpec as P

MESH = pl.DeviceIdType.MESH
F32 = jnp.float32
BF16 = jnp.bfloat16
BLK = 64
CHUNKS = 4
LANES = 128
ANY = pl.ANY


def mm(a, b):
    return jnp.dot(a, b, preferred_element_type=F32)


def mm_t(a, b):
    return lax.dot_general(a, b, (((1,), (1,)), ((), ())), preferred_element_type=F32)


def tmm(a, b):
    return lax.dot_general(a, b, (((0,), (0,)), ((), ())), preferred_element_type=F32)


def iota(shape, dim):
    return lax.broadcasted_iota(jnp.int32, shape, dim)


def far_first(sizes):
    steps = [()]
    for size in sizes:
        steps = [done + (k,) for done in steps for k in range(size)]
    return sorted(steps, key=lambda d: (-sum(min(k, n - k) for k, n in zip(d, sizes)), d))


def layer_norm(values, gain):
    mean = jnp.mean(values, axis=-1, keepdims=True)
    spread = jnp.mean(jnp.square(values - mean), axis=-1, keepdims=True)
    return (values - mean) * lax.rsqrt(spread + 1e-05) * gain


def kernel(
    cfg,
    q1h, k1h, v1h, g1h, d1h, q2h, k2h, v2h, g2h, d2h, hgh, p1h, p2h, sth, gmh, goh, rth, afh, egh, euh, edh,
    out,
    qk1, wide_in, gates, d1, d2, hg, own_proj, other_proj, stream, gains, rt, af, wgu, down,
    sbuf, sarr, fsum, sret, sback,
    qin, kin, grow, mixed, heads, heads_in, part,
    pbuf, parr, settled, settled_cols, own_stats, stats, chosen, xsend, xarr, tilt, cols, dsend, darr, rows, acc, act, rbuf, rarr, rsend, rback,
    pick_hi, pick_lo, term, mix,
    sems,
):
    nsp, nx, ntp, toks, cap = cfg
    nz = nsp // nx
    ny = ntp // 2
    half_way = ny // 2
    sp = lax.axis_index("sp")
    tp = lax.axis_index("tp")
    y = lax.div(tp, 2)
    c = lax.rem(tp, 2)
    sib = (sp, tp + 1 - 2 * c)
    blocks = toks // BLK
    own_rows = toks // ntp
    width = ntp * LANES
    per = LANES // nsp
    mrow = sbuf.shape[1]
    nrow = nsp * cap
    crow = nrow // CHUNKS
    z_at, x_at = lax.div(sp, nx), lax.rem(sp, nx)
    sp_moves = far_first((nz, nx))
    tp_moves = far_first((ny, 2))

    def sp_peer(move, way):
        return lax.rem(z_at + way * move[0] + nz, nz) * nx + lax.rem(x_at + way * move[1] + nx, nx)

    def chip(step):
        return lax.rem(y + step + ny, ny)

    def tp_peer(move):
        return 2 * chip(move[0]) + lax.rem(c + move[1], 2)

    scope = []

    def phase(name):
        if scope:
            scope.pop().__exit__(None, None, None)
        if name:
            scope.append(jax.named_scope(name))
            scope[0].__enter__()

    numbers = iter(range(sems.shape[0]))

    def new_sem():
        return sems.at[next(numbers)]

    def await_bytes(ref, sem):
        pltpu.make_async_copy(ref, ref, sem).wait()

    def load(*pairs):
        sem = new_sem()
        for src, dst in pairs:
            pltpu.make_async_copy(src, dst, sem).start()
        return sem

    phase("greet")
    barrier = pltpu.get_barrier_semaphore()
    for move in sp_moves[:-1]:
        pl.semaphore_signal(barrier, inc=1, device_id=(sp_peer(move, 1), tp), device_id_type=MESH)
    for move in tp_moves[:-1]:
        pl.semaphore_signal(barrier, inc=1, device_id=(sp, tp_peer(move)), device_id_type=MESH)
    first = [
        (d1, load((d1h, d1))), (d2, load((d2h, d2))),
        (wide_in, load((k2h, wide_in.at[0]), (v1h, wide_in.at[1]), (v2h, wide_in.at[2]), (q2h, wide_in.at[3]))),
        (qk1, load((q1h, qk1.at[0]), (k1h, qk1.at[1]))),
    ]
    own_stream = sth.at[:, pl.ds(pl.multiple_of(tp * LANES, LANES), LANES)]
    second = [
        (gates, load((g1h, gates.at[0]), (g2h, gates.at[1]))), (hg, load((hgh, hg))),
        (own_proj, load((p1h, own_proj.at[0:LANES]), (p2h, own_proj.at[LANES:2 * LANES]))),
        (stream, load((own_stream, stream))), (gains, load((gmh, gains.at[0:1]), (goh, gains.at[1:2]))),
        (rt, load((rth, rt))), (af, load((afh, af))),
        (wgu.at[:, 0:2 * LANES], load((egh.at[0], wgu.at[:, 0:LANES]), (euh.at[0], wgu.at[:, LANES:2 * LANES]))),
        (down.at[0:LANES], load((edh.at[0], down.at[0:LANES]))),
    ]

    phase("constants")
    r = iota((toks, toks), 0)
    s = iota((toks, toks), 1)
    tri = jnp.where((r // BLK == s // BLK) & (s <= r), 1.0, 0.0).astype(BF16)
    low = iota((1, LANES), 1) < LANES // 2
    m = iota((nsp * mrow, LANES), 0)
    o, i = m // mrow, m % mrow
    wanted = jnp.where(i < 3 * per, (i // per) * LANES + o * per + i % per, 3 * LANES + i - 3 * per)
    wanted = jnp.where(i < 3 * per + 3, wanted, -1)
    lane = iota((nsp * mrow, LANES), 1)
    pack = [jnp.where(wanted == lane + g * LANES, 1.0, 0.0).astype(BF16) for g in range(3)]
    lane16 = iota((nsp * mrow, 16), 1)
    pack.append(jnp.where(wanted[:, 0:16] == lane16 + 3 * LANES, 1.0, 0.0).astype(BF16))

    phase("load_wait")
    for item in first:
        await_bytes(*item)
    phase("fading")

    def two(a):
        a = a.astype(F32)
        return jnp.concatenate([a, a], axis=0).T

    fading = (d1[...].T, d2[0], d2[1])
    keys = (two(qk1[1]), wide_in[0].astype(F32), wide_in[0].astype(F32))
    queries = (two(qk1[0]) * 64 ** (-0.5), wide_in[3].astype(F32) * 128 ** (-0.5), wide_in[3].astype(F32) * 128 ** (-0.5))
    values = (wide_in[1], wide_in[2], wide_in[2])
    totals = []
    for g in range(3):
        x = fading[g]
        logs = (jnp.minimum(x, 0.0) - jnp.log1p(jnp.exp(-jnp.abs(x)))) * (1.0 / 16.0)
        hi = logs.astype(BF16)
        rest = logs - hi.astype(F32)
        mid = rest.astype(BF16)
        lo = (rest - mid.astype(F32)).astype(BF16)
        cum = mm(tri, hi) + mm(tri, mid) + mm(tri, lo)
        rows_of = []
        for b in range(blocks):
            at = slice(b * BLK, (b + 1) * BLK)
            ahead = cum[at]
            tot = ahead[BLK - 1:BLK]
            behind = tot - ahead + logs[at]
            run = ahead if g == 1 else behind if g == 2 else jnp.where(low, ahead, behind)
            qin[g, at] = (queries[g][at] * jnp.exp(run)).astype(BF16)
            kin[g, at] = (keys[g][at] * jnp.exp(-run)).astype(BF16)
            kst = (keys[g][at] * jnp.exp(tot - run)).astype(BF16)
            grow[g, b] = tmm(values[g][at], kst)
            rows_of.append(tot)
        totals.append(rows_of)

    fades = [[jnp.exp(t) for t in row] for row in totals]

    def chained(g, order, start):
        state = start
        seen = {}
        for b in order:
            seen[b] = state
            state = fades[g][b] * state + grow[g, b]
        return seen, state

    phase("chain")
    rise, fall = list(range(blocks)), list(range(blocks - 1, -1, -1))
    zero = jnp.zeros((LANES, LANES), F32)
    ends = [
        jnp.where(low, chained(0, rise, zero)[1], chained(0, fall, zero)[1]),
        chained(1, rise, zero)[1],
        chained(2, fall, zero)[1],
    ]
    sums = [sum(row[1:], row[0]) for row in totals]
    r16 = iota((16, LANES), 0)
    tail = jnp.where(r16 == 0, sums[0], jnp.where(r16 == 1, sums[1], jnp.where(r16 == 2, sums[2], 0.0)))
    packed = mm(pack[3], tail.astype(BF16))
    for g in range(3):
        packed = packed + mm(pack[g], ends[g].astype(BF16))
    sbuf[...] = packed.astype(BF16).reshape(nsp, mrow, LANES)

    phase("barrier")
    pl.semaphore_wait(barrier, nsp - 1 + ntp - 1)

    left = []

    def push(src, dst, ssem, rsem, device):
        pltpu.make_async_remote_copy(src, dst, ssem, rsem, device_id=device, device_id_type=MESH).start()

    def lend(size, *pairs):
        ssem, rsem = new_sem(), new_sem()
        for src, dst in pairs:
            push(src, dst, ssem, rsem, sib)
        left.append((size, ssem))
        return size, rsem

    def drain():
        while left:
            await_bytes(*left.pop(0))

    def to_sp(p, way=1):
        return (sp_peer(sp_moves[p], way), tp)

    phase("send_states")
    def over_sp(src, dst):
        ssem, rsem = new_sem(), new_sem()
        for p in range(nsp - 1):
            to = to_sp(p)
            push(src.at[to[0]], dst.at[sp], ssem, rsem, to)
        left.append((src.at[0:nsp - 1], ssem))
        dst[sp] = src[sp]
        return dst.at[0:nsp - 1], rsem

    coming = over_sp(sbuf, sarr)
    lent_proj = lend(other_proj, (p1h, other_proj.at[0:LANES]), (p2h, other_proj.at[LANES:2 * LANES]))
    lent_wgu = lend(
        wgu.at[:, 2 * LANES:4 * LANES], (egh.at[0], wgu.at[:, 2 * LANES:3 * LANES]), (euh.at[0], wgu.at[:, 3 * LANES:4 * LANES])
    )
    lent_down = lend(down.at[LANES:2 * LANES], (edh.at[0], down.at[LANES:2 * LANES]))

    phase("inner")
    rr, cc = iota((BLK, BLK), 0), iota((BLK, BLK), 1)
    lower, upper = cc <= rr, cc >= rr
    for b in range(blocks):
        at = slice(b * BLK, (b + 1) * BLK)
        q, k = qin[0, at], kin[0, at]
        nil = jnp.zeros_like(q)
        score = jnp.where(lower, mm_t(jnp.where(low, q, nil), k), 0.0) + jnp.where(upper, mm_t(jnp.where(low, nil, q), k), 0.0)
        mixed[0, at] = mm(score.astype(BF16), values[0][at])
        score = jnp.where(lower, mm_t(qin[1, at], kin[1, at]), 0.0) + jnp.where(upper, mm_t(qin[2, at], kin[2, at]), 0.0)
        mixed[1, at] = mm(score.astype(BF16), values[1][at])

    phase("wait_states")
    await_bytes(*coming)
    phase("scan")
    row = iota((mrow, LANES), 0)
    in_a, in_b = row < per, row < 2 * per

    def tile_of(j):
        t = sarr[j].astype(F32)
        fade = jnp.where(in_a, t[3 * per:3 * per + 1], jnp.where(in_b, t[3 * per + 1:3 * per + 2], t[3 * per + 2:3 * per + 3]))
        return t, jnp.exp(fade)

    state = jnp.zeros((mrow, LANES), F32)
    for j in range(nsp):
        t, fade = tile_of(j)
        fsum[j] = state
        state = fade * state + t
    forward = (in_a & low) | (in_b & jnp.logical_not(in_a))
    state = jnp.zeros((mrow, LANES), F32)
    for j in range(nsp - 1, -1, -1):
        t, fade = tile_of(j)
        sret[j] = jnp.where(forward, fsum[j], state).astype(BF16)
        state = fade * state + t
    phase("send_back")
    coming = over_sp(sret, sback)

    phase("places")
    z = iota((LANES, nsp * mrow), 0)
    m = iota((LANES, nsp * mrow), 1)
    lift = (z // per) * mrow + z % per
    unpack = [jnp.where(m == lift + g * per, 1.0, 0.0).astype(BF16) for g in range(3)]

    for item in second:
        await_bytes(*item)
    experts = iota((nsp, toks), 0)
    hits = [jnp.where(rt[k:k + 1] == experts, 1.0, 0.0) for k in range(2)]
    before = jnp.where(r < s, 1.0, 0.0).astype(BF16)
    counts = mm((hits[0] + hits[1]).astype(BF16), before)
    places = [
        rt[k:k + 1] * cap + jnp.sum(hits[k] * counts, axis=0, keepdims=True).astype(jnp.int32) for k in range(2)
    ]

    slots = iota((nrow, toks), 0)
    named = [slots == places[k] for k in range(2)]
    chosen[...] = jnp.where(named[0] | named[1], 1.0, 0.0).astype(BF16)
    share = af[0:1] + af[1:2]
    scaled = jnp.where(named[0], af[0:1] / share, 0.0) + jnp.where(named[1], af[1:2] / share, 0.0)
    scaled = scaled.T
    high = scaled.astype(BF16)
    pick_hi[...] = high
    pick_lo[...] = (scaled - high.astype(F32)).astype(BF16)

    await_bytes(*lent_wgu)
    apart = jnp.where(iota((ntp, width), 1) // LANES == iota((ntp, width), 0), gains[0:1], 0.0)
    coarse = apart.astype(BF16)
    fine = (apart - coarse.astype(F32)).astype(BF16)
    slope = mm(coarse, wgu[...]) + mm(fine, wgu[...])
    coarse = slope.astype(BF16)
    fine = (slope - coarse.astype(F32)).astype(BF16)
    tilt[0:ntp], tilt[ntp:2 * ntp], tilt[2 * ntp:3 * ntp] = coarse, coarse, fine
    tilt[3 * ntp:LANES] = jnp.zeros((LANES - 3 * ntp, 4 * LANES), BF16)
    await_bytes(*lent_proj)
    await_bytes(*lent_down)

    phase("wait_back")
    await_bytes(*coming)
    phase("readout")
    back = sback[...].reshape(nsp * mrow, LANES)
    come = [mm(unpack[g], back) for g in range(3)]
    fwd_a, back_a = chained(0, rise, come[0])[0], chained(0, fall, come[0])[0]
    fwd_b, back_b = chained(1, rise, come[1])[0], chained(2, fall, come[2])[0]
    shared = []
    for b in range(blocks):
        at = slice(b * BLK, (b + 1) * BLK)
        one = mixed[0, at] + mm_t(qin[0, at], jnp.where(low, fwd_a[b], back_a[b]).astype(BF16))
        other = mixed[1, at] + mm_t(qin[1, at], fwd_b[b].astype(BF16)) + mm_t(qin[2, at], back_b[b].astype(BF16))
        done = []
        for value, gate in ((one, gates.at[0]), (other, gates.at[1])):
            normed = value * lax.rsqrt(jnp.mean(value * value, axis=-1, keepdims=True) + 1e-06) * hg[...]
            done.append((normed * jax.nn.silu(gate[at].astype(F32))).astype(BF16))
        for k in range(2):
            heads[at, k * LANES:(k + 1) * LANES] = done[k]
        if b % 2:
            both = slice((b - 1) * BLK, (b + 1) * BLK)
            shared.append((both, lend(heads_in.at[both], (heads.at[both], heads_in.at[both]))))

    phase("proj")
    def lanes_of(k):
        return pl.ds(pl.multiple_of(k * LANES, LANES), LANES)

    def rows_at(k):
        return pl.ds(pl.multiple_of(k * own_rows, own_rows), own_rows)

    def slot(place, core):
        return 2 * place + core

    order = (3, ny - 3, 4, 1, ny - 1, 2, ny - 2, 0)
    far = [chip(d) for d in order]
    for both, item in shared:
        for d in far:
            part[d, both] = mm(heads[both], own_proj[:, lanes_of(slot(d, c))])

    phase("attn_ring")
    chains = [(way, q, (q % 2 == 0) != (way == 1)) for q in range(CHUNKS) for way in (1, -1)]
    chain_no = {(way, q): n for n, (way, q, skip) in enumerate(chains)}

    def at_chip(place):
        return (sp, 2 * place + c)

    tall = toks // CHUNKS
    pieces, all_sent = [0], new_sem()

    def span(q):
        return slice(q * tall, (q + 1) * tall)

    def toward(n, kind, total, hops, sem):
        way = chains[n][0]
        pbuf[n, kind] = total.astype(BF16)
        push(pbuf.at[n, kind], parr.at[n, kind], all_sent, sem, at_chip(chip(way * hops)))
        pieces[0] += 1

    early = [new_sem() for n in chains]
    final = [new_sem() for q in range(CHUNKS)]
    for both, item in shared:
        await_bytes(*item)
        for d in far:
            part[d, both] = part[d, both] + mm(heads_in[both], other_proj[:, lanes_of(slot(d, c))])
        for n, (way, q, skip) in enumerate(chains):
            if both.start <= span(q).start < both.stop:
                toward(n, 0, part[chip(3 * way), span(q)], 1, early[n])
                if not skip:
                    toward(n, 1, part[chip(4 * way), span(q)], 2, early[n])
    for n, (way, q, skip) in enumerate(chains):
        toward(n, 2, part[chip(way), span(q)], 1, final[q])
    for n, (way, q, skip) in enumerate(chains):
        kinds = 1 if skip else 2
        await_bytes(parr.at[n, 0:kinds], early[n])
        total = part[chip(2 * way), span(q)]
        for kind in range(kinds):
            total = total + parr[n, kind].astype(F32)
        toward(n, 3, total, 2, final[q])
    own_gain = gains[0:1, lanes_of(tp)]
    for q in range(CHUNKS):
        total = part[y, span(q)]
        await_bytes(parr.at[0], final[q])
        for kind in (2, 3):
            for way in (1, -1):
                total = total + parr[chain_no[way, q], kind].astype(F32)
        summed = stream[span(q)].astype(F32) + total.astype(BF16).astype(F32)
        settled_cols[span(q)] = summed
        cols[span(q)] = ((summed - jnp.mean(summed, axis=-1, keepdims=True)) * own_gain).astype(BF16)
    left.append((pbuf.at[0:pieces[0] // 4], all_sent))
    phase("dispatch")

    def over_tp(src_of, dst, size):
        ssem, rsem = new_sem(), new_sem()
        for move in tp_moves[:-1]:
            to = tp_peer(move)
            push(src_of(to), dst, ssem, rsem, (sp, to))
        left.append((size, ssem))
        return size, rsem

    dsend[...] = mm(chosen[...], cols[...]).astype(BF16).reshape(nrow // 8, 8, LANES)
    unit = cap // 8
    rows_of_peer = lambda k: pl.ds(k * unit, unit)

    def to_experts(src, dst):
        all_sent, coming = new_sem(), []
        for q in range(CHUNKS):
            some = range(q * nsp // CHUNKS, min((q + 1) * nsp // CHUNKS, nsp - 1))
            rsem = new_sem()
            for p in some:
                to = to_sp(p)
                push(src.at[rows_of_peer(to[0])], dst.at[p * unit:(p + 1) * unit], all_sent, rsem, to)
            coming.append((dst.at[some[0] * unit:(some[-1] + 1) * unit], rsem) if some else None)
        left.append((src.at[0:(nsp - 1) * unit], all_sent))
        dst[(nsp - 1) * unit:nsp * unit] = src[rows_of_peer(sp)]
        return coming

    coming = to_experts(dsend, darr)
    rowed = over_tp(lambda to: settled_cols.at[rows_at(to)], settled.at[:, lanes_of(tp)], settled_cols.at[0:(ntp - 1) * own_rows])
    settled[:, lanes_of(tp)] = settled_cols[rows_at(tp)]
    drain()
    phase("stats")
    await_bytes(*rowed)
    whole = settled[...]
    mean = jnp.mean(whole, axis=-1, keepdims=True)
    spread = jnp.mean(jnp.square(whole - mean), axis=-1, keepdims=True)
    rate = lax.rsqrt(spread + 1e-05)
    settled[...] = (whole - mean) * rate * gains[0:1]
    lane = iota((own_rows, LANES), 1)
    offset = jnp.zeros((own_rows, LANES), F32)
    for k in range(ntp):
        shift = jnp.mean(whole[:, k * LANES:(k + 1) * LANES], axis=-1, keepdims=True) - mean
        offset = jnp.where((lane % ntp == k) & (lane < 3 * ntp), shift, offset)
    coarse = offset.astype(BF16).astype(F32)
    offset = jnp.where((lane >= ntp) & (lane < 2 * ntp), offset - coarse, coarse)
    for k in range(3):
        top = rate.astype(BF16).astype(F32)
        offset = jnp.where(lane == 3 * ntp + k, top, offset)
        rate = rate - top
    own_stats[...] = offset.astype(BF16)
    told = over_tp(lambda to: own_stats, stats.at[rows_at(tp)], stats.at[0:(ntp - 1) * own_rows])
    stats[rows_at(tp)] = own_stats[...]
    phase("dispatch_wait")

    def chunk(q):
        return slice(q * crow, (q + 1) * crow)

    ring_sent, hand_sent = new_sem(), new_sem()
    counts_of = [0, 0]

    def ways_at(q, h):
        return [way for way in (1, -1) if h < half_way - chains[chain_no[way, q]][2]]

    def some_rows(count):
        return rows.at[0, 0:count * crow]

    def hand_on(q, spots):
        sem = new_sem()
        for place in spots:
            at = rows.at[slot(place, c), chunk(q)]
            push(at, at, hand_sent, sem, sib)
            counts_of[1] += 1
        return (some_rows(len(spots)), sem), q, spots

    def ring(q, h):
        sem = new_sem()
        for way in ways_at(q, h):
            at = rows.at[slot(chip(-way * h), c), chunk(q)]
            push(at, at, ring_sent, sem, at_chip(chip(way)))
            counts_of[0] += 1
        return some_rows(len(ways_at(q, h))), sem

    def grow_acc(item, q, spots, fresh=False):
        await_bytes(*item)
        more = None
        for place in spots:
            both = jnp.concatenate([rows[slot(place, 0), chunk(q)], rows[slot(place, 1), chunk(q)]], axis=1)
            one = mm(both, wgu[pl.ds(pl.multiple_of(place * 2 * LANES, 2 * LANES), 2 * LANES)])
            more = one if more is None else more + one
        acc[chunk(q)] = more if fresh else acc[chunk(q)] + more

    link, passed = [], []
    for q in range(CHUNKS):
        if coming[q]:
            await_bytes(*coming[q])
        rows[tp, chunk(q)] = darr[q * crow // 8:(q + 1) * crow // 8].reshape(crow, LANES)
        link.append(ring(q, 0))
        passed.append((*hand_on(q, [y]), True))
    phase("gather_ring")
    for h in range(half_way - 1):
        fresh = []
        for q in range(CHUNKS):
            await_bytes(*link[q])
            if ways_at(q, h + 1):
                link[q] = ring(q, h + 1)
            fresh.append(hand_on(q, [chip(-way * (h + 1)) for way in ways_at(q, h)]))
            if h == 0 and q == 1:
                await_bytes(*told)
                xsend[...] = mm(chosen[...], stats[...]).astype(BF16).reshape(nrow // 8, 8, LANES)
                facts = to_experts(xsend, xarr)
            if h > 0:
                grow_acc(*passed[q])
        if h == 0:
            for item in passed:
                grow_acc(*item)
        passed = fresh
    for q in range(CHUNKS):
        grow_acc(*passed[q])

    def last_piece(q):
        await_bytes(*link[q])
        return hand_on(q, [chip(half_way)])

    def own_part(place, q):
        return mm(act[chunk(q)], down[:, lanes_of(slot(place, c))])

    sent, reduced, all_sent = {}, [0], new_sem()

    def landed(q, t):
        await_bytes(rarr.at[0, 0:len(ways_at(q, t))], sent[q])

    def reduce_step(q, t):
        ways = ways_at(q, t)
        where = {way: t + chains[chain_no[way, q]][2] for way in ways}
        totals = {way: own_part(chip(way * (half_way - where[way])), q) for way in ways}
        if t > 0:
            landed(q, t - 1)
        sent[q] = new_sem()
        for way in ways:
            n, h = chain_no[way, q], where[way]
            total = totals[way]
            if t > 0:
                total = total + rarr[n, h - 1].astype(F32)
            rbuf[n, h] = total.astype(BF16)
            push(rbuf.at[n, h], rarr.at[n, h], all_sent, sent[q], at_chip(chip(way)))
            reduced[0] += 1

    def told_rows(q):
        return xarr[q * crow // 8:(q + 1) * crow // 8].reshape(crow, LANES)

    def finish_rows(item):
        grow_acc(*item)
        q = item[1]
        rate = told_rows(q)[:, 3 * ntp:3 * ntp + 3].astype(F32)
        a = acc[chunk(q)] * jnp.sum(rate, axis=-1, keepdims=True)
        for k in range(2):
            gate, up = a[:, 2 * k * LANES:(2 * k + 1) * LANES], a[:, (2 * k + 1) * LANES:(2 * k + 2) * LANES]
            act[chunk(q), k * LANES:(k + 1) * LANES] = (jax.nn.silu(gate) * up).astype(BF16)
        reduce_step(q, 0)

    phase("facts")
    for q in range(CHUNKS):
        if facts[q]:
            await_bytes(*facts[q])
        acc[chunk(q)] = acc[chunk(q)] + mm(told_rows(q), tilt[...])
    drain()
    phase("last_pieces")
    waiting = [last_piece(0)]
    for q in range(1, CHUNKS):
        waiting.append(last_piece(q))
        finish_rows(waiting[q - 1])
    finish_rows(waiting[CHUNKS - 1])
    phase("reduce_ring")
    for t in range(1, half_way):
        for q in range(CHUNKS):
            reduce_step(q, t)
    left.append((rbuf.at[0:reduced[0] // half_way], all_sent))
    left.append((rows.at[0:counts_of[0] // CHUNKS], ring_sent))
    left.append((rows.at[0:counts_of[1] // CHUNKS], hand_sent))
    all_sent, arrived = new_sem(), new_sem()
    for q in range(CHUNKS):
        total = own_part(y, q)
        landed(q, half_way - 1)
        for way in (1, -1):
            total = total + rarr[chain_no[way, q], half_way - 1].astype(F32)
        rsend[q * crow // 8:(q + 1) * crow // 8] = total.astype(BF16).reshape(crow // 8, 8, LANES)
        for p in range(q * nsp // CHUNKS, min((q + 1) * nsp // CHUNKS, nsp - 1)):
            push(rsend.at[p * unit:(p + 1) * unit], rback.at[rows_of_peer(sp)], all_sent, arrived, to_sp(p, -1))
    left.append((rsend.at[0:(nsp - 1) * unit], all_sent))
    rback[rows_of_peer(sp)] = rsend[(nsp - 1) * unit:nsp * unit]
    phase("return_wait")
    drain()
    await_bytes(rback.at[0:(nsp - 1) * unit], arrived)
    phase("combine")

    back = rback[...].reshape(nrow, LANES)
    term[...] = (mm(pick_hi[...], back) + mm(pick_lo[...], back)).astype(BF16)
    phase("mix_over_tp")
    moved = over_tp(lambda to: term.at[rows_at(to)], mix.at[:, lanes_of(tp)], cols.at[0:(ntp - 1) * own_rows])
    mix[:, lanes_of(tp)] = term[rows_at(tp)]
    await_bytes(*moved)
    phase("last_norm")
    out[...] = layer_norm(settled[...] + mix[...].astype(F32), gains[1:2]).astype(BF16)

    phase("drain")
    drain()
    phase(None)


def layer(nsp, ntp, *args):
    (q1, k1, v1, g1, d1, q2, k2, v2, g2, d2, hg, p1, p2, st, gm, go, rt, af, eg, eu, ed) = args
    toks = q1.shape[0]
    width = st.shape[1]
    own_rows = toks // ntp
    cap = 3 * toks * 2 // (2 * nsp)
    nrow = nsp * cap
    ny = ntp // 2
    steps = ny // 2
    per = LANES // nsp
    mrow = -(-(3 * per + 3) // 16) * 16
    V = pltpu.VMEM
    D = pltpu.SemaphoreType.DMA
    one = (hg.reshape(1, -1), gm.reshape(1, -1), go.reshape(1, -1), rt.T, af.T)
    q1, k1 = q1.T, k1.T
    d1 = d1.transpose(0, 2, 1).reshape(2 * q1.shape[0], toks)
    operands = (q1, k1, v1, g1, d1, q2, k2, v2, g2, d2, one[0], p1, p2, st, one[1], one[2], one[3], one[4], eg, eu, ed)
    scratch = [
        V((2, *q1.shape), BF16), V((4, *q2.shape), BF16), V((2, *q2.shape), BF16), V(d1.shape, F32), V(d2.shape, F32),
        V((1, LANES), F32), V((2 * LANES, width), BF16), V((2 * LANES, width), BF16), V((toks, LANES), BF16),
        V((2, width), F32), V((2, toks), jnp.int32), V((2, toks), F32),
        V((width, 4 * LANES), BF16), V((2 * LANES, width), BF16),
        V((nsp, mrow, LANES), BF16), V((nsp, mrow, LANES), BF16), V((nsp, mrow, LANES), F32),
        V((nsp, mrow, LANES), BF16), V((nsp, mrow, LANES), BF16),
        V((3, toks, LANES), BF16), V((3, toks, LANES), BF16), V((3, toks // BLK, LANES, LANES), F32),
        V((2, toks, LANES), F32), V((toks, 2 * LANES), BF16), V((toks, 2 * LANES), BF16),
        V((ny, toks, LANES), F32),
        V((2 * CHUNKS, 4, toks // CHUNKS, LANES), BF16), V((2 * CHUNKS, 4, toks // CHUNKS, LANES), BF16),
        V((own_rows, width), F32), V((toks, LANES), F32), V((own_rows, LANES), BF16), V((toks, LANES), BF16),
        V((nrow, toks), BF16), V((nrow // 8, 8, LANES), BF16), V((nrow // 8, 8, LANES), BF16), V((LANES, 4 * LANES), BF16),
        V((toks, LANES), BF16),
        V((nrow // 8, 8, LANES), BF16), V((nrow // 8, 8, LANES), BF16), V((ntp, nrow, LANES), BF16),
        V((nrow, 4 * LANES), F32), V((nrow, 2 * LANES), BF16),
        V((2 * CHUNKS, steps, nrow // CHUNKS, LANES), BF16), V((2 * CHUNKS, steps, nrow // CHUNKS, LANES), BF16),
        V((nrow // 8, 8, LANES), BF16), V((nrow // 8, 8, LANES), BF16),
        V((toks, nrow), BF16), V((toks, nrow), BF16), V((toks, LANES), BF16), V((own_rows, width), BF16),
        D((113,)),
    ]
    return pl.pallas_call(
        functools.partial(kernel, (nsp, 4 if nsp % 4 == 0 else 1, ntp, toks, cap)),
        out_shape=jax.ShapeDtypeStruct((own_rows, width), BF16),
        in_specs=[pl.BlockSpec(memory_space=ANY)] * len(operands),
        out_specs=pl.BlockSpec(memory_space=pltpu.VMEM),
        scratch_shapes=scratch,
        compiler_params=pltpu.CompilerParams(collective_id=0, has_side_effects=True, vmem_limit_bytes=60 * 1024 * 1024),
        name="layer",
    )(*operands)


def solution(mesh):
    spec = P("sp", "tp")
    fade = P(None, "sp", "tp")
    return jax.shard_map(
        functools.partial(layer, mesh.shape["sp"], mesh.shape["tp"]),
        mesh=mesh,
        in_specs=(
            spec, spec, spec, spec, fade, spec, spec, spec, spec, fade,
            P(), P("tp", None), P("tp", None), P("sp", None), P(), P(), P("sp", None), P("sp", None),
            P("sp", None, "tp"), P("sp", None, "tp"), P("sp", "tp", None),
        ),
        out_specs=P(("sp", "tp"), None),
        check_vma=False,
    )
```

```python
import functools

import jax
import jax.numpy as jnp
from jax import lax
from jax.experimental import pallas as pl
from jax.experimental.pallas import tpu as pltpu
from jax.sharding import PartitionSpec as P

MESH = pl.DeviceIdType.MESH
F32 = jnp.float32
BF16 = jnp.bfloat16
BLK = 64
CHUNKS = 4
LANES = 128
ANY = pl.ANY


def mm(a, b):
    return jnp.dot(a, b, preferred_element_type=F32)


def mm_t(a, b):
    return lax.dot_general(a, b, (((1,), (1,)), ((), ())), preferred_element_type=F32)


def tmm(a, b):
    return lax.dot_general(a, b, (((0,), (0,)), ((), ())), preferred_element_type=F32)


def iota(shape, dim):
    return lax.broadcasted_iota(jnp.int32, shape, dim)


def far_first(sizes):
    steps = [()]
    for size in sizes:
        steps = [done + (k,) for done in steps for k in range(size)]
    return sorted(steps, key=lambda d: (-sum(min(k, n - k) for k, n in zip(d, sizes)), d))


def layer_norm(values, gain):
    mean = jnp.mean(values, axis=-1, keepdims=True)
    spread = jnp.mean(jnp.square(values - mean), axis=-1, keepdims=True)
    return (values - mean) * lax.rsqrt(spread + 1e-05) * gain


def kernel(
    cfg,
    q1h, k1h, v1h, g1h, d1h, q2h, k2h, v2h, g2h, d2h, hgh, p1h, p2h, sth, gmh, goh, rth, afh, egh, euh, edh,
    out,
    qk1, wide_in, gates, d1, d2, hg, own_proj, other_proj, stream, gains, rt, af, wgu, down,
    sbuf, sarr, fsum, sret, sback,
    qin, kin, grow, mixed, heads, heads_in, part,
    pbuf, parr, settled, settled_cols, own_stats, stats, chosen, xsend, xarr, tilt, cols, dsend, darr, rows, acc, act, rbuf, rarr, rsend, rback,
    pick_hi, pick_lo, term, mix,
    sems,
):
    nsp, nx, ntp, toks, cap = cfg
    nz = nsp // nx
    ny = ntp // 2
    half_way = ny // 2
    sp = lax.axis_index("sp")
    tp = lax.axis_index("tp")
    y = lax.div(tp, 2)
    c = lax.rem(tp, 2)
    sib = (sp, tp + 1 - 2 * c)
    blocks = toks // BLK
    own_rows = toks // ntp
    width = ntp * LANES
    per = LANES // nsp
    mrow = sbuf.shape[1]
    nrow = nsp * cap
    crow = nrow // CHUNKS
    z_at, x_at = lax.div(sp, nx), lax.rem(sp, nx)
    sp_moves = far_first((nz, nx))
    tp_moves = far_first((ny, 2))

    def sp_peer(move, way):
        return lax.rem(z_at + way * move[0] + nz, nz) * nx + lax.rem(x_at + way * move[1] + nx, nx)

    def chip(step):
        return lax.rem(y + step + ny, ny)

    def tp_peer(move):
        return 2 * chip(move[0]) + lax.rem(c + move[1], 2)

    scope = []

    def phase(name):
        if scope:
            scope.pop().__exit__(None, None, None)
        if name:
            scope.append(jax.named_scope(name))
            scope[0].__enter__()

    numbers = iter(range(sems.shape[0]))

    def new_sem():
        return sems.at[next(numbers)]

    def await_bytes(ref, sem):
        pltpu.make_async_copy(ref, ref, sem).wait()

    def load(*pairs):
        sem = new_sem()
        for src, dst in pairs:
            pltpu.make_async_copy(src, dst, sem).start()
        return sem

    phase("greet")
    barrier = pltpu.get_barrier_semaphore()
    for move in sp_moves[:-1]:
        pl.semaphore_signal(barrier, inc=1, device_id=(sp_peer(move, 1), tp), device_id_type=MESH)
    for move in tp_moves[:-1]:
        pl.semaphore_signal(barrier, inc=1, device_id=(sp, tp_peer(move)), device_id_type=MESH)
    first = [
        (d1, load((d1h, d1))), (d2, load((d2h, d2))),
        (wide_in, load((k2h, wide_in.at[0]), (v1h, wide_in.at[1]), (v2h, wide_in.at[2]), (q2h, wide_in.at[3]))),
        (qk1, load((q1h, qk1.at[0]), (k1h, qk1.at[1]))),
    ]
    own_stream = sth.at[:, pl.ds(pl.multiple_of(tp * LANES, LANES), LANES)]
    second = [
        (gates, load((g1h, gates.at[0]), (g2h, gates.at[1]))), (hg, load((hgh, hg))),
        (own_proj, load((p1h, own_proj.at[0:LANES]), (p2h, own_proj.at[LANES:2 * LANES]))),
        (stream, load((own_stream, stream))), (gains, load((gmh, gains.at[0:1]), (goh, gains.at[1:2]))),
        (rt, load((rth, rt))), (af, load((afh, af))),
        (wgu.at[:, 0:2 * LANES], load((egh.at[0], wgu.at[:, 0:LANES]), (euh.at[0], wgu.at[:, LANES:2 * LANES]))),
        (down.at[0:LANES], load((edh.at[0], down.at[0:LANES]))),
    ]

    phase("constants")
    r = iota((toks, toks), 0)
    s = iota((toks, toks), 1)
    tri = jnp.where((r // BLK == s // BLK) & (s <= r), 1.0, 0.0).astype(BF16)
    low = iota((1, LANES), 1) < LANES // 2
    m = iota((nsp * mrow, LANES), 0)
    o, i = m // mrow, m % mrow
    wanted = jnp.where(i < 3 * per, (i // per) * LANES + o * per + i % per, 3 * LANES + i - 3 * per)
    wanted = jnp.where(i < 3 * per + 3, wanted, -1)
    lane = iota((nsp * mrow, LANES), 1)
    pack = [jnp.where(wanted == lane + g * LANES, 1.0, 0.0).astype(BF16) for g in range(3)]
    lane16 = iota((nsp * mrow, 16), 1)
    pack.append(jnp.where(wanted[:, 0:16] == lane16 + 3 * LANES, 1.0, 0.0).astype(BF16))

    phase("load_wait")
    for item in first:
        await_bytes(*item)
    phase("fading")

    def two(a):
        a = a.astype(F32)
        return jnp.concatenate([a, a], axis=0).T

    fading = (d1[...].T, d2[0], d2[1])
    keys = (two(qk1[1]), wide_in[0].astype(F32), wide_in[0].astype(F32))
    queries = (two(qk1[0]) * 64 ** (-0.5), wide_in[3].astype(F32) * 128 ** (-0.5), wide_in[3].astype(F32) * 128 ** (-0.5))
    values = (wide_in[1], wide_in[2], wide_in[2])
    totals = []
    for g in range(3):
        x = fading[g]
        logs = (jnp.minimum(x, 0.0) - jnp.log1p(jnp.exp(-jnp.abs(x)))) * (1.0 / 16.0)
        hi = logs.astype(BF16)
        rest = logs - hi.astype(F32)
        mid = rest.astype(BF16)
        lo = (rest - mid.astype(F32)).astype(BF16)
        cum = mm(tri, hi) + mm(tri, mid) + mm(tri, lo)
        rows_of = []
        for b in range(blocks):
            at = slice(b * BLK, (b + 1) * BLK)
            ahead = cum[at]
            tot = ahead[BLK - 1:BLK]
            behind = tot - ahead + logs[at]
            run = ahead if g == 1 else behind if g == 2 else jnp.where(low, ahead, behind)
            qin[g, at] = (queries[g][at] * jnp.exp(run)).astype(BF16)
            kin[g, at] = (keys[g][at] * jnp.exp(-run)).astype(BF16)
            kst = (keys[g][at] * jnp.exp(tot - run)).astype(BF16)
            grow[g, b] = tmm(values[g][at], kst)
            rows_of.append(tot)
        totals.append(rows_of)

    fades = [[jnp.exp(t) for t in row] for row in totals]

    def chained(g, order, start):
        state = start
        seen = {}
        for b in order:
            seen[b] = state
            state = fades[g][b] * state + grow[g, b]
        return seen, state

    phase("chain")
    rise, fall = list(range(blocks)), list(range(blocks - 1, -1, -1))
    zero = jnp.zeros((LANES, LANES), F32)
    ends = [
        jnp.where(low, chained(0, rise, zero)[1], chained(0, fall, zero)[1]),
        chained(1, rise, zero)[1],
        chained(2, fall, zero)[1],
    ]
    sums = [sum(row[1:], row[0]) for row in totals]
    r16 = iota((16, LANES), 0)
    tail = jnp.where(r16 == 0, sums[0], jnp.where(r16 == 1, sums[1], jnp.where(r16 == 2, sums[2], 0.0)))
    packed = mm(pack[3], tail.astype(BF16))
    for g in range(3):
        packed = packed + mm(pack[g], ends[g].astype(BF16))
    sbuf[...] = packed.astype(BF16).reshape(nsp, mrow, LANES)

    phase("barrier")
    pl.semaphore_wait(barrier, nsp - 1 + ntp - 1)

    left = []

    def push(src, dst, ssem, rsem, device):
        pltpu.make_async_remote_copy(src, dst, ssem, rsem, device_id=device, device_id_type=MESH).start()

    def lend(size, *pairs):
        ssem, rsem = new_sem(), new_sem()
        for src, dst in pairs:
            push(src, dst, ssem, rsem, sib)
        left.append((size, ssem))
        return size, rsem

    def drain():
        while left:
            await_bytes(*left.pop(0))

    def to_sp(p, way=1):
        return (sp_peer(sp_moves[p], way), tp)

    phase("send_states")
    def over_sp(src, dst):
        ssem, rsem = new_sem(), new_sem()
        for p in range(nsp - 1):
            to = to_sp(p)
            push(src.at[to[0]], dst.at[sp], ssem, rsem, to)
        left.append((src.at[0:nsp - 1], ssem))
        dst[sp] = src[sp]
        return dst.at[0:nsp - 1], rsem

    coming = over_sp(sbuf, sarr)
    lent_proj = lend(other_proj, (p1h, other_proj.at[0:LANES]), (p2h, other_proj.at[LANES:2 * LANES]))
    lent_wgu = lend(
        wgu.at[:, 2 * LANES:4 * LANES], (egh.at[0], wgu.at[:, 2 * LANES:3 * LANES]), (euh.at[0], wgu.at[:, 3 * LANES:4 * LANES])
    )
    lent_down = lend(down.at[LANES:2 * LANES], (edh.at[0], down.at[LANES:2 * LANES]))

    phase("inner")
    rr, cc = iota((BLK, BLK), 0), iota((BLK, BLK), 1)
    lower, upper = cc <= rr, cc >= rr
    for b in range(blocks):
        at = slice(b * BLK, (b + 1) * BLK)
        q, k = qin[0, at], kin[0, at]
        nil = jnp.zeros_like(q)
        score = jnp.where(lower, mm_t(jnp.where(low, q, nil), k), 0.0) + jnp.where(upper, mm_t(jnp.where(low, nil, q), k), 0.0)
        mixed[0, at] = mm(score.astype(BF16), values[0][at])
        score = jnp.where(lower, mm_t(qin[1, at], kin[1, at]), 0.0) + jnp.where(upper, mm_t(qin[2, at], kin[2, at]), 0.0)
        mixed[1, at] = mm(score.astype(BF16), values[1][at])

    def reached(g, order):
        share = jnp.ones((1, LANES), F32)
        seen = {}
        for b in order:
            seen[b] = share
            share = share * fades[g][b]
        return seen

    rise_a, fall_a = chained(0, rise, zero)[0], chained(0, fall, zero)[0]
    rise_b, fall_b = chained(1, rise, zero)[0], chained(2, fall, zero)[0]
    reach = [
        {b: jnp.where(low, reached(0, rise)[b], reached(0, fall)[b]) for b in rise}, reached(1, rise), reached(2, fall)
    ]
    for b in range(blocks):
        at = slice(b * BLK, (b + 1) * BLK)
        mixed[0, at] = mixed[0, at] + mm_t(qin[0, at], jnp.where(low, rise_a[b], fall_a[b]).astype(BF16))
        mixed[1, at] = mixed[1, at] + mm_t(qin[1, at], rise_b[b].astype(BF16)) + mm_t(qin[2, at], fall_b[b].astype(BF16))
        for g in range(3):
            qin[g, at] = (qin[g, at].astype(F32) * reach[g][b]).astype(BF16)

    phase("wait_states")
    await_bytes(*coming)
    phase("scan")
    row = iota((mrow, LANES), 0)
    in_a, in_b = row < per, row < 2 * per

    def tile_of(j):
        t = sarr[j].astype(F32)
        fade = jnp.where(in_a, t[3 * per:3 * per + 1], jnp.where(in_b, t[3 * per + 1:3 * per + 2], t[3 * per + 2:3 * per + 3]))
        return t, jnp.exp(fade)

    state = jnp.zeros((mrow, LANES), F32)
    for j in range(nsp):
        t, fade = tile_of(j)
        fsum[j] = state
        state = fade * state + t
    forward = (in_a & low) | (in_b & jnp.logical_not(in_a))
    state = jnp.zeros((mrow, LANES), F32)
    for j in range(nsp - 1, -1, -1):
        t, fade = tile_of(j)
        sret[j] = jnp.where(forward, fsum[j], state).astype(BF16)
        state = fade * state + t
    phase("send_back")
    coming = over_sp(sret, sback)

    phase("places")
    z = iota((LANES, nsp * mrow), 0)
    m = iota((LANES, nsp * mrow), 1)
    lift = (z // per) * mrow + z % per
    unpack = [jnp.where(m == lift + g * per, 1.0, 0.0).astype(BF16) for g in range(3)]

    for item in second:
        await_bytes(*item)
    experts = iota((nsp, toks), 0)
    hits = [jnp.where(rt[k:k + 1] == experts, 1.0, 0.0) for k in range(2)]
    before = jnp.where(r < s, 1.0, 0.0).astype(BF16)
    counts = mm((hits[0] + hits[1]).astype(BF16), before)
    spot = jnp.zeros((nsp, toks), jnp.int32)
    for p, move in enumerate(sp_moves):
        spot = jnp.where(experts == sp_peer(move, 1), p * cap, spot)
    counts = counts + spot.astype(F32)
    places = [jnp.sum(hits[k] * counts, axis=0, keepdims=True).astype(jnp.int32) for k in range(2)]

    slots = iota((nrow, toks), 0)
    named = [slots == places[k] for k in range(2)]
    chosen[...] = jnp.where(named[0] | named[1], 1.0, 0.0).astype(BF16)
    share = af[0:1] + af[1:2]
    scaled = jnp.where(named[0], af[0:1] / share, 0.0) + jnp.where(named[1], af[1:2] / share, 0.0)
    for q in range(CHUNKS):
        some = scaled[q * crow:(q + 1) * crow].T
        high = some.astype(BF16)
        pick_hi[q] = high
        pick_lo[q] = (some - high.astype(F32)).astype(BF16)

    await_bytes(*lent_wgu)
    apart = jnp.where(iota((ntp, width), 1) // LANES == iota((ntp, width), 0), gains[0:1], 0.0)
    coarse = apart.astype(BF16)
    fine = (apart - coarse.astype(F32)).astype(BF16)
    slope = mm(coarse, wgu[...]) + mm(fine, wgu[...])
    coarse = slope.astype(BF16)
    fine = (slope - coarse.astype(F32)).astype(BF16)
    tilt[0:ntp], tilt[ntp:2 * ntp], tilt[2 * ntp:3 * ntp] = coarse, coarse, fine
    tilt[3 * ntp:LANES] = jnp.zeros((LANES - 3 * ntp, 4 * LANES), BF16)
    await_bytes(*lent_proj)
    await_bytes(*lent_down)

    phase("wait_back")
    await_bytes(*coming)
    phase("readout")
    back = sback[...].reshape(nsp * mrow, LANES)
    come = [mm(unpack[g], back).astype(BF16) for g in range(3)]
    shared = []
    for n in range(2):
        at = slice(n * toks // 2, (n + 1) * toks // 2)
        one = mixed[0, at] + mm_t(qin[0, at], come[0])
        other = mixed[1, at] + mm_t(qin[1, at], come[1]) + mm_t(qin[2, at], come[2])
        for k, (value, gate) in enumerate(((one, gates.at[0]), (other, gates.at[1]))):
            normed = value * lax.rsqrt(jnp.mean(value * value, axis=-1, keepdims=True) + 1e-06) * hg[...]
            heads[at, k * LANES:(k + 1) * LANES] = (normed * jax.nn.silu(gate[at].astype(F32))).astype(BF16)
        shared.append((at, lend(heads_in.at[at], (heads.at[at], heads_in.at[at]))))

    phase("proj")
    def lanes_of(k):
        return pl.ds(pl.multiple_of(k * LANES, LANES), LANES)

    def rows_at(k):
        return pl.ds(pl.multiple_of(k * own_rows, own_rows), own_rows)

    def slot(place, core):
        return 2 * place + core

    order = (3, ny - 3, 4, 1, ny - 1, 2, ny - 2, 0)
    far = [chip(d) for d in order]
    for both, item in shared:
        for d in far:
            part[d, both] = mm(heads[both], own_proj[:, lanes_of(slot(d, c))])

    phase("attn_ring")
    chains = [(way, q, (q % 2 == 0) != (way == 1)) for q in range(CHUNKS) for way in (1, -1)]
    chain_no = {(way, q): n for n, (way, q, skip) in enumerate(chains)}

    def at_chip(place):
        return (sp, 2 * place + c)

    tall = toks // CHUNKS
    pieces, all_sent = [0], new_sem()

    def span(q):
        return slice(q * tall, (q + 1) * tall)

    def toward(n, kind, total, hops, sem):
        way = chains[n][0]
        pbuf[n, kind] = total.astype(BF16)
        push(pbuf.at[n, kind], parr.at[n, kind], all_sent, sem, at_chip(chip(way * hops)))
        pieces[0] += 1

    early = [new_sem() for n in chains]
    final = [new_sem() for q in range(CHUNKS)]
    for both, item in shared:
        await_bytes(*item)
        for d in far:
            part[d, both] = part[d, both] + mm(heads_in[both], other_proj[:, lanes_of(slot(d, c))])
        for n, (way, q, skip) in enumerate(chains):
            if both.start <= span(q).start < both.stop:
                toward(n, 0, part[chip(3 * way), span(q)], 1, early[n])
                if not skip:
                    toward(n, 1, part[chip(4 * way), span(q)], 2, early[n])
    for n, (way, q, skip) in enumerate(chains):
        toward(n, 2, part[chip(way), span(q)], 1, final[q])
    for n, (way, q, skip) in enumerate(chains):
        kinds = 1 if skip else 2
        await_bytes(parr.at[n, 0:kinds], early[n])
        total = part[chip(2 * way), span(q)]
        for kind in range(kinds):
            total = total + parr[n, kind].astype(F32)
        toward(n, 3, total, 2, final[q])
    own_gain = gains[0:1, lanes_of(tp)]
    for q in range(CHUNKS):
        total = part[y, span(q)]
        await_bytes(parr.at[0], final[q])
        for kind in (2, 3):
            for way in (1, -1):
                total = total + parr[chain_no[way, q], kind].astype(F32)
        summed = stream[span(q)].astype(F32) + total.astype(BF16).astype(F32)
        settled_cols[span(q)] = summed
        cols[span(q)] = ((summed - jnp.mean(summed, axis=-1, keepdims=True)) * own_gain).astype(BF16)
    left.append((pbuf.at[0:pieces[0] // 4], all_sent))
    phase("dispatch")

    def over_tp(src_of, dst, size):
        ssem, rsem = new_sem(), new_sem()
        for move in tp_moves[:-1]:
            to = tp_peer(move)
            push(src_of(to), dst, ssem, rsem, (sp, to))
        left.append((size, ssem))
        return size, rsem

    unit = cap // 8

    def chunk(q):
        return slice(q * crow, (q + 1) * crow)

    def units(q):
        return slice(q * crow // 8, (q + 1) * crow // 8)

    def peers(q):
        return range(q * nsp // CHUNKS, min((q + 1) * nsp // CHUNKS, nsp - 1))

    def to_experts(values, src, dst):
        all_sent, coming = new_sem(), []
        for q in range(CHUNKS):
            src[units(q)] = mm(chosen[chunk(q)], values[...]).astype(BF16).reshape(crow // 8, 8, LANES)
            rsem = new_sem()
            for p in peers(q):
                at = slice(p * unit, (p + 1) * unit)
                push(src.at[at], dst.at[at], all_sent, rsem, to_sp(p))
            coming.append((dst.at[peers(q)[0] * unit:(peers(q)[-1] + 1) * unit], rsem) if peers(q) else None)
        left.append((src.at[0:(nsp - 1) * unit], all_sent))
        dst[(nsp - 1) * unit:nsp * unit] = src[(nsp - 1) * unit:nsp * unit]
        return coming

    coming = to_experts(cols, dsend, darr)
    rowed = over_tp(lambda to: settled_cols.at[rows_at(to)], settled.at[:, lanes_of(tp)], settled_cols.at[0:(ntp - 1) * own_rows])
    settled[:, lanes_of(tp)] = settled_cols[rows_at(tp)]
    drain()
    phase("stats")
    await_bytes(*rowed)
    whole = settled[...]
    mean = jnp.mean(whole, axis=-1, keepdims=True)
    spread = jnp.mean(jnp.square(whole - mean), axis=-1, keepdims=True)
    rate = lax.rsqrt(spread + 1e-05)
    settled[...] = (whole - mean) * rate * gains[0:1]
    lane = iota((own_rows, LANES), 1)
    offset = jnp.zeros((own_rows, LANES), F32)
    for k in range(ntp):
        shift = jnp.mean(whole[:, k * LANES:(k + 1) * LANES], axis=-1, keepdims=True) - mean
        offset = jnp.where((lane % ntp == k) & (lane < 3 * ntp), shift, offset)
    coarse = offset.astype(BF16).astype(F32)
    offset = jnp.where((lane >= ntp) & (lane < 2 * ntp), offset - coarse, coarse)
    for k in range(3):
        top = rate.astype(BF16).astype(F32)
        offset = jnp.where(lane == 3 * ntp + k, top, offset)
        rate = rate - top
    own_stats[...] = offset.astype(BF16)
    told = over_tp(lambda to: own_stats, stats.at[rows_at(tp)], stats.at[0:(ntp - 1) * own_rows])
    stats[rows_at(tp)] = own_stats[...]
    phase("dispatch_wait")

    ring_sent, hand_sent = new_sem(), new_sem()
    counts_of = [0, 0]

    def ways_at(q, h):
        return [way for way in (1, -1) if h < half_way - chains[chain_no[way, q]][2]]

    def some_rows(count):
        return rows.at[0, 0:count * crow]

    def hand_on(q, spots):
        sem = new_sem()
        for place in spots:
            at = rows.at[slot(place, c), chunk(q)]
            push(at, at, hand_sent, sem, sib)
            counts_of[1] += 1
        return (some_rows(len(spots)), sem), q, spots

    def ring(q, h):
        sem = new_sem()
        for way in ways_at(q, h):
            at = rows.at[slot(chip(-way * h), c), chunk(q)]
            push(at, at, ring_sent, sem, at_chip(chip(way)))
            counts_of[0] += 1
        return some_rows(len(ways_at(q, h))), sem

    def grow_acc(item, q, spots, fresh=False):
        await_bytes(*item)
        more = None
        for place in spots:
            both = jnp.concatenate([rows[slot(place, 0), chunk(q)], rows[slot(place, 1), chunk(q)]], axis=1)
            one = mm(both, wgu[pl.ds(pl.multiple_of(place * 2 * LANES, 2 * LANES), 2 * LANES)])
            more = one if more is None else more + one
        acc[chunk(q)] = more if fresh else acc[chunk(q)] + more

    link, passed = [], []
    for q in range(CHUNKS):
        if coming[q]:
            await_bytes(*coming[q])
        rows[tp, chunk(q)] = darr[units(q)].reshape(crow, LANES)
        link.append(ring(q, 0))
        passed.append((*hand_on(q, [y]), True))
    phase("gather_ring")
    for h in range(half_way - 1):
        fresh = []
        for q in range(CHUNKS):
            await_bytes(*link[q])
            if ways_at(q, h + 1):
                link[q] = ring(q, h + 1)
            fresh.append(hand_on(q, [chip(-way * (h + 1)) for way in ways_at(q, h)]))
            if h == 0 and q == 1:
                await_bytes(*told)
                facts = to_experts(stats, xsend, xarr)
            if h > 0:
                grow_acc(*passed[q])
        if h == 0:
            for item in passed:
                grow_acc(*item)
        passed = fresh
    for q in range(CHUNKS):
        grow_acc(*passed[q])

    def last_piece(q):
        await_bytes(*link[q])
        return hand_on(q, [chip(half_way)])

    def own_part(place, q):
        return mm(act[chunk(q)], down[:, lanes_of(slot(place, c))])

    sent, reduced, all_sent = {}, [0], new_sem()

    def landed(q, t):
        await_bytes(rarr.at[0, 0:len(ways_at(q, t))], sent[q])

    def reduce_step(q, t):
        ways = ways_at(q, t)
        where = {way: t + chains[chain_no[way, q]][2] for way in ways}
        totals = {way: own_part(chip(way * (half_way - where[way])), q) for way in ways}
        if t > 0:
            landed(q, t - 1)
        sent[q] = new_sem()
        for way in ways:
            n, h = chain_no[way, q], where[way]
            total = totals[way]
            if t > 0:
                total = total + rarr[n, h - 1].astype(F32)
            rbuf[n, h] = total.astype(BF16)
            push(rbuf.at[n, h], rarr.at[n, h], all_sent, sent[q], at_chip(chip(way)))
            reduced[0] += 1

    def told_rows(q):
        return xarr[units(q)].reshape(crow, LANES)

    def finish_rows(item):
        grow_acc(*item)
        q = item[1]
        rate = told_rows(q)[:, 3 * ntp:3 * ntp + 3].astype(F32)
        a = acc[chunk(q)] * jnp.sum(rate, axis=-1, keepdims=True)
        for k in range(2):
            gate, up = a[:, 2 * k * LANES:(2 * k + 1) * LANES], a[:, (2 * k + 1) * LANES:(2 * k + 2) * LANES]
            act[chunk(q), k * LANES:(k + 1) * LANES] = (jax.nn.silu(gate) * up).astype(BF16)
        reduce_step(q, 0)

    phase("facts")
    for q in range(CHUNKS):
        if facts[q]:
            await_bytes(*facts[q])
        acc[chunk(q)] = acc[chunk(q)] + mm(told_rows(q), tilt[...])
    drain()
    phase("last_pieces")
    waiting = [last_piece(0)]
    for q in range(1, CHUNKS):
        waiting.append(last_piece(q))
        finish_rows(waiting[q - 1])
    finish_rows(waiting[CHUNKS - 1])
    phase("reduce_ring")
    for t in range(1, half_way):
        for q in range(CHUNKS):
            reduce_step(q, t)
    left.append((rbuf.at[0:reduced[0] // half_way], all_sent))
    left.append((rows.at[0:counts_of[0] // CHUNKS], ring_sent))
    left.append((rows.at[0:counts_of[1] // CHUNKS], hand_sent))
    all_sent, arrived = new_sem(), [new_sem() for q in range(CHUNKS)]
    for q in range(CHUNKS):
        total = own_part(y, q)
        landed(q, half_way - 1)
        for way in (1, -1):
            total = total + rarr[chain_no[way, q], half_way - 1].astype(F32)
        rsend[units(q)] = total.astype(BF16).reshape(crow // 8, 8, LANES)
        for p in peers(q):
            at = slice(p * unit, (p + 1) * unit)
            push(rsend.at[at], rback.at[at], all_sent, arrived[q], to_sp(p, -1))
    left.append((rsend.at[0:(nsp - 1) * unit], all_sent))
    rback[(nsp - 1) * unit:nsp * unit] = rsend[(nsp - 1) * unit:nsp * unit]
    phase("return_wait")
    drain()
    total = None
    for q in range(CHUNKS):
        if peers(q):
            await_bytes(rback.at[peers(q)[0] * unit:(peers(q)[-1] + 1) * unit], arrived[q])
        back = rback[units(q)].reshape(crow, LANES)
        more = mm(pick_hi[q], back) + mm(pick_lo[q], back)
        total = more if total is None else total + more
    phase("combine")
    term[...] = total.astype(BF16)
    phase("mix_over_tp")
    moved = over_tp(lambda to: term.at[rows_at(to)], mix.at[:, lanes_of(tp)], cols.at[0:(ntp - 1) * own_rows])
    mix[:, lanes_of(tp)] = term[rows_at(tp)]
    await_bytes(*moved)
    phase("last_norm")
    out[...] = layer_norm(settled[...] + mix[...].astype(F32), gains[1:2]).astype(BF16)

    phase("drain")
    drain()
    phase(None)


def layer(nsp, ntp, *args):
    (q1, k1, v1, g1, d1, q2, k2, v2, g2, d2, hg, p1, p2, st, gm, go, rt, af, eg, eu, ed) = args
    toks = q1.shape[0]
    width = st.shape[1]
    own_rows = toks // ntp
    cap = 3 * toks * 2 // (2 * nsp)
    nrow = nsp * cap
    ny = ntp // 2
    steps = ny // 2
    per = LANES // nsp
    mrow = -(-(3 * per + 3) // 16) * 16
    V = pltpu.VMEM
    D = pltpu.SemaphoreType.DMA
    one = (hg.reshape(1, -1), gm.reshape(1, -1), go.reshape(1, -1), rt.T, af.T)
    q1, k1 = q1.T, k1.T
    d1 = d1.transpose(0, 2, 1).reshape(2 * q1.shape[0], toks)
    operands = (q1, k1, v1, g1, d1, q2, k2, v2, g2, d2, one[0], p1, p2, st, one[1], one[2], one[3], one[4], eg, eu, ed)
    scratch = [
        V((2, *q1.shape), BF16), V((4, *q2.shape), BF16), V((2, *q2.shape), BF16), V(d1.shape, F32), V(d2.shape, F32),
        V((1, LANES), F32), V((2 * LANES, width), BF16), V((2 * LANES, width), BF16), V((toks, LANES), BF16),
        V((2, width), F32), V((2, toks), jnp.int32), V((2, toks), F32),
        V((width, 4 * LANES), BF16), V((2 * LANES, width), BF16),
        V((nsp, mrow, LANES), BF16), V((nsp, mrow, LANES), BF16), V((nsp, mrow, LANES), F32),
        V((nsp, mrow, LANES), BF16), V((nsp, mrow, LANES), BF16),
        V((3, toks, LANES), BF16), V((3, toks, LANES), BF16), V((3, toks // BLK, LANES, LANES), F32),
        V((2, toks, LANES), F32), V((toks, 2 * LANES), BF16), V((toks, 2 * LANES), BF16),
        V((ny, toks, LANES), F32),
        V((2 * CHUNKS, 4, toks // CHUNKS, LANES), BF16), V((2 * CHUNKS, 4, toks // CHUNKS, LANES), BF16),
        V((own_rows, width), F32), V((toks, LANES), F32), V((own_rows, LANES), BF16), V((toks, LANES), BF16),
        V((nrow, toks), BF16), V((nrow // 8, 8, LANES), BF16), V((nrow // 8, 8, LANES), BF16), V((LANES, 4 * LANES), BF16),
        V((toks, LANES), BF16),
        V((nrow // 8, 8, LANES), BF16), V((nrow // 8, 8, LANES), BF16), V((ntp, nrow, LANES), BF16),
        V((nrow, 4 * LANES), F32), V((nrow, 2 * LANES), BF16),
        V((2 * CHUNKS, steps, nrow // CHUNKS, LANES), BF16), V((2 * CHUNKS, steps, nrow // CHUNKS, LANES), BF16),
        V((nrow // 8, 8, LANES), BF16), V((nrow // 8, 8, LANES), BF16),
        V((CHUNKS, toks, nrow // CHUNKS), BF16), V((CHUNKS, toks, nrow // CHUNKS), BF16),
        V((toks, LANES), BF16), V((own_rows, width), BF16),
        D((116,)),
    ]
    return pl.pallas_call(
        functools.partial(kernel, (nsp, 4 if nsp % 4 == 0 else 1, ntp, toks, cap)),
        out_shape=jax.ShapeDtypeStruct((own_rows, width), BF16),
        in_specs=[pl.BlockSpec(memory_space=ANY)] * len(operands),
        out_specs=pl.BlockSpec(memory_space=pltpu.VMEM),
        scratch_shapes=scratch,
        compiler_params=pltpu.CompilerParams(collective_id=0, has_side_effects=True, vmem_limit_bytes=48 * 1024 * 1024),
        name="layer",
    )(*[pltpu.with_memory_space_constraint(a, pltpu.HBM) for a in operands])


def solution(mesh):
    spec = P("sp", "tp")
    fade = P(None, "sp", "tp")
    return jax.shard_map(
        functools.partial(layer, mesh.shape["sp"], mesh.shape["tp"]),
        mesh=mesh,
        in_specs=(
            spec, spec, spec, spec, fade, spec, spec, spec, spec, fade,
            P(), P("tp", None), P("tp", None), P("sp", None), P(), P(), P("sp", None), P("sp", None),
            P("sp", None, "tp"), P("sp", None, "tp"), P("sp", "tp", None),
        ),
        out_specs=P(("sp", "tp"), None),
        check_vma=False,
    )
```

```python
import functools

import jax
import jax.numpy as jnp
from jax import lax
from jax.experimental import pallas as pl
from jax.experimental.pallas import tpu as pltpu
from jax.sharding import PartitionSpec as P

MESH = pl.DeviceIdType.MESH
F32 = jnp.float32
BF16 = jnp.bfloat16
BLK = 64
CHUNKS = 4
LANES = 128
ANY = pl.ANY


def mm(a, b):
    return jnp.dot(a, b, preferred_element_type=F32)


def mm_t(a, b):
    return lax.dot_general(a, b, (((1,), (1,)), ((), ())), preferred_element_type=F32)


def tmm(a, b):
    return lax.dot_general(a, b, (((0,), (0,)), ((), ())), preferred_element_type=F32)


def iota(shape, dim):
    return lax.broadcasted_iota(jnp.int32, shape, dim)


def far_first(sizes):
    steps = [()]
    for size in sizes:
        steps = [done + (k,) for done in steps for k in range(size)]
    return sorted(steps, key=lambda d: (-sum(min(k, n - k) for k, n in zip(d, sizes)), d))


def layer_norm(values, gain):
    mean = jnp.mean(values, axis=-1, keepdims=True)
    spread = jnp.mean(jnp.square(values - mean), axis=-1, keepdims=True)
    return (values - mean) * lax.rsqrt(spread + 1e-05) * gain


def kernel(
    cfg,
    q1h, k1h, v1h, g1h, d1h, q2h, k2h, v2h, g2h, d2h, hgh, p1h, p2h, sth, gmh, goh, rth, afh, egh, euh, edh,
    out,
    qk1, wide_in, gates, d1, d2, hg, own_proj, other_proj, stream, gains, rt, af, wgu, down,
    sbuf, sarr, fsum, sret, sback,
    qin, kin, grow, mixed, heads, heads_in, part,
    pbuf, parr, settled, settled_cols, own_stats, stats, chosen, xsend, xarr, tilt, cols, dsend, darr, rows, acc, act, rbuf, rarr, rsend, rback,
    pick_hi, pick_lo, term, mix,
    sems,
):
    nsp, nx, ntp, toks, cap = cfg
    nz = nsp // nx
    ny = ntp // 2
    half_way = ny // 2
    sp = lax.axis_index("sp")
    tp = lax.axis_index("tp")
    y = lax.div(tp, 2)
    c = lax.rem(tp, 2)
    sib = (sp, tp + 1 - 2 * c)
    blocks = toks // BLK
    own_rows = toks // ntp
    width = ntp * LANES
    per = LANES // nsp
    mrow = sbuf.shape[1]
    nrow = nsp * cap
    crow = nrow // CHUNKS
    z_at, x_at = lax.div(sp, nx), lax.rem(sp, nx)
    sp_moves = far_first((nz, nx))
    tp_moves = far_first((ny, 2))

    def sp_peer(move, way):
        return lax.rem(z_at + way * move[0] + nz, nz) * nx + lax.rem(x_at + way * move[1] + nx, nx)

    def chip(step):
        return lax.rem(y + step + ny, ny)

    def tp_peer(move):
        return 2 * chip(move[0]) + lax.rem(c + move[1], 2)

    scope = []

    def phase(name):
        if scope:
            scope.pop().__exit__(None, None, None)
        if name:
            scope.append(jax.named_scope(name))
            scope[0].__enter__()

    numbers = iter(range(sems.shape[0]))

    def new_sem():
        return sems.at[next(numbers)]

    def await_bytes(ref, sem):
        pltpu.make_async_copy(ref, ref, sem).wait()

    def load(*pairs):
        sem = new_sem()
        for src, dst in pairs:
            pltpu.make_async_copy(src, dst, sem).start()
        return sem

    phase("greet")
    barrier = pltpu.get_barrier_semaphore()
    for move in sp_moves[:-1]:
        pl.semaphore_signal(barrier, inc=1, device_id=(sp_peer(move, 1), tp), device_id_type=MESH)
    for move in tp_moves[:-1]:
        pl.semaphore_signal(barrier, inc=1, device_id=(sp, tp_peer(move)), device_id_type=MESH)
    first = [
        (d1, load((d1h, d1))), (d2, load((d2h, d2))),
        (wide_in, load((k2h, wide_in.at[0]), (v1h, wide_in.at[1]), (v2h, wide_in.at[2]), (q2h, wide_in.at[3]))),
        (qk1, load((q1h, qk1.at[0]), (k1h, qk1.at[1]))),
    ]
    own_stream = sth.at[:, pl.ds(pl.multiple_of(tp * LANES, LANES), LANES)]
    second = [
        (gates, load((g1h, gates.at[0]), (g2h, gates.at[1]))), (hg, load((hgh, hg))),
        (own_proj, load((p1h, own_proj.at[0:LANES]), (p2h, own_proj.at[LANES:2 * LANES]))),
        (stream, load((own_stream, stream))), (gains, load((gmh, gains.at[0:1]), (goh, gains.at[1:2]))),
        (rt, load((rth, rt))), (af, load((afh, af))),
        (wgu.at[:, 0:2 * LANES], load((egh.at[0], wgu.at[:, 0:LANES]), (euh.at[0], wgu.at[:, LANES:2 * LANES]))),
        (down.at[0:LANES], load((edh.at[0], down.at[0:LANES]))),
    ]

    phase("constants")
    r = iota((toks, toks), 0)
    s = iota((toks, toks), 1)
    tri = jnp.where((r // BLK == s // BLK) & (s <= r), 1.0, 0.0).astype(BF16)
    low = iota((1, LANES), 1) < LANES // 2
    m = iota((nsp * mrow, LANES), 0)
    o, i = m // mrow, m % mrow
    wanted = jnp.where(i < 3 * per, (i // per) * LANES + o * per + i % per, 3 * LANES + i - 3 * per)
    wanted = jnp.where(i < 3 * per + 3, wanted, -1)
    lane = iota((nsp * mrow, LANES), 1)
    pack = [jnp.where(wanted == lane + g * LANES, 1.0, 0.0).astype(BF16) for g in range(3)]
    lane16 = iota((nsp * mrow, 16), 1)
    pack.append(jnp.where(wanted[:, 0:16] == lane16 + 3 * LANES, 1.0, 0.0).astype(BF16))

    phase("load_wait")
    for item in first:
        await_bytes(*item)
    phase("fading")

    def two(a):
        a = a.astype(F32)
        return jnp.concatenate([a, a], axis=0).T

    fading = (d1[...].T, d2[0], d2[1])
    keys = (two(qk1[1]), wide_in[0].astype(F32), wide_in[0].astype(F32))
    queries = (two(qk1[0]) * 64 ** (-0.5), wide_in[3].astype(F32) * 128 ** (-0.5), wide_in[3].astype(F32) * 128 ** (-0.5))
    values = (wide_in[1], wide_in[2], wide_in[2])
    totals = []
    for g in range(3):
        x = fading[g]
        logs = (jnp.minimum(x, 0.0) - jnp.log1p(jnp.exp(-jnp.abs(x)))) * (1.0 / 16.0)
        hi = logs.astype(BF16)
        rest = logs - hi.astype(F32)
        mid = rest.astype(BF16)
        lo = (rest - mid.astype(F32)).astype(BF16)
        cum = mm(tri, hi) + mm(tri, mid) + mm(tri, lo)
        rows_of = []
        for b in range(blocks):
            at = slice(b * BLK, (b + 1) * BLK)
            ahead = cum[at]
            tot = ahead[BLK - 1:BLK]
            behind = tot - ahead + logs[at]
            run = ahead if g == 1 else behind if g == 2 else jnp.where(low, ahead, behind)
            qin[g, at] = (queries[g][at] * jnp.exp(run)).astype(BF16)
            kin[g, at] = (keys[g][at] * jnp.exp(-run)).astype(BF16)
            kst = (keys[g][at] * jnp.exp(tot - run)).astype(BF16)
            grow[g, b] = tmm(values[g][at], kst)
            rows_of.append(tot)
        totals.append(rows_of)

    fades = [[jnp.exp(t) for t in row] for row in totals]

    def chained(g, order, start):
        state = start
        seen = {}
        for b in order:
            seen[b] = state
            state = fades[g][b] * state + grow[g, b]
        return seen, state

    phase("chain")
    rise, fall = list(range(blocks)), list(range(blocks - 1, -1, -1))
    zero = jnp.zeros((LANES, LANES), F32)
    ends = [
        jnp.where(low, chained(0, rise, zero)[1], chained(0, fall, zero)[1]),
        chained(1, rise, zero)[1],
        chained(2, fall, zero)[1],
    ]
    sums = [sum(row[1:], row[0]) for row in totals]
    r16 = iota((16, LANES), 0)
    tail = jnp.where(r16 == 0, sums[0], jnp.where(r16 == 1, sums[1], jnp.where(r16 == 2, sums[2], 0.0)))
    packed = mm(pack[3], tail.astype(BF16))
    for g in range(3):
        packed = packed + mm(pack[g], ends[g].astype(BF16))
    sbuf[...] = packed.astype(BF16).reshape(nsp, mrow, LANES)

    phase("barrier")
    pl.semaphore_wait(barrier, nsp - 1 + ntp - 1)

    left = []

    def push(src, dst, ssem, rsem, device):
        pltpu.make_async_remote_copy(src, dst, ssem, rsem, device_id=device, device_id_type=MESH).start()

    def lend(size, *pairs):
        ssem, rsem = new_sem(), new_sem()
        for src, dst in pairs:
            push(src, dst, ssem, rsem, sib)
        left.append((size, ssem))
        return size, rsem

    def drain():
        while left:
            await_bytes(*left.pop(0))

    def to_sp(p, way=1):
        return (sp_peer(sp_moves[p], way), tp)

    phase("send_states")
    def over_sp(src, dst):
        ssem, rsem = new_sem(), new_sem()
        for p in range(nsp - 1):
            to = to_sp(p)
            push(src.at[to[0]], dst.at[sp], ssem, rsem, to)
        left.append((src.at[0:nsp - 1], ssem))
        dst[sp] = src[sp]
        return dst.at[0:nsp - 1], rsem

    coming = over_sp(sbuf, sarr)
    lent_proj = lend(other_proj, (p1h, other_proj.at[0:LANES]), (p2h, other_proj.at[LANES:2 * LANES]))
    lent_wgu = lend(
        wgu.at[:, 2 * LANES:4 * LANES], (egh.at[0], wgu.at[:, 2 * LANES:3 * LANES]), (euh.at[0], wgu.at[:, 3 * LANES:4 * LANES])
    )
    lent_down = lend(down.at[LANES:2 * LANES], (edh.at[0], down.at[LANES:2 * LANES]))

    phase("inner")
    rr, cc = iota((BLK, BLK), 0), iota((BLK, BLK), 1)
    lower, upper = cc <= rr, cc >= rr
    for b in range(blocks):
        at = slice(b * BLK, (b + 1) * BLK)
        q, k = qin[0, at], kin[0, at]
        nil = jnp.zeros_like(q)
        score = jnp.where(lower, mm_t(jnp.where(low, q, nil), k), 0.0) + jnp.where(upper, mm_t(jnp.where(low, nil, q), k), 0.0)
        mixed[0, at] = mm(score.astype(BF16), values[0][at])
        score = jnp.where(lower, mm_t(qin[1, at], kin[1, at]), 0.0) + jnp.where(upper, mm_t(qin[2, at], kin[2, at]), 0.0)
        mixed[1, at] = mm(score.astype(BF16), values[1][at])

    def reached(g, order):
        share = jnp.ones((1, LANES), F32)
        seen = {}
        for b in order:
            seen[b] = share
            share = share * fades[g][b]
        return seen

    rise_a, fall_a = chained(0, rise, zero)[0], chained(0, fall, zero)[0]
    rise_b, fall_b = chained(1, rise, zero)[0], chained(2, fall, zero)[0]
    reach = [
        {b: jnp.where(low, reached(0, rise)[b], reached(0, fall)[b]) for b in rise}, reached(1, rise), reached(2, fall)
    ]
    for b in range(blocks):
        at = slice(b * BLK, (b + 1) * BLK)
        mixed[0, at] = mixed[0, at] + mm_t(qin[0, at], jnp.where(low, rise_a[b], fall_a[b]).astype(BF16))
        mixed[1, at] = mixed[1, at] + mm_t(qin[1, at], rise_b[b].astype(BF16)) + mm_t(qin[2, at], fall_b[b].astype(BF16))
        for g in range(3):
            qin[g, at] = (qin[g, at].astype(F32) * reach[g][b]).astype(BF16)

    phase("wait_states")
    await_bytes(*coming)
    phase("scan")
    row = iota((mrow, LANES), 0)
    in_a, in_b = row < per, row < 2 * per

    def tile_of(j):
        t = sarr[j].astype(F32)
        fade = jnp.where(in_a, t[3 * per:3 * per + 1], jnp.where(in_b, t[3 * per + 1:3 * per + 2], t[3 * per + 2:3 * per + 3]))
        return t, jnp.exp(fade)

    state = jnp.zeros((mrow, LANES), F32)
    for j in range(nsp):
        t, fade = tile_of(j)
        fsum[j] = state
        state = fade * state + t
    forward = (in_a & low) | (in_b & jnp.logical_not(in_a))
    state = jnp.zeros((mrow, LANES), F32)
    for j in range(nsp - 1, -1, -1):
        t, fade = tile_of(j)
        sret[j] = jnp.where(forward, fsum[j], state).astype(BF16)
        state = fade * state + t
    phase("send_back")
    coming = over_sp(sret, sback)

    phase("places")
    z = iota((LANES, nsp * mrow), 0)
    m = iota((LANES, nsp * mrow), 1)
    lift = (z // per) * mrow + z % per
    unpack = [jnp.where(m == lift + g * per, 1.0, 0.0).astype(BF16) for g in range(3)]

    for item in second:
        await_bytes(*item)
    experts = iota((nsp, toks), 0)
    hits = [jnp.where(rt[k:k + 1] == experts, 1.0, 0.0) for k in range(2)]
    before = jnp.where(r < s, 1.0, 0.0).astype(BF16)
    counts = mm((hits[0] + hits[1]).astype(BF16), before)
    spot = jnp.zeros((nsp, toks), jnp.int32)
    for p, move in enumerate(sp_moves):
        spot = jnp.where(experts == sp_peer(move, 1), p * cap, spot)
    counts = counts + spot.astype(F32)
    places = [jnp.sum(hits[k] * counts, axis=0, keepdims=True).astype(jnp.int32) for k in range(2)]

    slots = iota((nrow, toks), 0)
    named = [slots == places[k] for k in range(2)]
    chosen[...] = jnp.where(named[0] | named[1], 1.0, 0.0).astype(BF16)
    share = af[0:1] + af[1:2]
    scaled = jnp.where(named[0], af[0:1] / share, 0.0) + jnp.where(named[1], af[1:2] / share, 0.0)
    for q in range(CHUNKS):
        some = scaled[q * crow:(q + 1) * crow].T
        high = some.astype(BF16)
        pick_hi[q] = high
        pick_lo[q] = (some - high.astype(F32)).astype(BF16)

    await_bytes(*lent_wgu)
    apart = jnp.where(iota((ntp, width), 1) // LANES == iota((ntp, width), 0), gains[0:1], 0.0)
    coarse = apart.astype(BF16)
    fine = (apart - coarse.astype(F32)).astype(BF16)
    slope = mm(coarse, wgu[...]) + mm(fine, wgu[...])
    coarse = slope.astype(BF16)
    fine = (slope - coarse.astype(F32)).astype(BF16)
    tilt[0:ntp], tilt[ntp:2 * ntp], tilt[2 * ntp:3 * ntp] = coarse, coarse, fine
    tilt[3 * ntp:LANES] = jnp.zeros((LANES - 3 * ntp, 4 * LANES), BF16)
    await_bytes(*lent_proj)
    await_bytes(*lent_down)

    phase("wait_back")
    await_bytes(*coming)
    phase("readout")
    back = sback[...].reshape(nsp * mrow, LANES)
    come = [mm(unpack[g], back).astype(BF16) for g in range(3)]
    shared = []
    for n in range(2):
        at = slice(n * toks // 2, (n + 1) * toks // 2)
        one = mixed[0, at] + mm_t(qin[0, at], come[0])
        other = mixed[1, at] + mm_t(qin[1, at], come[1]) + mm_t(qin[2, at], come[2])
        for k, (value, gate) in enumerate(((one, gates.at[0]), (other, gates.at[1]))):
            normed = value * lax.rsqrt(jnp.mean(value * value, axis=-1, keepdims=True) + 1e-06) * hg[...]
            heads[at, k * LANES:(k + 1) * LANES] = (normed * jax.nn.silu(gate[at].astype(F32))).astype(BF16)
        shared.append((at, lend(heads_in.at[at], (heads.at[at], heads_in.at[at]))))

    phase("proj")
    def lanes_of(k):
        return pl.ds(pl.multiple_of(k * LANES, LANES), LANES)

    def rows_at(k):
        return pl.ds(pl.multiple_of(k * own_rows, own_rows), own_rows)

    def slot(place, core):
        return 2 * place + core

    order = (3, ny - 3, 4, 1, ny - 1, 2, ny - 2, 0)
    far = [chip(d) for d in order]
    for both, item in shared:
        for d in far:
            part[d, both] = mm(heads[both], own_proj[:, lanes_of(slot(d, c))])

    phase("attn_ring")
    chains = [(way, q, (q % 2 == 0) != (way == 1)) for q in range(CHUNKS) for way in (1, -1)]
    chain_no = {(way, q): n for n, (way, q, skip) in enumerate(chains)}

    def at_chip(place):
        return (sp, 2 * place + c)

    tall = toks // CHUNKS
    pieces, all_sent = [0], new_sem()

    def span(q):
        return slice(q * tall, (q + 1) * tall)

    def toward(n, kind, total, hops, sem):
        way = chains[n][0]
        pbuf[n, kind] = total.astype(BF16)
        push(pbuf.at[n, kind], parr.at[n, kind], all_sent, sem, at_chip(chip(way * hops)))
        pieces[0] += 1

    early = [new_sem() for n in chains]
    final = [new_sem() for q in range(CHUNKS)]
    for both, item in shared:
        await_bytes(*item)
        for d in far:
            part[d, both] = part[d, both] + mm(heads_in[both], other_proj[:, lanes_of(slot(d, c))])
        for n, (way, q, skip) in enumerate(chains):
            if both.start <= span(q).start < both.stop:
                toward(n, 0, part[chip(3 * way), span(q)], 1, early[n])
                if not skip:
                    toward(n, 1, part[chip(4 * way), span(q)], 2, early[n])
    for n, (way, q, skip) in enumerate(chains):
        toward(n, 2, part[chip(way), span(q)], 1, final[q])
    for n, (way, q, skip) in enumerate(chains):
        kinds = 1 if skip else 2
        await_bytes(parr.at[n, 0:kinds], early[n])
        total = part[chip(2 * way), span(q)]
        for kind in range(kinds):
            total = total + parr[n, kind].astype(F32)
        toward(n, 3, total, 2, final[q])
    own_gain = gains[0:1, lanes_of(tp)]
    for q in range(CHUNKS):
        total = part[y, span(q)]
        await_bytes(parr.at[0], final[q])
        for kind in (2, 3):
            for way in (1, -1):
                total = total + parr[chain_no[way, q], kind].astype(F32)
        summed = stream[span(q)].astype(F32) + total.astype(BF16).astype(F32)
        settled_cols[span(q)] = summed
        cols[span(q)] = ((summed - jnp.mean(summed, axis=-1, keepdims=True)) * own_gain).astype(BF16)
    left.append((pbuf.at[0:pieces[0] // 4], all_sent))
    phase("dispatch")

    def over_tp(src_of, dst, size):
        ssem, rsem = new_sem(), new_sem()
        for move in tp_moves[:-1]:
            to = tp_peer(move)
            push(src_of(to), dst, ssem, rsem, (sp, to))
        left.append((size, ssem))
        return size, rsem

    unit = cap // 8

    def chunk(q):
        return slice(q * crow, (q + 1) * crow)

    def units(q):
        return slice(q * crow // 8, (q + 1) * crow // 8)

    def peers(q):
        return range(q * nsp // CHUNKS, min((q + 1) * nsp // CHUNKS, nsp - 1))

    def to_experts(values, src, dst):
        all_sent, coming = new_sem(), []
        for q in range(CHUNKS):
            src[units(q)] = mm(chosen[chunk(q)], values[...]).astype(BF16).reshape(crow // 8, 8, LANES)
            rsem = new_sem()
            for p in peers(q):
                at = slice(p * unit, (p + 1) * unit)
                push(src.at[at], dst.at[at], all_sent, rsem, to_sp(p))
            coming.append((dst.at[peers(q)[0] * unit:(peers(q)[-1] + 1) * unit], rsem) if peers(q) else None)
        left.append((src.at[0:(nsp - 1) * unit], all_sent))
        dst[(nsp - 1) * unit:nsp * unit] = src[(nsp - 1) * unit:nsp * unit]
        return coming

    coming = to_experts(cols, dsend, darr)
    rowed = over_tp(lambda to: settled_cols.at[rows_at(to)], settled.at[:, lanes_of(tp)], settled_cols.at[0:(ntp - 1) * own_rows])
    settled[:, lanes_of(tp)] = settled_cols[rows_at(tp)]
    drain()
    phase("stats")
    await_bytes(*rowed)
    whole = settled[...]
    mean = jnp.mean(whole, axis=-1, keepdims=True)
    spread = jnp.mean(jnp.square(whole - mean), axis=-1, keepdims=True)
    rate = lax.rsqrt(spread + 1e-05)
    settled[...] = (whole - mean) * rate * gains[0:1]
    lane = iota((own_rows, LANES), 1)
    offset = jnp.zeros((own_rows, LANES), F32)
    for k in range(ntp):
        shift = jnp.mean(whole[:, k * LANES:(k + 1) * LANES], axis=-1, keepdims=True) - mean
        offset = jnp.where((lane % ntp == k) & (lane < 3 * ntp), shift, offset)
    coarse = offset.astype(BF16).astype(F32)
    offset = jnp.where((lane >= ntp) & (lane < 2 * ntp), offset - coarse, coarse)
    for k in range(3):
        top = rate.astype(BF16).astype(F32)
        offset = jnp.where(lane == 3 * ntp + k, top, offset)
        rate = rate - top
    own_stats[...] = offset.astype(BF16)
    told = over_tp(lambda to: own_stats, stats.at[rows_at(tp)], stats.at[0:(ntp - 1) * own_rows])
    stats[rows_at(tp)] = own_stats[...]
    phase("dispatch_wait")

    ring_sent, hand_sent = new_sem(), new_sem()
    counts_of = [0, 0]

    def ways_at(q, h):
        return [way for way in (1, -1) if h < half_way - chains[chain_no[way, q]][2]]

    def some_rows(count):
        return rows.at[0, 0:count * crow]

    def hand_on(q, spots):
        sem = new_sem()
        for place in spots:
            at = rows.at[slot(place, c), chunk(q)]
            push(at, at, hand_sent, sem, sib)
            counts_of[1] += 1
        return (some_rows(len(spots)), sem), q, spots

    def ring(q, h):
        sem = new_sem()
        for way in ways_at(q, h):
            at = rows.at[slot(chip(-way * h), c), chunk(q)]
            push(at, at, ring_sent, sem, at_chip(chip(way)))
            counts_of[0] += 1
        return some_rows(len(ways_at(q, h))), sem

    def grow_acc(item, q, spots, fresh=False):
        await_bytes(*item)
        more = None
        for place in spots:
            both = jnp.concatenate([rows[slot(place, 0), chunk(q)], rows[slot(place, 1), chunk(q)]], axis=1)
            one = mm(both, wgu[pl.ds(pl.multiple_of(place * 2 * LANES, 2 * LANES), 2 * LANES)])
            more = one if more is None else more + one
        acc[chunk(q)] = more if fresh else acc[chunk(q)] + more

    link, passed = [], []
    for q in range(CHUNKS):
        if coming[q]:
            await_bytes(*coming[q])
        rows[tp, chunk(q)] = darr[units(q)].reshape(crow, LANES)
        link.append(ring(q, 0))
        passed.append((*hand_on(q, [y]), True))
    phase("gather_ring")
    for h in range(half_way - 1):
        fresh = []
        for q in range(CHUNKS):
            await_bytes(*link[q])
            if ways_at(q, h + 1):
                link[q] = ring(q, h + 1)
            fresh.append(hand_on(q, [chip(-way * (h + 1)) for way in ways_at(q, h)]))
            if h == 0 and q == 1:
                await_bytes(*told)
                facts = to_experts(stats, xsend, xarr)
            if h > 0:
                grow_acc(*passed[q])
        if h == 0:
            for item in passed:
                grow_acc(*item)
        passed = fresh
    def last_piece(q):
        await_bytes(*link[q])
        return hand_on(q, [chip(half_way)])

    def own_part(place, q):
        return mm(act[chunk(q)], down[:, lanes_of(slot(place, c))])

    sent, reduced, all_sent = {}, [0], new_sem()

    def landed(q, t):
        await_bytes(rarr.at[0, 0:len(ways_at(q, t))], sent[q])

    def reduce_step(q, t):
        ways = ways_at(q, t)
        where = {way: t + chains[chain_no[way, q]][2] for way in ways}
        totals = {way: own_part(chip(way * (half_way - where[way])), q) for way in ways}
        if t > 0:
            landed(q, t - 1)
        sent[q] = new_sem()
        for way in ways:
            n, h = chain_no[way, q], where[way]
            total = totals[way]
            if t > 0:
                total = total + rarr[n, h - 1].astype(F32)
            rbuf[n, h] = total.astype(BF16)
            push(rbuf.at[n, h], rarr.at[n, h], all_sent, sent[q], at_chip(chip(way)))
            reduced[0] += 1

    def told_rows(q):
        return xarr[units(q)].reshape(crow, LANES)

    def finish_rows(item):
        grow_acc(*item)
        q = item[1]
        rate = told_rows(q)[:, 3 * ntp:3 * ntp + 3].astype(F32)
        a = acc[chunk(q)] * jnp.sum(rate, axis=-1, keepdims=True)
        for k in range(2):
            gate, up = a[:, 2 * k * LANES:(2 * k + 1) * LANES], a[:, (2 * k + 1) * LANES:(2 * k + 2) * LANES]
            act[chunk(q), k * LANES:(k + 1) * LANES] = (jax.nn.silu(gate) * up).astype(BF16)
        reduce_step(q, 0)

    phase("facts")
    for q in range(CHUNKS):
        if facts[q]:
            await_bytes(*facts[q])
        acc[chunk(q)] = acc[chunk(q)] + mm(told_rows(q), tilt[...])
    drain()
    for q in range(CHUNKS):
        grow_acc(*passed[q])
    phase("last_pieces")
    waiting = [last_piece(0)]
    for q in range(1, CHUNKS):
        waiting.append(last_piece(q))
        finish_rows(waiting[q - 1])
    finish_rows(waiting[CHUNKS - 1])
    phase("reduce_ring")
    for t in range(1, half_way):
        for q in range(CHUNKS):
            reduce_step(q, t)
    left.append((rbuf.at[0:reduced[0] // half_way], all_sent))
    left.append((rows.at[0:counts_of[0] // CHUNKS], ring_sent))
    left.append((rows.at[0:counts_of[1] // CHUNKS], hand_sent))
    all_sent, arrived = new_sem(), [new_sem() for q in range(CHUNKS)]
    for q in range(CHUNKS):
        total = own_part(y, q)
        landed(q, half_way - 1)
        for way in (1, -1):
            total = total + rarr[chain_no[way, q], half_way - 1].astype(F32)
        rsend[units(q)] = total.astype(BF16).reshape(crow // 8, 8, LANES)
        for p in peers(q):
            at = slice(p * unit, (p + 1) * unit)
            push(rsend.at[at], rback.at[at], all_sent, arrived[q], to_sp(p, -1))
    left.append((rsend.at[0:(nsp - 1) * unit], all_sent))
    rback[(nsp - 1) * unit:nsp * unit] = rsend[(nsp - 1) * unit:nsp * unit]
    phase("return_wait")
    drain()
    total = None
    for q in range(CHUNKS):
        if peers(q):
            await_bytes(rback.at[peers(q)[0] * unit:(peers(q)[-1] + 1) * unit], arrived[q])
        back = rback[units(q)].reshape(crow, LANES)
        more = mm(pick_hi[q], back) + mm(pick_lo[q], back)
        total = more if total is None else total + more
    phase("combine")
    term[...] = total.astype(BF16)
    phase("mix_over_tp")
    moved = over_tp(lambda to: term.at[rows_at(to)], mix.at[:, lanes_of(tp)], cols.at[0:(ntp - 1) * own_rows])
    mix[:, lanes_of(tp)] = term[rows_at(tp)]
    await_bytes(*moved)
    phase("last_norm")
    out[...] = layer_norm(settled[...] + mix[...].astype(F32), gains[1:2]).astype(BF16)

    phase("drain")
    drain()
    phase(None)


def layer(nsp, ntp, *args):
    (q1, k1, v1, g1, d1, q2, k2, v2, g2, d2, hg, p1, p2, st, gm, go, rt, af, eg, eu, ed) = args
    toks = q1.shape[0]
    width = st.shape[1]
    own_rows = toks // ntp
    cap = 3 * toks * 2 // (2 * nsp)
    nrow = nsp * cap
    ny = ntp // 2
    steps = ny // 2
    per = LANES // nsp
    mrow = -(-(3 * per + 3) // 16) * 16
    V = pltpu.VMEM
    D = pltpu.SemaphoreType.DMA
    one = (hg.reshape(1, -1), gm.reshape(1, -1), go.reshape(1, -1), rt.T, af.T)
    q1, k1 = q1.T, k1.T
    d1 = d1.transpose(0, 2, 1).reshape(2 * q1.shape[0], toks)
    operands = (q1, k1, v1, g1, d1, q2, k2, v2, g2, d2, one[0], p1, p2, st, one[1], one[2], one[3], one[4], eg, eu, ed)
    scratch = [
        V((2, *q1.shape), BF16), V((4, *q2.shape), BF16), V((2, *q2.shape), BF16), V(d1.shape, F32), V(d2.shape, F32),
        V((1, LANES), F32), V((2 * LANES, width), BF16), V((2 * LANES, width), BF16), V((toks, LANES), BF16),
        V((2, width), F32), V((2, toks), jnp.int32), V((2, toks), F32),
        V((width, 4 * LANES), BF16), V((2 * LANES, width), BF16),
        V((nsp, mrow, LANES), BF16), V((nsp, mrow, LANES), BF16), V((nsp, mrow, LANES), F32),
        V((nsp, mrow, LANES), BF16), V((nsp, mrow, LANES), BF16),
        V((3, toks, LANES), BF16), V((3, toks, LANES), BF16), V((3, toks // BLK, LANES, LANES), F32),
        V((2, toks, LANES), F32), V((toks, 2 * LANES), BF16), V((toks, 2 * LANES), BF16),
        V((ny, toks, LANES), F32),
        V((2 * CHUNKS, 4, toks // CHUNKS, LANES), BF16), V((2 * CHUNKS, 4, toks // CHUNKS, LANES), BF16),
        V((own_rows, width), F32), V((toks, LANES), F32), V((own_rows, LANES), BF16), V((toks, LANES), BF16),
        V((nrow, toks), BF16), V((nrow // 8, 8, LANES), BF16), V((nrow // 8, 8, LANES), BF16), V((LANES, 4 * LANES), BF16),
        V((toks, LANES), BF16),
        V((nrow // 8, 8, LANES), BF16), V((nrow // 8, 8, LANES), BF16), V((ntp, nrow, LANES), BF16),
        V((nrow, 4 * LANES), F32), V((nrow, 2 * LANES), BF16),
        V((2 * CHUNKS, steps, nrow // CHUNKS, LANES), BF16), V((2 * CHUNKS, steps, nrow // CHUNKS, LANES), BF16),
        V((nrow // 8, 8, LANES), BF16), V((nrow // 8, 8, LANES), BF16),
        V((CHUNKS, toks, nrow // CHUNKS), BF16), V((CHUNKS, toks, nrow // CHUNKS), BF16),
        V((toks, LANES), BF16), V((own_rows, width), BF16),
        D((116,)),
    ]
    return pl.pallas_call(
        functools.partial(kernel, (nsp, 4 if nsp % 4 == 0 else 1, ntp, toks, cap)),
        out_shape=jax.ShapeDtypeStruct((own_rows, width), BF16),
        in_specs=[pl.BlockSpec(memory_space=ANY)] * len(operands),
        out_specs=pl.BlockSpec(memory_space=pltpu.VMEM),
        scratch_shapes=scratch,
        compiler_params=pltpu.CompilerParams(collective_id=0, has_side_effects=True, vmem_limit_bytes=48 * 1024 * 1024),
        name="layer",
    )(*[pltpu.with_memory_space_constraint(a, pltpu.HBM) for a in operands])


def solution(mesh):
    spec = P("sp", "tp")
    fade = P(None, "sp", "tp")
    return jax.shard_map(
        functools.partial(layer, mesh.shape["sp"], mesh.shape["tp"]),
        mesh=mesh,
        in_specs=(
            spec, spec, spec, spec, fade, spec, spec, spec, spec, fade,
            P(), P("tp", None), P("tp", None), P("sp", None), P(), P(), P("sp", None), P("sp", None),
            P("sp", None, "tp"), P("sp", None, "tp"), P("sp", "tp", None),
        ),
        out_specs=P(("sp", "tp"), None),
        check_vma=False,
    )
```
